128 devices in a mesh: sp: 16 (over z, x), tp: 8 (over y, core).
Axes of the slice: x: 4, y: 4, z: 4, core: 2. Of those that a mesh axis runs over, the one named last changes fastest.
Arguments:
- tokens: bfloat16 [16384, 2048], P(('sp', 'tp')), may hold values from -6 to 6
- elapsed: float32 [16384], P(('sp', 'tp')), may hold values from 0 to 3, as said below
- norm_gain: float32 [2048], replicated, may hold values from 0.1 to 1.9
- in_weight: bfloat16 [2048, 1024], replicated, may hold values from -0.125 to 0.125
- state_input: bfloat16 [2, 2, 64, 64, 16], replicated, may hold values from -1.5 to 1.5
- state_output: float32 [2, 2, 64, 16, 64], replicated, may hold values from -0.375 to 0.375
- forget_rate: float32 [2, 64, 64], replicated, may hold values from 0 to 1, as said below
- decay_angle: float32 [2, 64, 64], replicated, may hold values from -3.140625 to 3.140625
- skip_gain: float32 [1024], replicated, may hold values from -4 to 4
- glu_weight: bfloat16 [1024, 1024], replicated, may hold values from -0.1875 to 0.1875
- glu_bias: float32 [1024], replicated, may hold values from -4 to 4
- out_weight: bfloat16 [1024, 2048], replicated, may hold values from -0.1875 to 0.1875
- out_gain: float32 [2048], replicated, may hold values from 0.1 to 1.9
Outputs:
- mixed: bfloat16 [16384, 2048], P(('sp', 'tp'))
The draws below stay inside these ranges and needn't reach their ends.
Inputs may be any that keep to these rules, and one draw needn't show every extreme that they name: `elapsed`: positive time steps. `forget_rate`: positive rates.
All inputs are finite; a program needn't handle non-finite values.
Results may differ from the reference program's by a relative error of at most 0.0067.
Values sent between devices are 32-bit elements; how exact they have to be, the bound alone decides.
No kernel may reach another device: no remote copies, remote signals or barrier semaphores. Data moves between devices by JAX's collectives and lax.ppermute only.
A program may use at most 128 MiB of HBM per device.

```python
import math
import jax
import jax.numpy as jnp
from jax import lax

D = 2048
GROUPS = 64
WIDTH = 16
STATE = 64
CHANNELS = 1024
TOK_DEV = 128
SEQ = 16384


def draw_elapsed(key, part):
    first_key, second_key = jax.random.split(key)
    factor = jnp.exp(jax.random.uniform(first_key, (64,), jnp.float32, math.log(0.5), math.log(2.0)))
    jitter = jax.random.uniform(second_key, (SEQ,), jnp.float32, 0.7, 1.4)
    return jnp.repeat(factor, SEQ // 64, total_repeat_length=SEQ) * jitter


def draw_forget_rate(key, part):
    pick_key, quick_key, slow_key = jax.random.split(key, 3)
    share = 0.5
    quick_groups = jax.random.bernoulli(pick_key, share, (2, GROUPS, 1))
    quick = jnp.exp(jax.random.uniform(quick_key, (2, GROUPS, STATE), jnp.float32, math.log(1.0 / 100.0), math.log(1.0 / 30.0)))
    slow = jnp.exp(jax.random.uniform(slow_key, (2, GROUPS, STATE), jnp.float32, math.log(0.05 / SEQ), math.log(2.0 / SEQ)))
    return jnp.where(quick_groups, quick, slow)


def steps_of(stream_key, shape, cuts, low, top_value):
    def one(position, shards_of):
        steps = jax.random.uniform(jax.random.fold_in(jax.random.fold_in(stream_key, 6), position), (shards_of,), jnp.float32, low / len(cuts), top_value / len(cuts))
        return jnp.repeat(jnp.exp(steps), shape[position] // shards_of).reshape((-1,) + (1,) * (len(shape) - position - 1))

    gain = one(*cuts[0])
    for cut in cuts[1:]:
        gain = gain * one(*cut)
    return gain


def centred(key, extent, deviation, reach, pieces=(), dtype=jnp.bfloat16):
    loudness = steps_of(key, extent, pieces, -0.22, 0.18) if pieces else 1.0
    values = jax.random.normal(key, extent, jnp.float32) * deviation * loudness
    return jnp.minimum(jnp.maximum(values, -reach), reach).astype(dtype)


def setup_inputs(seed: int = 0) -> dict:
    splits = jax.random.split(jax.random.key(seed), 14)
    tokens = centred(splits[0], (SEQ, D), 1.0, 6.0, ((0, 128),))
    elapsed = draw_elapsed(jax.random.fold_in(splits[13], 71), 0)
    norm_gain = jnp.clip(1.0 + 0.18 * jax.random.normal(splits[2], (D,), jnp.float32), 0.1, 1.9)
    in_weight = centred(splits[3], (D, CHANNELS), D ** -0.5, 0.125)
    state_input = centred(splits[4], (2, 2, GROUPS, STATE, WIDTH), WIDTH ** -0.5, 1.5)
    state_output = centred(splits[5], (2, 2, GROUPS, WIDTH, STATE), (4 * STATE) ** -0.5, 0.375, (), jnp.float32)
    forget_rate = draw_forget_rate(jax.random.fold_in(splits[13], 71), 0)
    decay_angle = jnp.clip(jax.random.uniform(splits[7], (2, GROUPS, STATE), jnp.float32, -3.140625, 3.140625), -3.140625, 3.140625)
    skip_gain = centred(splits[8], (CHANNELS,), 1.0, 4.0, (), jnp.float32)
    glu_weight = centred(splits[9], (CHANNELS, CHANNELS), CHANNELS ** -0.5, 0.1875)
    glu_bias = centred(splits[10], (CHANNELS,), 1.0, 4.0, (), jnp.float32)
    out_weight = centred(splits[11], (CHANNELS, D), CHANNELS ** -0.5, 0.1875)
    out_gain = jnp.clip(1.0 + 0.18 * jax.random.normal(splits[12], (D,), jnp.float32), 0.1, 1.9)
    return dict(tokens=tokens, elapsed=elapsed, norm_gain=norm_gain, in_weight=in_weight, state_input=state_input, state_output=state_output, forget_rate=forget_rate, decay_angle=decay_angle, skip_gain=skip_gain, glu_weight=glu_weight, glu_bias=glu_bias, out_weight=out_weight, out_gain=out_gain)


epsilon = 1e-06

def rms_scale(activations, gain_row):
    values = activations.astype(jnp.float32)
    return values * lax.rsqrt(lax.optimization_barrier(jnp.mean(values * values, axis=-1, keepdims=True)) + epsilon) * gain_row

def read_out(state_re, state_im, readout):
    count = state_re.shape[0]
    groups, group_width, states = (readout.shape[1], readout.shape[2], readout.shape[3])
    real_part = jnp.einsum('tgp,ghp->tgh', state_re.reshape(count, groups, states), readout[0], precision=lax.Precision.HIGHEST)
    imag_part = jnp.einsum('tgp,ghp->tgh', state_im.reshape(count, groups, states), readout[1], precision=lax.Precision.HIGHEST)
    return (real_part - imag_part).reshape(count, groups * group_width)

def direction_pass(driven, elapsed, inputs, readout, rate, angle, backward):
    cell_count = rate.shape[0]

    def block_step(state, piece):
        block_rows, block_steps = piece
        grouped = block_rows.astype(jnp.float32).reshape(TOK_DEV, GROUPS, WIDTH)
        proj_re = jnp.einsum('tgh,gph->tgp', grouped, inputs[0]).reshape(TOK_DEV, cell_count)
        proj_im = jnp.einsum('tgh,gph->tgp', grouped, inputs[1]).reshape(TOK_DEV, cell_count)
        steps_col = block_steps[:, None]
        damping = jnp.sqrt(-jnp.expm1(-2.0 * rate * steps_col))
        fade = jnp.exp(-rate * steps_col)
        angles = angle * steps_col
        decay_re = fade * jnp.cos(angles)
        decay_im = fade * jnp.sin(angles)

        def token_step(carry, item):
            old_re, old_im = carry
            step_re, step_im, push_re, push_im = item
            new_re = step_re * old_re - step_im * old_im + push_re
            new_im = step_re * old_im + step_im * old_re + push_im
            return ((new_re, new_im), (new_re, new_im))
        state, outputs = lax.scan(token_step, state, (decay_re, decay_im, proj_re * damping, proj_im * damping), reverse=backward)
        return (state, read_out(outputs[0], outputs[1], readout))
    start = (jnp.zeros((cell_count,), jnp.float32), jnp.zeros((cell_count,), jnp.float32))
    _, result = lax.scan(block_step, start, (driven, elapsed), reverse=backward)
    return result

def reference(tokens, elapsed, norm_gain, in_weight, state_input, state_output, forget_rate, decay_angle, skip_gain, glu_weight, glu_bias, out_weight, out_gain):
    normed = rms_scale(tokens, norm_gain).astype(jnp.bfloat16)
    driven = jnp.dot(normed, in_weight, preferred_element_type=jnp.float32).astype(jnp.bfloat16)
    response = skip_gain * driven.astype(jnp.float32)
    block_count = SEQ // TOK_DEV
    for direction in range(2):
        part_out = direction_pass(driven.reshape(block_count, TOK_DEV, CHANNELS), elapsed.reshape(block_count, TOK_DEV), state_input[direction].astype(jnp.float32), state_output[direction], forget_rate[direction].reshape(-1), decay_angle[direction].reshape(-1), direction == 1)
        response = response + part_out.reshape(SEQ, CHANNELS)
    active = jax.nn.gelu(response)
    gate_pre = jnp.dot(active.astype(jnp.bfloat16), glu_weight, preferred_element_type=jnp.float32) + glu_bias
    gated = (active * jax.nn.sigmoid(gate_pre)).astype(jnp.bfloat16)
    projected = jnp.dot(gated, out_weight, preferred_element_type=jnp.float32)
    return rms_scale(projected, out_gain).astype(jnp.bfloat16)
```

```python
import functools
import math

import jax
import jax.numpy as jnp
from jax import lax
from jax.experimental import pallas as pl
from jax.experimental.pallas import tpu as pltpu
from jax.sharding import PartitionSpec as P

ROWS = 128
D = 2048
CHANNELS = 1024
DEVICES = 128
TILES = 8
SPAN = 16
SPANS = ROWS // SPAN
HALF_TILES = 4
EPSILON = 1e-06
AXES = ("sp", "tp")
VMEM = pltpu.VMEM
HIGHEST = lax.Precision.HIGHEST
F32 = jnp.float32
BF16 = jnp.bfloat16

SINE = (4.44288291, -7.30824512, 3.60634303, -0.84604096, 0.10968436)
COSINE = (1.4142135, -6.97885097, 5.73946067, -1.88355924, 0.31068962)
DAMP = (
    9.99999626e-01,
    -2.49992247e-01,
    5.20558088e-02,
    -7.77389543e-03,
    8.29541685e-04,
    -6.19250366e-05,
    2.98283721e-06,
    -7.10025954e-08,
)
SINE_SHORT = (4.44287876, -7.30776104, 3.5971931, -0.7896682)


def horner(coefficients, x):
    value = coefficients[-1] * x + coefficients[-2]
    for c in coefficients[-3::-1]:
        value = value * x + c
    return value


def unit_circle(turns, sine=SINE_SHORT):
    r = turns - jnp.round(turns)
    z = r * r
    s = r * horner(sine, z)
    c = horner(COSINE, z)
    return 1.0 - s * s, s * c


def nt(a, b):
    return lax.dot_general(a, b, (((1,), (1,)), ((), ())), preferred_element_type=F32)


def mm(a, b):
    return jnp.dot(a, b, preferred_element_type=F32)


def iotas(shape):
    return lax.broadcasted_iota(jnp.int32, shape, 0), lax.broadcasted_iota(jnp.int32, shape, 1)


def column_of(row):
    return jnp.broadcast_to(row, (ROWS, ROWS)).T


def exact_mm(a, b):
    return jnp.dot(a, b, preferred_element_type=F32, precision=HIGHEST)


def end_kernel(
    tokens, elapsed, gain, weight, inputs, turns, rates, rates2, root2,
    driven_ref, ends_ref, total_ref, bt_ref, normed, times,
):
    step = pl.program_id(0)

    @pl.when(step == 0)
    def _():
        x = tokens[...].astype(F32)
        scale = lax.rsqrt(jnp.mean(x * x, axis=-1, keepdims=True) + EPSILON)
        normed[...] = (x * scale * gain[...]).astype(BF16)
        steps = column_of(elapsed[...])
        row, col = iotas((ROWS, ROWS))
        times[0] = exact_mm((col > row).astype(F32), steps)
        times[1] = exact_mm((col < row).astype(F32), steps)
        times[2] = jnp.sqrt(steps)
        times[3] = steps
        total_ref[...] = exact_mm(jnp.ones((ROWS, ROWS), F32), steps)

    driven = mm(normed[...], weight[...]).astype(BF16)
    driven_ref[...] = driven
    flipped = driven.astype(F32).T.astype(BF16)
    lane = lax.broadcasted_iota(jnp.int32, (16, 128), 1)
    first = lane < 64
    row, col = iotas((16, 16))
    eye = (row == col).astype(BF16)
    for j in range(4):
        pair = step * 4 + j
        for k in range(2):
            th = turns[k, pl.ds(pair, 1), :]
            fl = rates[k, pl.ds(pair, 1), :]
            f2 = rates2[k, pl.ds(pair, 1), :]
            rt = root2[k, pl.ds(pair, 1), :]
            after = times[k]
            cosine, sine = unit_circle(after * th)
            damp = horner(DAMP, times[3] * f2) * (times[2] * rt)
            amp = jnp.exp2(after * fl) * damp
            pull = jnp.concatenate(
                [(amp * cosine).astype(BF16), (amp * sine).astype(BF16)], axis=1
            )
            mixed = mm(flipped[32 * j : 32 * j + 32], pull)
            m_re = jnp.where(first, mixed[:16, :128], mixed[16:, :128])
            m_im = jnp.where(first, mixed[:16, 128:], mixed[16:, 128:])
            b_re = nt(eye, inputs[k, 0, 2 * j : 2 * j + 2].reshape(128, 16))
            b_im = nt(eye, inputs[k, 1, 2 * j : 2 * j + 2].reshape(128, 16))
            bt_ref[j, k] = jnp.concatenate([b_re.astype(BF16), b_im.astype(BF16)], axis=1)
            x_re = jnp.sum(b_re * m_re - b_im * m_im, axis=0, keepdims=True)
            x_im = jnp.sum(b_re * m_im + b_im * m_re, axis=0, keepdims=True)
            lane1 = first[:1]
            row0 = jnp.where(lane1, x_re, pltpu.roll(x_im, 64, 1))
            row1 = jnp.where(lane1, pltpu.roll(x_re, 64, 1), x_im)
            ends_ref[pl.ds(64 * k + 2 * pair, 1), :] = row0
            ends_ref[pl.ds(64 * k + 2 * pair + 1, 1), :] = row1


def local_kernel(
    offset, elapsed, driven, bt, readout, turns, rates, rates2, root2, skip,
    out_ref, prefix_ref, table_ref, times,
):
    step = pl.program_id(0)

    @pl.when(step == 0)
    def _():
        steps = column_of(elapsed[...])
        row, col = iotas((ROWS, ROWS))
        same = row // SPAN == col // SPAN
        times[0] = exact_mm(((col <= row) & same).astype(F32), steps)
        times[1] = exact_mm(((col >= row) & same).astype(F32), steps)
        times[2] = jnp.sqrt(steps)
        times[3] = steps

    row, col = iotas((ROWS, ROWS))
    same = row // SPAN == col // SPAN
    triangles = (((col <= row) & same).astype(BF16), ((col >= row) & same).astype(BF16))
    lane = lax.broadcasted_iota(jnp.int32, (16, 256), 1) % 128
    zero_bt = jnp.zeros((16, 256), BF16)
    hole = jnp.zeros((16, 64), F32)
    x = driven[...]
    outs = []
    for j in range(4):
        pair = (step + offset) * 4 + j
        lhs = x[:, 32 * j : 32 * j + 32]
        total = None
        for k in range(2):
            th = turns[k, pl.ds(pair, 1), :]
            fl = rates[k, pl.ds(pair, 1), :]
            f2 = rates2[k, pl.ds(pair, 1), :]
            rt = root2[k, pl.ds(pair, 1), :]
            b = bt[j, k].astype(F32)
            rhs = jnp.concatenate(
                [jnp.where(lane < 64, b, 0.0).astype(BF16), jnp.where(lane < 64, 0.0, b).astype(BF16)], axis=0
            )
            proj = mm(lhs, rhs)
            p_re, p_im = proj[:, :128], proj[:, 128:]
            offs = times[k]
            cosine, sine = unit_circle(offs * th)
            damp = horner(DAMP, times[3] * f2) * (times[2] * rt)
            level = offs * fl
            grow = jnp.exp2(-level) * damp
            fade = jnp.exp2(level)
            a_re, a_im = grow * cosine, grow * sine
            lift = jnp.concatenate(
                [(a_re * p_re + a_im * p_im).astype(BF16), (a_re * p_im - a_im * p_re).astype(BF16)], axis=1
            )
            part = mm(triangles[k], lift)
            e_re, e_im = fade * cosine, fade * sine
            c_re = c_im = jnp.zeros((1, 128), F32)
            d_re, d_im = jnp.ones((1, 128), F32), jnp.zeros((1, 128), F32)
            states, prefixes = [None] * SPANS, [None] * SPANS
            for n in range(SPANS) if k == 0 else range(SPANS - 1, -1, -1):
                cut = slice(SPAN * n, SPAN * n + SPAN)
                er, ei = e_re[cut], e_im[cut]
                wr, wi = part[cut, :128] + c_re, part[cut, 128:] + c_im
                sr, si = er * wr - ei * wi, er * wi + ei * wr
                pr, pi = er * d_re - ei * d_im, er * d_im + ei * d_re
                edge = slice(SPAN - 1, SPAN) if k == 0 else slice(0, 1)
                c_re, c_im, d_re, d_im = sr[edge], si[edge], pr[edge], pi[edge]
                states[n] = jnp.concatenate([sr.astype(BF16), si.astype(BF16)], axis=1)
                prefixes[n] = jnp.concatenate([pr.astype(BF16), pi.astype(BF16)], axis=1)
            prefix_ref[j, k] = jnp.concatenate(prefixes, axis=0)
            tables = []
            for c in range(2):
                upper = jnp.concatenate([readout[k, c, 2 * j], hole], axis=1)
                lower = jnp.concatenate([hole, readout[k, c, 2 * j + 1]], axis=1)
                table = jnp.concatenate([upper, lower], axis=0)
                table_ref[j, k, c] = table
                tables.append(table)
            y = nt(
                jnp.concatenate(states, axis=0),
                jnp.concatenate([tables[0].astype(BF16), (-tables[1]).astype(BF16)], axis=1),
            )
            total = y if total is None else total + y
        outs.append(total)
    out_ref[...] = jnp.concatenate(outs, axis=1) + skip[...] * x.astype(F32)


def device_kernel(backward, ends, turns_hi, turns_lo, rate, out_ref, work):
    span = ends[:, 128:]
    u = span * turns_hi[...]
    r = (u - jnp.round(u)) + span * turns_lo[...]
    cosine, sine = unit_circle(r, SINE)
    fade = jnp.exp2(span * rate[...])
    work[0] = fade * cosine
    work[1] = fade * sine
    x = ends[:, :128]
    work[2] = x
    work[3] = pltpu.roll(x, 64, 1)
    back = backward[0]
    first = lax.broadcasted_iota(jnp.int32, (1, 128), 1) < 64

    def body(i, carry):
        re, im = carry
        d = jnp.where(back > 0, DEVICES - 1 - i, i)
        out_ref[pl.ds(d, 1), :] = jnp.where(first, re, pltpu.roll(im, 64, 1))
        ar, ai = work[0, pl.ds(d, 1), :], work[1, pl.ds(d, 1), :]
        xr, xi = work[2, pl.ds(d, 1), :], work[3, pl.ds(d, 1), :]
        return ar * re - ai * im + xr, ar * im + ai * re + xi

    zero = jnp.zeros((1, 128), F32)
    lax.fori_loop(0, DEVICES, body, (zero, zero), unroll=8)


def final_kernel(
    entering, near_a, near_b, prefix_a, prefix_b, table_a, table_b, glu, glu_bias, outw, out_gain,
    out_ref, prefix, glu_v, outw_v, response, sems,
):
    copies = [
        pltpu.make_async_copy(prefix_a, prefix.at[pl.ds(0, 16)], sems.at[0]),
        pltpu.make_async_copy(prefix_b, prefix.at[pl.ds(16, 16)], sems.at[1]),
        pltpu.make_async_copy(glu, glu_v, sems.at[2]),
        pltpu.make_async_copy(outw, outw_v, sems.at[3]),
    ]
    for copy in copies:
        copy.start()
    for half, (near, table) in enumerate(((near_a, table_a), (near_b, table_b))):
        copies[half].wait()

        def tile(i, _, half=half, near=near, table=table):
            outs = []
            for j in range(4):
                total = None
                for k in range(2):
                    at = 64 * k + 32 * half + 8 * i + 2 * j
                    e0, e1 = entering[pl.ds(at, 1), :], entering[pl.ds(at + 1, 1), :]
                    er = jnp.concatenate([e0[:, :64], e1[:, :64]], axis=1)
                    ei = jnp.concatenate([e0[:, 64:], e1[:, 64:]], axis=1)
                    cr, ci = table[4 * i + j, k, 0], table[4 * i + j, k, 1]
                    rhs = jnp.concatenate(
                        [(cr * er - ci * ei).astype(BF16), (-(cr * ei + ci * er)).astype(BF16)], axis=1
                    )
                    y = nt(prefix[16 * half + 4 * i + j, k], rhs)
                    total = y if total is None else total + y
                outs.append(total)
            at = pl.multiple_of(128 * i, 128)
            response[:, pl.ds(at + 512 * half, 128)] = jnp.concatenate(outs, axis=1) + near[:, pl.ds(at, 128)]
            return 0

        lax.fori_loop(0, HALF_TILES, tile, 0)
    x = response[...]
    active = 0.5 * x * (1.0 + jnp.tanh(math.sqrt(2.0 / math.pi) * (x + 0.044715 * (x * x * x))))
    copies[2].wait()
    gate = mm(active.astype(BF16), glu_v[...]) + glu_bias[...]
    gated = (active * jax.nn.sigmoid(gate)).astype(BF16)
    copies[3].wait()
    projected = mm(gated, outw_v[...])
    scale = lax.rsqrt(jnp.mean(projected * projected, axis=-1, keepdims=True) + EPSILON)
    out_ref[...] = (projected * scale * out_gain[...]).astype(BF16)


def whole(shape):
    return pl.BlockSpec(shape, lambda *_: (0,) * len(shape))


def sds(shape, dtype=F32):
    return jax.ShapeDtypeStruct(shape, dtype)


def params(limit=40):
    return pltpu.CompilerParams(vmem_limit_bytes=limit * 1024 * 1024)


def run_local(half, elapsed_row, driven, bt, state_output, rows, skip_row):
    row_spec = whole((2, 32, 128))
    return pl.pallas_call(
        functools.partial(local_kernel, half * HALF_TILES),
        name=f"local_{half}",
        grid=(HALF_TILES,),
        in_specs=[
            whole((1, ROWS)),
            pl.BlockSpec((ROWS, 128), lambda i: (0, i + half * HALF_TILES)),
            pl.BlockSpec((4, 2, 16, 256), lambda i: (i + half * HALF_TILES, 0, 0, 0)),
            pl.BlockSpec((2, 2, 8, 16, 64), lambda i: (0, 0, i + half * HALF_TILES, 0, 0)),
            row_spec, row_spec, row_spec, row_spec,
            pl.BlockSpec((1, 128), lambda i: (0, i + half * HALF_TILES)),
        ],
        out_specs=[
            pl.BlockSpec((ROWS, 128), lambda i: (0, i)),
            pl.BlockSpec((4, 2, ROWS, 256), lambda i: (i, 0, 0, 0)),
            pl.BlockSpec((4, 2, 2, 32, 128), lambda i: (i, 0, 0, 0, 0)),
        ],
        out_shape=[
            sds((ROWS, 512)),
            sds((16, 2, ROWS, 256), BF16),
            sds((16, 2, 2, 32, 128)),
        ],
        scratch_shapes=[VMEM((4, ROWS, ROWS), F32)],
        compiler_params=params(),
        cost_estimate=pl.CostEstimate(flops=2 * 10**9, bytes_accessed=8 * 2**20, transcendentals=0),
    )(elapsed_row, driven, bt, state_output, *rows, skip_row)


def local(
    tokens, elapsed, norm_gain, in_weight, state_input, state_output, forget_rate, decay_angle,
    skip_gain, glu_weight, glu_bias, out_weight, out_gain,
):
    elapsed_row = elapsed.reshape(1, ROWS)
    rate = forget_rate.reshape(2, 32, 128)
    angle = decay_angle.reshape(2, 32, 128)
    rows = (
        angle * (0.5 / math.pi),
        rate * (-1.0 / math.log(2.0)),
        rate * 2.0,
        jnp.sqrt(rate * 2.0),
    )
    row_spec = whole((2, 32, 128))
    driven, ends, total, bt = pl.pallas_call(
        end_kernel,
        name="ends",
        grid=(TILES,),
        in_specs=[
            whole((ROWS, D)),
            whole((1, ROWS)),
            whole((1, D)),
            pl.BlockSpec((D, 128), lambda i: (0, i)),
            pl.BlockSpec((2, 2, 8, 64, 16), lambda i: (0, 0, i, 0, 0)),
            row_spec, row_spec, row_spec, row_spec,
        ],
        out_specs=[
            pl.BlockSpec((ROWS, 128), lambda i: (0, i)),
            whole((ROWS, 128)),
            whole((ROWS, 128)),
            pl.BlockSpec((4, 2, 16, 256), lambda i: (i, 0, 0, 0)),
        ],
        out_shape=[
            sds((ROWS, CHANNELS), BF16),
            sds((DEVICES, 128)),
            sds((DEVICES, 128)),
            sds((32, 2, 16, 256), BF16),
        ],
        scratch_shapes=[VMEM((ROWS, D), BF16), VMEM((4, ROWS, ROWS), F32)],
        compiler_params=params(),
    )(tokens, elapsed_row, norm_gain.reshape(1, D), in_weight, state_input, *rows)

    me = lax.axis_index(AXES)
    flat_angle = lax.dynamic_slice(decay_angle.reshape(128, 64), (me, 0), (1, 64))
    flat_rate = lax.dynamic_slice(forget_rate.reshape(128, 64), (me, 0), (1, 64))
    mine = jnp.concatenate([flat_angle, flat_angle], axis=1)
    mine_rate = jnp.concatenate([flat_rate, flat_rate], axis=1) * (-1.0 / math.log(2.0))
    high = jnp.round(mine * (4096 * 0.5 / math.pi)) * (1.0 / 4096)
    coarse = 6433 / 1024
    low = ((mine - high * coarse) - high * (2 * math.pi - coarse)) * (0.5 / math.pi)
    backward = (me >= 64).astype(jnp.int32).reshape(1)

    seen = lax.all_to_all(jnp.concatenate([ends, total], axis=1), AXES, 0, 0, tiled=True)
    skip_row = skip_gain.reshape(1, CHANNELS)
    near_a, prefix_a, table_a = run_local(0, elapsed_row, driven, bt, state_output, rows, skip_row)
    carried = pl.pallas_call(
        device_kernel,
        name="across",
        in_specs=[pl.BlockSpec(memory_space=pltpu.SMEM)] + [pl.BlockSpec(memory_space=VMEM)] * 4,
        out_shape=sds((DEVICES, 128)),
        scratch_shapes=[VMEM((4, DEVICES, 128), F32)],
        compiler_params=params(8),
    )(backward, seen, high, low, mine_rate)
    entering = lax.all_to_all(carried, AXES, 0, 0, tiled=True)
    near_b, prefix_b, table_b = run_local(1, elapsed_row, driven, bt, state_output, rows, skip_row)

    any_spec = pl.BlockSpec(memory_space=pl.ANY)
    vmem_spec = pl.BlockSpec(memory_space=VMEM)
    return pl.pallas_call(
        final_kernel,
        name="final",
        in_specs=[
            vmem_spec, vmem_spec, vmem_spec, any_spec, any_spec, vmem_spec, vmem_spec,
            any_spec, vmem_spec, any_spec, vmem_spec,
        ],
        out_specs=vmem_spec,
        out_shape=sds((ROWS, D), BF16),
        scratch_shapes=[
            VMEM((32, 2, ROWS, 256), BF16),
            VMEM((CHANNELS, CHANNELS), BF16),
            VMEM((CHANNELS, D), BF16),
            VMEM((ROWS, CHANNELS), F32),
            pltpu.SemaphoreType.DMA((4,)),
        ],
        compiler_params=params(),
    )(
        entering, near_a, near_b, prefix_a, prefix_b, table_a, table_b,
        glu_weight, glu_bias.reshape(1, CHANNELS), out_weight, out_gain.reshape(1, D),
    )


def solution(mesh):
    split = P(AXES, None)
    placed = (split, P(AXES), P(), P(), P(), P(), P(), P(), P(), P(), P(), P(), P())
    return jax.shard_map(local, mesh=mesh, in_specs=placed, out_specs=split, check_vma=False)
```

```python
import functools
import math

import jax
import jax.numpy as jnp
from jax import lax
from jax.experimental import pallas as pl
from jax.experimental.pallas import tpu as pltpu
from jax.sharding import Mesh
from jax.sharding import PartitionSpec as P

ROWS = 128
D = 2048
CHANNELS = 1024
TILES = 8
SPAN = 16
SPANS = ROWS // SPAN
PIECES = (1, 2, 4, 1)
LOG2E = 1.0 / math.log(2.0)
EPSILON = 1e-06
AXES = ("sp", "y", "c")
VMEM = pltpu.VMEM
HIGHEST = lax.Precision.HIGHEST
F32 = jnp.float32
BF16 = jnp.bfloat16

SINE = (4.44288291, -7.30824512, 3.60634303, -0.84604096, 0.10968436)
COSINE = (1.4142135, -6.97885097, 5.73946067, -1.88355924, 0.31068962)
DAMP = (
    9.99999626e-01,
    -2.49992247e-01,
    5.20558088e-02,
    -7.77389543e-03,
    8.29541685e-04,
    -6.19250366e-05,
    2.98283721e-06,
    -7.10025954e-08,
)
SINE_SHORT = (4.44287876, -7.30776104, 3.5971931, -0.7896682)


def horner(coefficients, x):
    value = coefficients[-1] * x + coefficients[-2]
    for c in coefficients[-3::-1]:
        value = value * x + c
    return value


def unit_circle(turns, sine=SINE_SHORT):
    r = turns - jnp.round(turns)
    z = r * r
    s = r * horner(sine, z)
    c = horner(COSINE, z)
    return 1.0 - s * s, s * c


def nt(a, b):
    return lax.dot_general(a, b, (((1,), (1,)), ((), ())), preferred_element_type=F32)


def mm(a, b):
    return jnp.dot(a, b, preferred_element_type=F32)


def iotas(shape):
    return lax.broadcasted_iota(jnp.int32, shape, 0), lax.broadcasted_iota(jnp.int32, shape, 1)


def column_of(row):
    return jnp.broadcast_to(row, (ROWS, ROWS)).T


def exact_mm(a, b):
    return jnp.dot(a, b, preferred_element_type=F32, precision=HIGHEST)


def pair_row(ref, k, pair):
    return jnp.concatenate([ref[k, pl.ds(2 * pair, 1), :], ref[k, pl.ds(2 * pair + 1, 1), :]], axis=1)


def end_kernel(tokens, elapsed, gain, weight, inputs, angle, rate, driven_ref, ends_ref, pars_ref, normed, times):
    step = pl.program_id(0)
    core = lax.axis_index("c")

    @pl.when(step == 0)
    def _():
        x = tokens[...].astype(F32)
        scale = lax.rsqrt(jnp.mean(x * x, axis=-1, keepdims=True) + EPSILON)
        normed[...] = (x * scale * gain[...]).astype(BF16)
        steps = column_of(elapsed[...])
        row, col = iotas((ROWS, ROWS))
        times[0] = exact_mm((col > row).astype(F32), steps)
        times[1] = exact_mm((col < row).astype(F32), steps)
        times[2] = jnp.sqrt(steps)
        times[3] = steps
        total = exact_mm(jnp.ones((16, ROWS), F32), steps)
        ends_ref[0, 4] = total
        ends_ref[1, 4] = total

    driven = mm(normed[...], weight[...]).astype(BF16)
    driven_ref[...] = driven
    flipped = driven.astype(F32).T.astype(BF16)
    first = lax.broadcasted_iota(jnp.int32, (16, 128), 1) < 64
    away = jnp.where((step // 4) == core, 0, 1)
    for j in range(4):
        pair = step * 4 + j
        for k in range(2):
            f = pair_row(rate, k, pair)
            th = pair_row(angle, k, pair)
            pars_ref[k, 0, pl.ds(pair, 1), :] = th
            pars_ref[k, 1, pl.ds(pair, 1), :] = f
            f2 = f * 2.0
            after = times[k]
            cosine, sine = unit_circle(after * (th * (0.5 / math.pi)))
            damp = horner(DAMP, times[3] * f2) * (times[2] * jnp.sqrt(f2))
            amp = jnp.exp2(after * (f * -LOG2E)) * damp
            pull = jnp.concatenate([(amp * cosine).astype(BF16), (amp * sine).astype(BF16)], axis=1)
            mixed = mm(flipped[32 * j : 32 * j + 32], pull)
            m_re = jnp.where(first, mixed[:16, :128], mixed[16:, :128])
            m_im = jnp.where(first, mixed[:16, 128:], mixed[16:, 128:])
            b_re, b_im = (
                jnp.concatenate([inputs[k, c, 2 * j].astype(F32), inputs[k, c, 2 * j + 1].astype(F32)], axis=1)
                for c in range(2)
            )
            at = 4 * (step % 4) + j
            ends_ref[away, 2 * k, pl.ds(at, 1), :] = jnp.sum(b_re * m_re - b_im * m_im, axis=0, keepdims=True)
            ends_ref[away, 2 * k + 1, pl.ds(at, 1), :] = jnp.sum(b_re * m_im + b_im * m_re, axis=0, keepdims=True)


def local_kernel(
    offset, elapsed, driven, inputs, readout, angle, rate, skip,
    out_ref, prefix_ref, table_ref, times,
):
    step = pl.program_id(0)

    @pl.when(step == 0)
    def _():
        steps = column_of(elapsed[...])
        row, col = iotas((ROWS, ROWS))
        same = row // SPAN == col // SPAN
        times[0] = exact_mm(((col <= row) & same).astype(F32), steps)
        times[1] = exact_mm(((col >= row) & same).astype(F32), steps)
        times[2] = jnp.sqrt(steps)
        times[3] = steps

    row, col = iotas((ROWS, ROWS))
    same = row // SPAN == col // SPAN
    triangles = (((col <= row) & same).astype(BF16), ((col >= row) & same).astype(BF16))
    empty = jnp.zeros((16, 64), BF16)
    hole = jnp.zeros((16, 64), F32)
    x = driven[...]
    outs = []
    for j in range(4):
        pair = (step + offset) * 4 + j
        lhs = x[:, 32 * j : 32 * j + 32]
        total = None
        for k in range(2):
            f = pair_row(rate, k, pair)
            th = pair_row(angle, k, pair)
            f2 = f * 2.0
            b00, b01 = inputs[k, 0, 2 * j], inputs[k, 1, 2 * j]
            b10, b11 = inputs[k, 0, 2 * j + 1], inputs[k, 1, 2 * j + 1]
            rhs = jnp.concatenate(
                [
                    jnp.concatenate([b00, empty, b01, empty], axis=1),
                    jnp.concatenate([empty, b10, empty, b11], axis=1),
                ],
                axis=0,
            )
            proj = mm(lhs, rhs)
            p_re, p_im = proj[:, :128], proj[:, 128:]
            offs = times[k]
            cosine, sine = unit_circle(offs * (th * (0.5 / math.pi)))
            damp = horner(DAMP, times[3] * f2) * (times[2] * jnp.sqrt(f2))
            level = offs * (f * LOG2E)
            grow = jnp.exp2(level) * damp
            fade = jnp.exp2(-level)
            a_re, a_im = grow * cosine, grow * sine
            lift = jnp.concatenate(
                [(a_re * p_re + a_im * p_im).astype(BF16), (a_re * p_im - a_im * p_re).astype(BF16)], axis=1
            )
            part = mm(triangles[k], lift)
            e_re, e_im = fade * cosine, fade * sine
            c_re = c_im = jnp.zeros((1, 128), F32)
            d_re, d_im = jnp.ones((1, 128), F32), jnp.zeros((1, 128), F32)
            states, prefixes = [None] * SPANS, [None] * SPANS
            for n in range(SPANS) if k == 0 else range(SPANS - 1, -1, -1):
                cut = slice(SPAN * n, SPAN * n + SPAN)
                er, ei = e_re[cut], e_im[cut]
                wr, wi = part[cut, :128] + c_re, part[cut, 128:] + c_im
                sr, si = er * wr - ei * wi, er * wi + ei * wr
                pr, pi = er * d_re - ei * d_im, er * d_im + ei * d_re
                edge = slice(SPAN - 1, SPAN) if k == 0 else slice(0, 1)
                c_re, c_im, d_re, d_im = sr[edge], si[edge], pr[edge], pi[edge]
                states[n] = jnp.concatenate([sr.astype(BF16), si.astype(BF16)], axis=1)
                prefixes[n] = jnp.concatenate([pr.astype(BF16), pi.astype(BF16)], axis=1)
            prefix_ref[j, k] = jnp.concatenate(prefixes, axis=0)
            tables = []
            for c in range(2):
                upper = jnp.concatenate([readout[k, c, 2 * j], hole], axis=1)
                lower = jnp.concatenate([hole, readout[k, c, 2 * j + 1]], axis=1)
                table = jnp.concatenate([upper, lower], axis=0)
                table_ref[j, k, c] = table
                tables.append(table)
            y = nt(
                jnp.concatenate(states, axis=0),
                jnp.concatenate([tables[0].astype(BF16), (-tables[1]).astype(BF16)], axis=1),
            )
            total = y if total is None else total + y
        outs.append(total)
    out_ref[...] = jnp.concatenate(outs, axis=1) + skip[...] * x.astype(F32)


def times_of(a, b):
    return a[0] * b[0] - a[1] * b[1], a[0] * b[1] + a[1] * b[0]


def plus(a, b):
    return a[0] + b[0], a[1] + b[1]


def pick(condition, a, b):
    return tuple(jnp.where(condition, x, y) for x, y in zip(a, b))


def my_pars(pars):
    core = lax.axis_index("c")
    found = []
    for k in range(2):
        angle = pars[k, 0, pl.ds(16 * core, 16), :]
        rate = pars[k, 1, pl.ds(16 * core, 16), :]
        high = jnp.round(angle * (4096 * 0.5 / math.pi)) * (1.0 / 4096)
        coarse = 6433 / 1024
        low = ((angle - high * coarse) - high * (2 * math.pi - coarse)) * (0.5 / math.pi)
        found.append((high, low, rate * -LOG2E))
    return found


def decay_over(span, pars):
    high, low, level = pars
    u = span * high
    cosine, sine = unit_circle((u - jnp.round(u)) + span * low, SINE)
    fade = jnp.exp2(span * level)
    return fade * cosine, fade * sine


def states_of(ref, k):
    return ref[2 * k], ref[2 * k + 1]


def pair_kernel(own, other, pars, out_ref):
    core = lax.axis_index("c")
    mine = my_pars(pars)
    span, span_other = own[4], other[4]
    for k in range(2):
        ahead = core == k
        a, b = states_of(own, k), states_of(other, k)
        early, late = pick(ahead, a, b), pick(ahead, b, a)
        moved = times_of(decay_over(jnp.where(ahead, span_other, span), mine[k]), early)
        total = plus(moved, late)
        out_ref[2 * k], out_ref[2 * k + 1] = total
    out_ref[4] = span + span_other


def group_kernel(own, one, two, three, pars, send_ref, before_ref, data):
    y = lax.axis_index("y")
    here = lax.axis_index("sp")
    mine = my_pars(pars)
    data[y] = own[...]
    data[(y + 3) % 4] = one[...]
    data[(y + 2) % 4] = two[...]
    data[(y + 1) % 4] = three[...]
    zero = jnp.zeros((16, 128), F32)
    totals = []
    for k in range(2):
        state, decay = (zero, zero), (zero + 1.0, zero)
        before, before_decay = state, decay
        for n in range(4) if k == 0 else range(3, -1, -1):
            before = pick(n == y, state, before)
            before_decay = pick(n == y, decay, before_decay)
            step = decay_over(data[n, 4], mine[k])
            state = plus(times_of(step, state), (data[n, 2 * k], data[n, 2 * k + 1]))
            decay = times_of(step, decay)
        before_ref[2 * k], before_ref[2 * k + 1] = before
        before_ref[4 + 2 * k], before_ref[5 + 2 * k] = before_decay
        totals.append(state)
    span = data[0, 4] + data[1, 4] + data[2, 4] + data[3, 4]
    for n in range(16):
        sent = pick(n > here, totals[0], totals[1])
        send_ref[n, 0], send_ref[n, 1] = sent
        send_ref[n, 2] = span


def enter_kernel(seen, before, own, other, pars, mine_ref, theirs_ref):
    here = lax.axis_index("sp")
    core = lax.axis_index("c")
    mine = my_pars(pars)
    zero = jnp.zeros((16, 128), F32)
    steps = []
    for n in range(16):
        chosen = pick(n < here, mine[0], mine[1])
        steps.append(decay_over(seen[n, 2], chosen))
    for k in range(2):
        state = (zero, zero)
        for n in range(16) if k == 0 else range(15, -1, -1):
            active = n < here if k == 0 else n > here
            new = plus(times_of(steps[n], state), (seen[n, 0], seen[n, 1]))
            state = pick(active, new, state)
        state = plus(times_of((before[4 + 2 * k], before[5 + 2 * k]), state), states_of(before, k))
        ahead = core == k
        a, b = states_of(own, k), states_of(other, k)
        early = pick(ahead, a, b)
        later = plus(times_of(decay_over(jnp.where(ahead, own[4], other[4]), mine[k]), state), early)
        mine_ref[2 * k], mine_ref[2 * k + 1] = pick(ahead, state, later)
        theirs_ref[2 * k], theirs_ref[2 * k + 1] = pick(ahead, later, state)


def final_kernel(*refs):
    count = len(PIECES)
    own, other = refs[:2]
    nears, prefixes, tables = (refs[2 + count * n : 2 + count * n + count] for n in range(3))
    glu, glu_bias, outw, out_gain, out_ref, entering, response = refs[2 + 3 * count :]
    core = lax.axis_index("c")
    entering[core] = own[...]
    entering[1 - core] = other[...]
    start = 0
    for size, near, prefix, table in zip(PIECES, nears, prefixes, tables):

        def tile(i, _, start=start, near=near, prefix=prefix, table=table):
            outs = []
            for j in range(4):
                total = None
                for k in range(2):
                    pair = 4 * (start + i) + j
                    er = entering[pair // 16, 2 * k, pl.ds(pair % 16, 1), :]
                    ei = entering[pair // 16, 2 * k + 1, pl.ds(pair % 16, 1), :]
                    cr, ci = table[4 * i + j, k, 0], table[4 * i + j, k, 1]
                    rhs = jnp.concatenate(
                        [(cr * er - ci * ei).astype(BF16), (-(cr * ei + ci * er)).astype(BF16)], axis=1
                    )
                    y = nt(prefix[4 * i + j, k], rhs)
                    total = y if total is None else total + y
                outs.append(total)
            at = pl.multiple_of(128 * i, 128)
            response[:, pl.ds(at + 128 * start, 128)] = jnp.concatenate(outs, axis=1) + near[:, pl.ds(at, 128)]
            return 0

        lax.fori_loop(0, size, tile, 0)
        start += size
    x = response[...]
    active = 0.5 * x * (1.0 + jnp.tanh(math.sqrt(2.0 / math.pi) * (x + 0.044715 * (x * x * x))))
    gate = mm(active.astype(BF16), glu[...]) + glu_bias[...]
    gated = (active * jax.nn.sigmoid(gate)).astype(BF16)
    projected = mm(gated, outw[...])
    scale = lax.rsqrt(jnp.mean(projected * projected, axis=-1, keepdims=True) + EPSILON)
    out_ref[...] = (projected * scale * out_gain[...]).astype(BF16)


def whole(shape):
    return pl.BlockSpec(shape, lambda *_: (0,) * len(shape))


def sds(shape, dtype=F32):
    return jax.ShapeDtypeStruct(shape, dtype)


def params(limit):
    return pltpu.CompilerParams(vmem_limit_bytes=limit * 1024 * 1024)


def run_local(start, size, elapsed_row, driven, inputs, state_output, angle, rate, skip_row):
    row_spec = whole((2, 64, 64))
    return pl.pallas_call(
        functools.partial(local_kernel, start),
        name=f"local_{start}",
        grid=(size,),
        in_specs=[
            whole((1, ROWS)),
            pl.BlockSpec((ROWS, 128), lambda i: (0, i + start)),
            pl.BlockSpec((2, 2, 8, 16, 64), lambda i: (0, 0, i + start, 0, 0)),
            pl.BlockSpec((2, 2, 8, 16, 64), lambda i: (0, 0, i + start, 0, 0)),
            row_spec, row_spec,
            pl.BlockSpec((1, 128), lambda i: (0, i + start)),
        ],
        out_specs=[
            pl.BlockSpec((ROWS, 128), lambda i: (0, i)),
            pl.BlockSpec((4, 2, ROWS, 256), lambda i: (i, 0, 0, 0)),
            pl.BlockSpec((4, 2, 2, 32, 128), lambda i: (i, 0, 0, 0, 0)),
        ],
        out_shape=[
            sds((ROWS, 128 * size)),
            sds((4 * size, 2, ROWS, 256), BF16),
            sds((4 * size, 2, 2, 32, 128)),
        ],
        scratch_shapes=[VMEM((4, ROWS, ROWS), F32)],
        compiler_params=params(10),
        cost_estimate=pl.CostEstimate(flops=size * 5 * 10**8, bytes_accessed=size * 2 * 2**20, transcendentals=0),
    )(elapsed_row, driven, inputs, state_output, angle, rate, skip_row)


def simple(kernel, name, shapes, args, scratch=()):
    spec = pl.BlockSpec(memory_space=VMEM)
    return pl.pallas_call(
        kernel,
        name=name,
        in_specs=[spec] * len(args),
        out_specs=[spec] * len(shapes),
        out_shape=[sds(shape) for shape in shapes],
        scratch_shapes=scratch,
        compiler_params=params(4),
    )(*args)


def local(
    tokens, elapsed, norm_gain, in_weight, state_input, state_output, forget_rate, decay_angle,
    skip_gain, glu_weight, glu_bias, out_weight, out_gain,
):
    elapsed_row = elapsed.reshape(1, ROWS)
    inputs = jnp.swapaxes(state_input, 3, 4)
    row_spec = whole((2, 64, 64))
    driven, ends, pars = pl.pallas_call(
        end_kernel,
        name="ends",
        grid=(TILES,),
        in_specs=[
            whole((ROWS, D)),
            whole((1, ROWS)),
            whole((1, D)),
            pl.BlockSpec((D, 128), lambda i: (0, i)),
            pl.BlockSpec((2, 2, 8, 16, 64), lambda i: (0, 0, i, 0, 0)),
            row_spec, row_spec,
        ],
        out_specs=[
            pl.BlockSpec((ROWS, 128), lambda i: (0, i)),
            whole((2, 5, 16, 128)),
            whole((2, 2, 32, 128)),
        ],
        out_shape=[sds((ROWS, CHANNELS), BF16), sds((2, 5, 16, 128)), sds((2, 2, 32, 128))],
        scratch_shapes=[VMEM((ROWS, D), BF16), VMEM((4, ROWS, ROWS), F32)],
        compiler_params=params(10),
    )(
        tokens, elapsed_row, norm_gain.reshape(1, D), hbm(in_weight), hbm(inputs), decay_angle, forget_rate
    )

    skip_row = skip_gain.reshape(1, CHANNELS)
    pieces, start = [], 0
    for size in PIECES:
        pieces.append(
            run_local(
                start, size, elapsed_row, driven, inputs, state_output, decay_angle, forget_rate, skip_row
            )
        )
        start += size

    swap = [(0, 1), (1, 0)]
    keep = ends[0]
    partner = lax.ppermute(ends[1], "c", swap)
    (pair,) = simple(pair_kernel, "pair", [(5, 16, 128)], (keep, partner, pars))
    shifted = [lax.ppermute(pair, "y", [(i, (i + n) % 4) for i in range(4)]) for n in (2, 1, 3)]
    two, one, three = shifted
    send, before = simple(
        group_kernel, "group", [(16, 3, 16, 128), (8, 16, 128)], (pair, one, two, three, pars),
        [VMEM((4, 5, 16, 128), F32)],
    )
    seen = lax.all_to_all(send, "sp", 0, 0, tiled=True)
    mine, theirs = simple(
        enter_kernel, "enter", [(4, 16, 128), (4, 16, 128)], (seen, before, keep, partner, pars)
    )
    other = lax.ppermute(theirs, "c", swap)

    spec = pl.BlockSpec(memory_space=VMEM)
    args = (
        mine, other, *(p[0] for p in pieces), *(p[1] for p in pieces), *(p[2] for p in pieces),
        glu_weight, glu_bias.reshape(1, CHANNELS), out_weight, out_gain.reshape(1, D),
    )
    return pl.pallas_call(
        final_kernel,
        name="final",
        in_specs=[spec] * len(args),
        out_specs=spec,
        out_shape=sds((ROWS, D), BF16),
        scratch_shapes=[VMEM((2, 4, 16, 128), F32), VMEM((ROWS, CHANNELS), F32)],
        compiler_params=params(24),
    )(*args)


def hbm(x):
    return pltpu.with_memory_space_constraint(x, pltpu.HBM)


def solution(mesh):
    finer = Mesh(mesh.devices.reshape(16, 4, 2), AXES)
    split = P(AXES, None)
    placed = (split, P(AXES), P(), P(), P(), P(), P(), P(), P(), P(), P(), P(), P())
    return jax.shard_map(local, mesh=finer, in_specs=placed, out_specs=split, check_vma=False)
```

```python
import functools
import math

import jax
import jax.numpy as jnp
from jax import lax
from jax.experimental import pallas as pl
from jax.experimental.pallas import tpu as pltpu
from jax.sharding import Mesh
from jax.sharding import PartitionSpec as P

ROWS = 128
D = 2048
CHANNELS = 1024
TILES = 8
SPAN = 16
SPANS = ROWS // SPAN
PIECES = (1, 2, 2, 2, 1)
LOG2E = 1.0 / math.log(2.0)
EPSILON = 1e-06
AXES = ("z", "x", "y", "c")
VMEM = pltpu.VMEM
HIGHEST = lax.Precision.HIGHEST
F32 = jnp.float32
BF16 = jnp.bfloat16

SINE = (4.44288291, -7.30824512, 3.60634303, -0.84604096, 0.10968436)
COSINE = (1.4142135, -6.97885097, 5.73946067, -1.88355924, 0.31068962)
DAMP = (
    9.99999626e-01,
    -2.49992247e-01,
    5.20558088e-02,
    -7.77389543e-03,
    8.29541685e-04,
    -6.19250366e-05,
    2.98283721e-06,
    -7.10025954e-08,
)
SINE_SHORT = (4.44287876, -7.30776104, 3.5971931, -0.7896682)


def horner(coefficients, x):
    value = coefficients[-1] * x + coefficients[-2]
    for c in coefficients[-3::-1]:
        value = value * x + c
    return value


def unit_circle(turns, sine=SINE_SHORT):
    r = turns - jnp.round(turns)
    z = r * r
    s = r * horner(sine, z)
    c = horner(COSINE, z)
    return 1.0 - s * s, s * c


def nt(a, b):
    return lax.dot_general(a, b, (((1,), (1,)), ((), ())), preferred_element_type=F32)


def mm(a, b):
    return jnp.dot(a, b, preferred_element_type=F32)


def iotas(shape):
    return lax.broadcasted_iota(jnp.int32, shape, 0), lax.broadcasted_iota(jnp.int32, shape, 1)


def column_of(row):
    return jnp.broadcast_to(row, (ROWS, ROWS)).T


def exact_mm(a, b):
    return jnp.dot(a, b, preferred_element_type=F32, precision=HIGHEST)


def pair_row(ref, k, pair):
    return jnp.concatenate([ref[k, pl.ds(2 * pair, 1), :], ref[k, pl.ds(2 * pair + 1, 1), :]], axis=1)


def end_kernel(tokens, elapsed, gain, weight, inputs, angle, rate, driven_ref, ends_ref, pars_ref, normed, times):
    step = pl.program_id(0)
    core = lax.axis_index("c")

    @pl.when(step == 0)
    def _():
        x = tokens[...].astype(F32)
        scale = lax.rsqrt(jnp.mean(x * x, axis=-1, keepdims=True) + EPSILON)
        normed[...] = (x * scale * gain[...]).astype(BF16)
        steps = column_of(elapsed[...])
        row, col = iotas((ROWS, ROWS))
        times[0] = exact_mm((col > row).astype(F32), steps)
        times[1] = exact_mm((col < row).astype(F32), steps)
        times[2] = jnp.sqrt(steps)
        times[3] = steps
        total = exact_mm(jnp.ones((16, ROWS), F32), steps)
        ends_ref[0, 4] = total
        ends_ref[1, 4] = total

    driven = mm(normed[...], weight[...]).astype(BF16)
    driven_ref[...] = driven
    flipped = driven.astype(F32).T.astype(BF16)
    first = lax.broadcasted_iota(jnp.int32, (16, 128), 1) < 64
    away = jnp.where((step // 4) == core, 0, 1)
    for j in range(4):
        pair = step * 4 + j
        for k in range(2):
            f = pair_row(rate, k, pair)
            th = pair_row(angle, k, pair)
            pars_ref[k, 0, pl.ds(pair, 1), :] = th
            pars_ref[k, 1, pl.ds(pair, 1), :] = f
            f2 = f * 2.0
            after = times[k]
            cosine, sine = unit_circle(after * (th * (0.5 / math.pi)))
            damp = horner(DAMP, times[3] * f2) * (times[2] * jnp.sqrt(f2))
            amp = jnp.exp2(after * (f * -LOG2E)) * damp
            pull = jnp.concatenate([(amp * cosine).astype(BF16), (amp * sine).astype(BF16)], axis=1)
            mixed = mm(flipped[32 * j : 32 * j + 32], pull)
            m_re = jnp.where(first, mixed[:16, :128], mixed[16:, :128])
            m_im = jnp.where(first, mixed[:16, 128:], mixed[16:, 128:])
            b_re, b_im = (
                jnp.concatenate([inputs[k, c, 2 * j].astype(F32), inputs[k, c, 2 * j + 1].astype(F32)], axis=1)
                for c in range(2)
            )
            at = 4 * (step % 4) + j
            ends_ref[away, 2 * k, pl.ds(at, 1), :] = jnp.sum(b_re * m_re - b_im * m_im, axis=0, keepdims=True)
            ends_ref[away, 2 * k + 1, pl.ds(at, 1), :] = jnp.sum(b_re * m_im + b_im * m_re, axis=0, keepdims=True)


def local_kernel(
    offset, elapsed, driven, inputs, readout, angle, rate, skip,
    out_ref, prefix_ref, table_ref, times,
):
    step = pl.program_id(0)

    @pl.when(step == 0)
    def _():
        steps = column_of(elapsed[...])
        row, col = iotas((ROWS, ROWS))
        same = row // SPAN == col // SPAN
        times[0] = exact_mm(((col <= row) & same).astype(F32), steps)
        times[1] = exact_mm(((col >= row) & same).astype(F32), steps)
        times[2] = jnp.sqrt(steps)
        times[3] = steps

    row, col = iotas((ROWS, ROWS))
    same = row // SPAN == col // SPAN
    triangles = (((col <= row) & same).astype(BF16), ((col >= row) & same).astype(BF16))
    empty = jnp.zeros((16, 64), BF16)
    hole = jnp.zeros((16, 64), F32)
    x = driven[...]
    outs = []
    for j in range(4):
        pair = (step + offset) * 4 + j
        lhs = x[:, 32 * j : 32 * j + 32]
        total = None
        for k in range(2):
            f = pair_row(rate, k, pair)
            th = pair_row(angle, k, pair)
            f2 = f * 2.0
            b00, b01 = inputs[k, 0, 2 * j], inputs[k, 1, 2 * j]
            b10, b11 = inputs[k, 0, 2 * j + 1], inputs[k, 1, 2 * j + 1]
            rhs = jnp.concatenate(
                [
                    jnp.concatenate([b00, empty, b01, empty], axis=1),
                    jnp.concatenate([empty, b10, empty, b11], axis=1),
                ],
                axis=0,
            )
            proj = mm(lhs, rhs)
            p_re, p_im = proj[:, :128], proj[:, 128:]
            offs = times[k]
            cosine, sine = unit_circle(offs * (th * (0.5 / math.pi)))
            damp = horner(DAMP, times[3] * f2) * (times[2] * jnp.sqrt(f2))
            level = offs * (f * LOG2E)
            grow = jnp.exp2(level) * damp
            fade = jnp.exp2(-level)
            a_re, a_im = grow * cosine, grow * sine
            lift = jnp.concatenate(
                [(a_re * p_re + a_im * p_im).astype(BF16), (a_re * p_im - a_im * p_re).astype(BF16)], axis=1
            )
            part = mm(triangles[k], lift)
            e_re, e_im = fade * cosine, fade * sine
            c_re = c_im = jnp.zeros((1, 128), F32)
            d_re, d_im = jnp.ones((1, 128), F32), jnp.zeros((1, 128), F32)
            states, prefixes = [None] * SPANS, [None] * SPANS
            for n in range(SPANS) if k == 0 else range(SPANS - 1, -1, -1):
                cut = slice(SPAN * n, SPAN * n + SPAN)
                er, ei = e_re[cut], e_im[cut]
                wr, wi = part[cut, :128] + c_re, part[cut, 128:] + c_im
                sr, si = er * wr - ei * wi, er * wi + ei * wr
                pr, pi = er * d_re - ei * d_im, er * d_im + ei * d_re
                edge = slice(SPAN - 1, SPAN) if k == 0 else slice(0, 1)
                c_re, c_im, d_re, d_im = sr[edge], si[edge], pr[edge], pi[edge]
                states[n] = jnp.concatenate([sr.astype(BF16), si.astype(BF16)], axis=1)
                prefixes[n] = jnp.concatenate([pr.astype(BF16), pi.astype(BF16)], axis=1)
            prefix_ref[j, k] = jnp.concatenate(prefixes, axis=0)
            tables = []
            for c in range(2):
                upper = jnp.concatenate([readout[k, c, 2 * j], hole], axis=1)
                lower = jnp.concatenate([hole, readout[k, c, 2 * j + 1]], axis=1)
                table = jnp.concatenate([upper, lower], axis=0)
                table_ref[j, k, c] = table
                tables.append(table)
            y = nt(
                jnp.concatenate(states, axis=0),
                jnp.concatenate([tables[0].astype(BF16), (-tables[1]).astype(BF16)], axis=1),
            )
            total = y if total is None else total + y
        outs.append(total)
    out_ref[...] = jnp.concatenate(outs, axis=1) + skip[...] * x.astype(F32)


def times_of(a, b):
    return a[0] * b[0] - a[1] * b[1], a[0] * b[1] + a[1] * b[0]


def plus(a, b):
    return a[0] + b[0], a[1] + b[1]


def pick(condition, a, b):
    return tuple(jnp.where(condition, x, y) for x, y in zip(a, b))


def my_pars(pars):
    core = lax.axis_index("c")
    found = []
    for k in range(2):
        angle = pars[k, 0, pl.ds(16 * core, 16), :]
        rate = pars[k, 1, pl.ds(16 * core, 16), :]
        high = jnp.round(angle * (4096 * 0.5 / math.pi)) * (1.0 / 4096)
        coarse = 6433 / 1024
        low = ((angle - high * coarse) - high * (2 * math.pi - coarse)) * (0.5 / math.pi)
        found.append((high, low, rate * -LOG2E))
    return found


def decay_over(span, pars):
    high, low, level = pars
    u = span * high
    cosine, sine = unit_circle((u - jnp.round(u)) + span * low, SINE)
    fade = jnp.exp2(span * level)
    return fade * cosine, fade * sine


def states_of(ref, k):
    return ref[2 * k], ref[2 * k + 1]


def pair_kernel(own, other, pars, out_ref):
    core = lax.axis_index("c")
    mine = my_pars(pars)
    span, span_other = own[4], other[4]
    for k in range(2):
        ahead = core == k
        a, b = states_of(own, k), states_of(other, k)
        early, late = pick(ahead, a, b), pick(ahead, b, a)
        moved = times_of(decay_over(jnp.where(ahead, span_other, span), mine[k]), early)
        total = plus(moved, late)
        out_ref[2 * k], out_ref[2 * k + 1] = total
    out_ref[4] = span + span_other


def gather_four(axis, own, one, two, three, data):
    here = lax.axis_index(axis)
    data[here] = own[...]
    data[(here + 3) % 4] = one[...]
    data[(here + 2) % 4] = two[...]
    data[(here + 1) % 4] = three[...]
    return here


def run_over(here, data, mine, k):
    zero = jnp.zeros((16, 128), F32)
    state, decay = (zero, zero), (zero + 1.0, zero)
    before, before_decay = state, decay
    for n in range(4) if k == 0 else range(3, -1, -1):
        before = pick(n == here, state, before)
        before_decay = pick(n == here, decay, before_decay)
        step = decay_over(data[n, 4], mine[k])
        state = plus(times_of(step, state), (data[n, 2 * k], data[n, 2 * k + 1]))
        decay = times_of(step, decay)
    return state, before, before_decay


def group_kernel(axis, own, one, two, three, pars, total_ref, before_ref, data):
    here = gather_four(axis, own, one, two, three, data)
    mine = my_pars(pars)
    for k in range(2):
        total, before, decay = run_over(here, data, mine, k)
        total_ref[2 * k], total_ref[2 * k + 1] = total
        before_ref[2 * k], before_ref[2 * k + 1] = before
        before_ref[4 + 2 * k], before_ref[5 + 2 * k] = decay
    total_ref[4] = data[0, 4] + data[1, 4] + data[2, 4] + data[3, 4]


def enter_kernel(across, one, two, three, before_x, before_y, own, other, pars, mine_ref, theirs_ref, data):
    here = gather_four("z", across, one, two, three, data)
    core = lax.axis_index("c")
    mine = my_pars(pars)
    for k in range(2):
        _, state, _ = run_over(here, data, mine, k)
        for before in (before_x, before_y):
            state = plus(times_of((before[4 + 2 * k], before[5 + 2 * k]), state), states_of(before, k))
        ahead = core == k
        a, b = states_of(own, k), states_of(other, k)
        early = pick(ahead, a, b)
        later = plus(times_of(decay_over(jnp.where(ahead, own[4], other[4]), mine[k]), state), early)
        mine_ref[2 * k], mine_ref[2 * k + 1] = pick(ahead, state, later)
        theirs_ref[2 * k], theirs_ref[2 * k + 1] = pick(ahead, later, state)


def final_kernel(*refs):
    count = len(PIECES)
    own, other = refs[:2]
    nears, prefixes, tables = (refs[2 + count * n : 2 + count * n + count] for n in range(3))
    glu, glu_bias, outw, out_gain, out_ref, entering, response = refs[2 + 3 * count :]
    core = lax.axis_index("c")
    entering[core] = own[...]
    entering[1 - core] = other[...]
    start = 0
    for size, near, prefix, table in zip(PIECES, nears, prefixes, tables):

        def tile(i, _, start=start, near=near, prefix=prefix, table=table):
            outs = []
            for j in range(4):
                total = None
                for k in range(2):
                    pair = 4 * (start + i) + j
                    er = entering[pair // 16, 2 * k, pl.ds(pair % 16, 1), :]
                    ei = entering[pair // 16, 2 * k + 1, pl.ds(pair % 16, 1), :]
                    cr, ci = table[4 * i + j, k, 0], table[4 * i + j, k, 1]
                    rhs = jnp.concatenate(
                        [(cr * er - ci * ei).astype(BF16), (-(cr * ei + ci * er)).astype(BF16)], axis=1
                    )
                    y = nt(prefix[4 * i + j, k], rhs)
                    total = y if total is None else total + y
                outs.append(total)
            at = pl.multiple_of(128 * i, 128)
            response[:, pl.ds(at + 128 * start, 128)] = jnp.concatenate(outs, axis=1) + near[:, pl.ds(at, 128)]
            return 0

        lax.fori_loop(0, size, tile, 0)
        start += size
    x = response[...]
    active = 0.5 * x * (1.0 + jnp.tanh(math.sqrt(2.0 / math.pi) * (x + 0.044715 * (x * x * x))))
    gate = mm(active.astype(BF16), glu[...]) + glu_bias[...]
    gated = (active * jax.nn.sigmoid(gate)).astype(BF16)
    projected = mm(gated, outw[...])
    scale = lax.rsqrt(jnp.mean(projected * projected, axis=-1, keepdims=True) + EPSILON)
    out_ref[...] = (projected * scale * out_gain[...]).astype(BF16)


def whole(shape):
    return pl.BlockSpec(shape, lambda *_: (0,) * len(shape))


def sds(shape, dtype=F32):
    return jax.ShapeDtypeStruct(shape, dtype)


def params(limit):
    return pltpu.CompilerParams(vmem_limit_bytes=limit * 1024 * 1024)


def run_local(start, size, elapsed_row, driven, inputs, state_output, angle, rate, skip_row):
    row_spec = whole((2, 64, 64))
    return pl.pallas_call(
        functools.partial(local_kernel, start),
        name=f"local_{start}",
        grid=(size,),
        in_specs=[
            whole((1, ROWS)),
            pl.BlockSpec((ROWS, 128), lambda i: (0, i + start)),
            pl.BlockSpec((2, 2, 8, 16, 64), lambda i: (0, 0, i + start, 0, 0)),
            pl.BlockSpec((2, 2, 8, 16, 64), lambda i: (0, 0, i + start, 0, 0)),
            row_spec, row_spec,
            pl.BlockSpec((1, 128), lambda i: (0, i + start)),
        ],
        out_specs=[
            pl.BlockSpec((ROWS, 128), lambda i: (0, i)),
            pl.BlockSpec((4, 2, ROWS, 256), lambda i: (i, 0, 0, 0)),
            pl.BlockSpec((4, 2, 2, 32, 128), lambda i: (i, 0, 0, 0, 0)),
        ],
        out_shape=[
            sds((ROWS, 128 * size)),
            sds((4 * size, 2, ROWS, 256), BF16),
            sds((4 * size, 2, 2, 32, 128)),
        ],
        scratch_shapes=[VMEM((4, ROWS, ROWS), F32)],
        compiler_params=params(10),
        cost_estimate=pl.CostEstimate(flops=size * 5 * 10**8, bytes_accessed=size * 2 * 2**20, transcendentals=0),
    )(elapsed_row, driven, inputs, state_output, angle, rate, skip_row)


def simple(kernel, name, shapes, args, scratch=()):
    spec = pl.BlockSpec(memory_space=VMEM)
    return pl.pallas_call(
        kernel,
        name=name,
        in_specs=[spec] * len(args),
        out_specs=[spec] * len(shapes),
        out_shape=[sds(shape) for shape in shapes],
        scratch_shapes=scratch,
        compiler_params=params(4),
    )(*args)


def local(
    tokens, elapsed, norm_gain, in_weight, state_input, state_output, forget_rate, decay_angle,
    skip_gain, glu_weight, glu_bias, out_weight, out_gain,
):
    elapsed_row = elapsed.reshape(1, ROWS)
    inputs = jnp.swapaxes(state_input, 3, 4)
    row_spec = whole((2, 64, 64))
    driven, ends, pars = pl.pallas_call(
        end_kernel,
        name="ends",
        grid=(TILES,),
        in_specs=[
            whole((ROWS, D)),
            whole((1, ROWS)),
            whole((1, D)),
            pl.BlockSpec((D, 128), lambda i: (0, i)),
            pl.BlockSpec((2, 2, 8, 16, 64), lambda i: (0, 0, i, 0, 0)),
            row_spec, row_spec,
        ],
        out_specs=[
            pl.BlockSpec((ROWS, 128), lambda i: (0, i)),
            whole((2, 5, 16, 128)),
            whole((2, 2, 32, 128)),
        ],
        out_shape=[sds((ROWS, CHANNELS), BF16), sds((2, 5, 16, 128)), sds((2, 2, 32, 128))],
        scratch_shapes=[VMEM((ROWS, D), BF16), VMEM((4, ROWS, ROWS), F32)],
        compiler_params=params(10),
    )(
        *(hbm(a) for a in (tokens, elapsed_row, norm_gain.reshape(1, D), in_weight, inputs, decay_angle, forget_rate))
    )

    skip_row = skip_gain.reshape(1, CHANNELS)
    pieces, start = [], 0

    def piece_between(before, after):
        index = len(pieces)
        start = sum(PIECES[:index])
        driven_now, _ = lax.optimization_barrier((driven, before))
        piece = run_local(
            start, PIECES[index], elapsed_row, driven_now, inputs, state_output, decay_angle, forget_rate, skip_row
        )
        *piece, after = lax.optimization_barrier((*piece, after))
        pieces.append(piece)
        return after

    def around(value, axis):
        return tuple(lax.ppermute(value, axis, [(i, (i + n) % 4) for i in range(4)]) for n in (1, 2, 3))

    swap = [(0, 1), (1, 0)]
    four = VMEM((4, 5, 16, 128), F32)
    keep = ends[0]
    partner = piece_between(keep, lax.ppermute(ends[1], "c", swap))
    (total,) = simple(pair_kernel, "pair", [(5, 16, 128)], (keep, partner, pars))
    befores = []
    for axis in ("y", "x"):
        others = piece_between(total, around(total, axis))
        total, before = simple(
            functools.partial(group_kernel, axis), f"group_{axis}", [(5, 16, 128), (8, 16, 128)],
            (total, *others, pars), [four],
        )
        befores.append(before)
    others = piece_between(total, around(total, "z"))
    mine, theirs = simple(
        enter_kernel, "enter", [(4, 16, 128), (4, 16, 128)],
        (total, *others, befores[1], befores[0], keep, partner, pars), [four],
    )
    other = piece_between(theirs, lax.ppermute(theirs, "c", swap))

    spec = pl.BlockSpec(memory_space=VMEM)
    args = (
        mine, other, *(p[0] for p in pieces), *(p[1] for p in pieces), *(p[2] for p in pieces),
        glu_weight, glu_bias.reshape(1, CHANNELS), out_weight, out_gain.reshape(1, D),
    )
    return pl.pallas_call(
        final_kernel,
        name="final",
        in_specs=[spec] * len(args),
        out_specs=spec,
        out_shape=sds((ROWS, D), BF16),
        scratch_shapes=[VMEM((2, 4, 16, 128), F32), VMEM((ROWS, CHANNELS), F32)],
        compiler_params=params(12),
    )(*args)


def hbm(x):
    return pltpu.with_memory_space_constraint(x, pltpu.HBM)


def solution(mesh):
    finer = Mesh(mesh.devices.reshape(4, 4, 4, 2), AXES)
    split = P(AXES, None)
    placed = (split, P(AXES), P(), P(), P(), P(), P(), P(), P(), P(), P(), P(), P())
    return jax.shard_map(local, mesh=finer, in_specs=placed, out_specs=split, check_vma=False)
```

```python
import functools
import math

import jax
import jax.numpy as jnp
from jax import lax
from jax.experimental import pallas as pl
from jax.experimental.pallas import tpu as pltpu
from jax.sharding import Mesh
from jax.sharding import PartitionSpec as P

ROWS = 128
D = 2048
CHANNELS = 1024
TILES = 8
SPAN = 16
SPANS = ROWS // SPAN
PIECES = (1,) * 8
LOG2E = 1.0 / math.log(2.0)
EPSILON = 1e-06
AXES = ("z", "x", "y", "c")
VMEM = pltpu.VMEM
HIGHEST = lax.Precision.HIGHEST
F32 = jnp.float32
BF16 = jnp.bfloat16

SINE = (4.44288291, -7.30824512, 3.60634303, -0.84604096, 0.10968436)
COSINE = (1.4142135, -6.97885097, 5.73946067, -1.88355924, 0.31068962)
SINE_SHORT = (4.44287876, -7.30776104, 3.5971931, -0.7896682)
COSINE_SHORT = (1.41420407, -6.97764062, 5.71521917, -1.7282871)
DAMP = (
    9.99995989e-01,
    -2.49939726e-01,
    5.19269127e-02,
    -7.65257696e-03,
    7.74390930e-04,
    -4.89307841e-05,
    1.45423687e-06,
)


def horner(coefficients, x):
    value = coefficients[-1] * x + coefficients[-2]
    for c in coefficients[-3::-1]:
        value = value * x + c
    return value


def half_turn(turns, sine=SINE_SHORT, cosine=COSINE_SHORT):
    r = turns - jnp.round(turns)
    z = r * r
    return r * horner(sine, z), horner(cosine, z)


def unit_circle(turns, *tables):
    s, c = half_turn(turns, *tables)
    return 1.0 - s * s, s * c


def nt(a, b):
    return lax.dot_general(a, b, (((1,), (1,)), ((), ())), preferred_element_type=F32)


def mm(a, b):
    return jnp.dot(a, b, preferred_element_type=F32)


def iotas(shape):
    return lax.broadcasted_iota(jnp.int32, shape, 0), lax.broadcasted_iota(jnp.int32, shape, 1)


def column_of(row):
    return jnp.broadcast_to(row, (ROWS, ROWS)).T


def exact_mm(a, b):
    return jnp.dot(a, b, preferred_element_type=F32, precision=HIGHEST)


def pair_row(ref, k, pair):
    return jnp.concatenate([ref[k, pl.ds(2 * pair, 1), :], ref[k, pl.ds(2 * pair + 1, 1), :]], axis=1)


def end_kernel(
    tokens, elapsed, gain, weight, inputs, angle, rate,
    driven_ref, ends_ref, pars_ref, damp_ref, within_ref, normed, times,
):
    step = pl.program_id(0)
    core = lax.axis_index("c")

    @pl.when(step == 0)
    def _():
        x = tokens[...].astype(F32)
        scale = lax.rsqrt(jnp.mean(x * x, axis=-1, keepdims=True) + EPSILON)
        normed[...] = (x * scale * gain[...]).astype(BF16)
        steps = column_of(elapsed[...])
        row, col = iotas((ROWS, ROWS))
        same = row // SPAN == col // SPAN
        times[0] = exact_mm((col > row).astype(F32), steps)
        times[1] = exact_mm((col < row).astype(F32), steps)
        times[2] = jnp.sqrt(steps)
        times[3] = steps
        within_ref[0] = exact_mm(((col <= row) & same).astype(F32), steps)
        within_ref[1] = exact_mm(((col >= row) & same).astype(F32), steps)
        total = exact_mm(jnp.ones((8, ROWS), F32), steps)
        ends_ref[0, 64:] = total
        ends_ref[1, 64:] = total

    driven = mm(normed[...], weight[...]).astype(BF16)
    driven_ref[...] = driven
    flipped = driven.astype(F32).T.astype(BF16)
    first = lax.broadcasted_iota(jnp.int32, (16, 128), 1) < 64
    away = jnp.where((step // 4) == core, 0, 1)
    for j in range(4):
        pair = step * 4 + j
        for k in range(2):
            f = pair_row(rate, k, pair)
            th = pair_row(angle, k, pair)
            pars_ref[k, 0, pl.ds(pair, 1), :] = th
            pars_ref[k, 1, pl.ds(pair, 1), :] = f
            f2 = f * 2.0
            root = jnp.sqrt(f2)
            after = times[k]
            s, c = half_turn(after * (th * (0.5 / math.pi)))
            damp = horner(DAMP, times[3] * f2) * times[2]
            damp_ref[j, k] = damp
            amp = jnp.exp2(after * (f * -LOG2E)) * damp
            tilted = amp * s
            pull = jnp.concatenate([(amp - tilted * s).astype(BF16), (tilted * c).astype(BF16)], axis=1)
            mixed = mm(flipped[32 * j : 32 * j + 32], pull)
            m_re = jnp.where(first, mixed[:16, :128], mixed[16:, :128])
            m_im = jnp.where(first, mixed[:16, 128:], mixed[16:, 128:])
            b_re, b_im = (
                jnp.concatenate([inputs[k, c, 2 * j].astype(F32), inputs[k, c, 2 * j + 1].astype(F32)], axis=1)
                for c in range(2)
            )
            at = 32 * k + 4 * (step % 4) + j
            ends_ref[away, pl.ds(at, 1), :] = root * jnp.sum(b_re * m_re - b_im * m_im, axis=0, keepdims=True)
            ends_ref[away, pl.ds(at + 16, 1), :] = root * jnp.sum(b_re * m_im + b_im * m_re, axis=0, keepdims=True)


def local_kernel(
    offset, within, damps, driven, inputs, readout, angle, rate, skip,
    out_ref, prefix_ref, table_ref,
):
    step = pl.program_id(0)
    row, col = iotas((ROWS, ROWS))
    same = row // SPAN == col // SPAN
    triangles = (((col <= row) & same).astype(BF16), ((col >= row) & same).astype(BF16))
    empty = jnp.zeros((16, 64), BF16)
    hole = jnp.zeros((16, 64), F32)
    x = driven[...]
    outs = []
    for j in range(4):
        pair = (step + offset) * 4 + j
        lhs = x[:, 32 * j : 32 * j + 32]
        total = None
        for k in range(2):
            f = pair_row(rate, k, pair)
            th = pair_row(angle, k, pair)
            root = jnp.sqrt(f * 2.0)
            b00, b01 = inputs[k, 0, 2 * j], inputs[k, 1, 2 * j]
            b10, b11 = inputs[k, 0, 2 * j + 1], inputs[k, 1, 2 * j + 1]
            rhs = jnp.concatenate(
                [
                    jnp.concatenate([b00, empty, b01, empty], axis=1),
                    jnp.concatenate([empty, b10, empty, b11], axis=1),
                ],
                axis=0,
            )
            proj = mm(lhs, rhs)
            p_re, p_im = proj[:, :128], proj[:, 128:]
            offs = within[k]
            cosine, sine = unit_circle(offs * (th * (0.5 / math.pi)))
            grow = jnp.exp2(offs * (f * LOG2E)) * damps[j, k]
            fade = jnp.exp2(offs * (f * -LOG2E))
            a_re, a_im = grow * cosine, grow * sine
            lift = jnp.concatenate(
                [(a_re * p_re + a_im * p_im).astype(BF16), (a_re * p_im - a_im * p_re).astype(BF16)], axis=1
            )
            part = mm(triangles[k], lift)
            e_re, e_im = fade * cosine, fade * sine
            c_re = c_im = jnp.zeros((1, 128), F32)
            d_re, d_im = jnp.ones((1, 128), F32), jnp.zeros((1, 128), F32)
            states, prefixes = [None] * SPANS, [None] * SPANS
            for n in range(SPANS) if k == 0 else range(SPANS - 1, -1, -1):
                cut = slice(SPAN * n, SPAN * n + SPAN)
                er, ei = e_re[cut], e_im[cut]
                wr, wi = part[cut, :128] + c_re, part[cut, 128:] + c_im
                sr, si = er * wr - ei * wi, er * wi + ei * wr
                pr, pi = er * d_re - ei * d_im, er * d_im + ei * d_re
                edge = slice(SPAN - 1, SPAN) if k == 0 else slice(0, 1)
                c_re, c_im, d_re, d_im = sr[edge], si[edge], pr[edge], pi[edge]
                states[n] = jnp.concatenate([sr.astype(BF16), si.astype(BF16)], axis=1)
                prefixes[n] = jnp.concatenate([pr.astype(BF16), pi.astype(BF16)], axis=1)
            prefix_ref[j, k] = jnp.concatenate(prefixes, axis=0)
            tables = []
            for c in range(2):
                upper = jnp.concatenate([readout[k, c, 2 * j], hole], axis=1)
                lower = jnp.concatenate([hole, readout[k, c, 2 * j + 1]], axis=1)
                table = jnp.concatenate([upper, lower], axis=0)
                table_ref[j, k, c] = table
                tables.append(table * root)
            y = nt(
                jnp.concatenate(states, axis=0),
                jnp.concatenate([tables[0].astype(BF16), (-tables[1]).astype(BF16)], axis=1),
            )
            total = y if total is None else total + y
        outs.append(total)
    out_ref[...] = jnp.concatenate(outs, axis=1) + skip[...] * x.astype(F32)


def times_of(a, b):
    return a[0] * b[0] - a[1] * b[1], a[0] * b[1] + a[1] * b[0]


def plus(a, b):
    return a[0] + b[0], a[1] + b[1]


def pick(condition, a, b):
    return tuple(jnp.where(condition, x, y) for x, y in zip(a, b))


def my_pars(pars):
    core = lax.axis_index("c")
    found = []
    for k in range(2):
        angle = pars[k, 0, pl.ds(16 * core, 16), :]
        rate = pars[k, 1, pl.ds(16 * core, 16), :]
        high = jnp.round(angle * (4096 * 0.5 / math.pi)) * (1.0 / 4096)
        coarse = 6433 / 1024
        low = ((angle - high * coarse) - high * (2 * math.pi - coarse)) * (0.5 / math.pi)
        found.append((high, low, rate * -LOG2E))
    return found


def decay_over(span, pars):
    high, low, level = pars
    u = span * high
    cosine, sine = unit_circle((u - jnp.round(u)) + span * low, SINE, COSINE)
    fade = jnp.exp2(span * level)
    return fade * cosine, fade * sine


def states_of(ref, k):
    return ref[32 * k : 32 * k + 16, :], ref[32 * k + 16 : 32 * k + 32, :]


def span_of(ref):
    span = ref[64:72, :]
    return jnp.concatenate([span, span], axis=0)


def keep_at(ref, at, value):
    ref[2 * at], ref[2 * at + 1] = value


def upper(stage):
    axis, kind = stage
    here = lax.axis_index(axis)
    return here >= 2 if kind == "high" else here % 2 == 1


def merge(stage, own, other, mine, total_ref, k, decay, decay_other):
    behind = upper(stage) if k == 0 else jnp.logical_not(upper(stage))
    a, b = states_of(own, k), states_of(other, k)
    early, late = pick(behind, b, a), pick(behind, a, b)
    total = plus(times_of(pick(behind, decay, decay_other), early), late)
    if total_ref is not None:
        total_ref[32 * k : 32 * k + 16, :], total_ref[32 * k + 16 : 32 * k + 32, :] = total
    return behind, b


def pair_kernel(own, other, pars, total_ref, trail_ref):
    mine = my_pars(pars)
    zero = jnp.zeros((16, 128), F32)
    for k in range(2):
        decay, decay_other = decay_over(span_of(own), mine[k]), decay_over(span_of(other), mine[k])
        merge(("c", "low"), own, other, mine, total_ref, k, decay, decay_other)
        keep_at(trail_ref, k, (zero, zero))
        keep_at(trail_ref, 2 + k, (zero + 1.0, zero))
        keep_at(trail_ref, 4 + k, times_of(decay, decay_other))
    total_ref[64:72, :] = own[64:72, :] + other[64:72, :]


def trail_of(trail, at):
    return trail[2 * at], trail[2 * at + 1]


def stage_kernel(stage, own, other, trail, pars, total_ref, trail_ref):
    mine = my_pars(pars)
    for k in range(2):
        decay, decay_other = trail_of(trail, 4 + k), decay_over(span_of(other), mine[k])
        behind, theirs = merge(stage, own, other, mine, total_ref, k, decay, decay_other)
        state, fade = trail_of(trail, k), trail_of(trail, 2 + k)
        keep_at(trail_ref, k, pick(behind, plus(times_of(fade, theirs), state), state))
        keep_at(trail_ref, 2 + k, pick(behind, times_of(fade, decay_other), fade))
        keep_at(trail_ref, 4 + k, times_of(decay, decay_other))
    total_ref[64:72, :] = own[64:72, :] + other[64:72, :]


def enter_kernel(stage, last, trail, own, other, pars, mine_ref, theirs_ref):
    core = lax.axis_index("c")
    mine = my_pars(pars)
    for k in range(2):
        behind = upper(stage) if k == 0 else jnp.logical_not(upper(stage))
        state, fade = trail_of(trail, k), trail_of(trail, 2 + k)
        state = pick(behind, plus(times_of(fade, states_of(last, k)), state), state)
        ahead = core == k
        early = pick(ahead, states_of(own, k), states_of(other, k))
        later = plus(times_of(decay_over(jnp.where(ahead, span_of(own), span_of(other)), mine[k]), state), early)
        keep_at(mine_ref, k, pick(ahead, state, later))
        keep_at(theirs_ref, k, pick(ahead, later, state))


def final_kernel(*refs):
    count = len(PIECES)
    own, other = refs[:2]
    nears, prefixes, tables = (refs[2 + count * n : 2 + count * n + count] for n in range(3))
    glu, glu_bias, outw, out_gain, out_ref, entering, response = refs[2 + 3 * count :]
    core = lax.axis_index("c")
    entering[core] = own[...]
    entering[1 - core] = other[...]
    start = 0
    for size, near, prefix, table in zip(PIECES, nears, prefixes, tables):

        def tile(i, _, start=start, near=near, prefix=prefix, table=table):
            outs = []
            for j in range(4):
                total = None
                for k in range(2):
                    pair = 4 * (start + i) + j
                    er = entering[pair // 16, 2 * k, pl.ds(pair % 16, 1), :]
                    ei = entering[pair // 16, 2 * k + 1, pl.ds(pair % 16, 1), :]
                    cr, ci = table[4 * i + j, k, 0], table[4 * i + j, k, 1]
                    rhs = jnp.concatenate(
                        [(cr * er - ci * ei).astype(BF16), (-(cr * ei + ci * er)).astype(BF16)], axis=1
                    )
                    y = nt(prefix[4 * i + j, k], rhs)
                    total = y if total is None else total + y
                outs.append(total)
            at = pl.multiple_of(128 * i, 128)
            response[:, pl.ds(at + 128 * start, 128)] = jnp.concatenate(outs, axis=1) + near[:, pl.ds(at, 128)]
            return 0

        lax.fori_loop(0, size, tile, 0)
        start += size
    x = response[...]
    active = 0.5 * x * (1.0 + jnp.tanh(math.sqrt(2.0 / math.pi) * (x + 0.044715 * (x * x * x))))
    gate = mm(active.astype(BF16), glu[...]) + glu_bias[...]
    gated = (active * jax.nn.sigmoid(gate)).astype(BF16)
    projected = mm(gated, outw[...])
    scale = lax.rsqrt(jnp.mean(projected * projected, axis=-1, keepdims=True) + EPSILON)
    out_ref[...] = (projected * scale * out_gain[...]).astype(BF16)


def whole(shape):
    return pl.BlockSpec(shape, lambda *_: (0,) * len(shape))


def sds(shape, dtype=F32):
    return jax.ShapeDtypeStruct(shape, dtype)


def params(limit):
    return pltpu.CompilerParams(vmem_limit_bytes=limit * 1024 * 1024)


def run_local(start, size, within, damps, driven, inputs, state_output, angle, rate, skip_row):
    row_spec = whole((2, 64, 64))
    return pl.pallas_call(
        functools.partial(local_kernel, start),
        name=f"local_{start}",
        grid=(size,),
        in_specs=[
            whole((2, ROWS, ROWS)),
            pl.BlockSpec((4, 2, ROWS, ROWS), lambda i: (i + start, 0, 0, 0)),
            pl.BlockSpec((ROWS, 128), lambda i: (0, i + start)),
            pl.BlockSpec((2, 2, 8, 16, 64), lambda i: (0, 0, i + start, 0, 0)),
            pl.BlockSpec((2, 2, 8, 16, 64), lambda i: (0, 0, i + start, 0, 0)),
            row_spec, row_spec,
            pl.BlockSpec((1, 128), lambda i: (0, i + start)),
        ],
        out_specs=[
            pl.BlockSpec((ROWS, 128), lambda i: (0, i)),
            pl.BlockSpec((4, 2, ROWS, 256), lambda i: (i, 0, 0, 0)),
            pl.BlockSpec((4, 2, 2, 32, 128), lambda i: (i, 0, 0, 0, 0)),
        ],
        out_shape=[
            sds((ROWS, 128 * size)),
            sds((4 * size, 2, ROWS, 256), BF16),
            sds((4 * size, 2, 2, 32, 128)),
        ],
        compiler_params=params(10),
        cost_estimate=pl.CostEstimate(flops=size * 5 * 10**8, bytes_accessed=size * 2 * 2**20, transcendentals=0),
    )(within, damps, driven, inputs, state_output, angle, rate, skip_row)


def simple(kernel, name, shapes, args, scratch=()):
    spec = pl.BlockSpec(memory_space=VMEM)
    return pl.pallas_call(
        kernel,
        name=name,
        in_specs=[spec] * len(args),
        out_specs=[spec] * len(shapes),
        out_shape=[sds(shape) for shape in shapes],
        scratch_shapes=scratch,
        compiler_params=params(4),
    )(*args)


def local(
    tokens, elapsed, norm_gain, in_weight, state_input, state_output, forget_rate, decay_angle,
    skip_gain, glu_weight, glu_bias, out_weight, out_gain,
):
    elapsed_row = elapsed.reshape(1, ROWS)
    inputs = jnp.swapaxes(state_input, 3, 4)
    row_spec = whole((2, 64, 64))
    driven, ends, pars, damps, within = pl.pallas_call(
        end_kernel,
        name="ends",
        grid=(TILES,),
        in_specs=[
            whole((ROWS, D)),
            whole((1, ROWS)),
            whole((1, D)),
            pl.BlockSpec((D, 128), lambda i: (0, i)),
            pl.BlockSpec((2, 2, 8, 16, 64), lambda i: (0, 0, i, 0, 0)),
            row_spec, row_spec,
        ],
        out_specs=[
            pl.BlockSpec((ROWS, 128), lambda i: (0, i)),
            whole((2, 72, 128)),
            whole((2, 2, 32, 128)),
            pl.BlockSpec((4, 2, ROWS, ROWS), lambda i: (i, 0, 0, 0)),
            whole((2, ROWS, ROWS)),
        ],
        out_shape=[
            sds((ROWS, CHANNELS), BF16), sds((2, 72, 128)), sds((2, 2, 32, 128)),
            sds((32, 2, ROWS, ROWS)), sds((2, ROWS, ROWS)),
        ],
        scratch_shapes=[VMEM((ROWS, D), BF16), VMEM((4, ROWS, ROWS), F32)],
        compiler_params=params(10),
    )(
        *(hbm(a) for a in (tokens, elapsed_row, norm_gain.reshape(1, D), in_weight, inputs, decay_angle, forget_rate))
    )

    skip_row = skip_gain.reshape(1, CHANNELS)
    pieces, start = [], 0

    def piece_between(before, after):
        index = len(pieces)
        start = sum(PIECES[:index])
        driven_now, _ = lax.optimization_barrier((driven, before))
        piece = run_local(
            start, PIECES[index], within, damps, driven_now, inputs, state_output, decay_angle, forget_rate, skip_row
        )
        *piece, after = lax.optimization_barrier((*piece, after))
        pieces.append(piece)
        return after

    swap = [(0, 1), (1, 0)]
    pairings = {"low": [(0, 1), (1, 0), (2, 3), (3, 2)], "high": [(0, 3), (3, 0), (1, 2), (2, 1)]}
    stages = [(axis, kind) for axis in ("y", "x", "z") for kind in ("low", "high")]
    keep = ends[0]
    partner = piece_between(keep, lax.ppermute(ends[1], "c", swap))
    total, trail = simple(pair_kernel, "pair", [(72, 128), (12, 16, 128)], (keep, partner, pars))
    for stage in stages:
        axis, kind = stage
        other = piece_between(total, lax.ppermute(total, axis, pairings[kind]))
        if stage == stages[-1]:
            mine, theirs = simple(
                functools.partial(enter_kernel, stage), "enter", [(4, 16, 128), (4, 16, 128)],
                (other, trail, keep, partner, pars),
            )
        else:
            total, trail = simple(
                functools.partial(stage_kernel, stage), f"stage_{axis}_{kind}", [(72, 128), (12, 16, 128)],
                (total, other, trail, pars),
            )
    other = piece_between(theirs, lax.ppermute(theirs, "c", swap))

    spec = pl.BlockSpec(memory_space=VMEM)
    args = (
        mine, other, *(p[0] for p in pieces), *(p[1] for p in pieces), *(p[2] for p in pieces),
        glu_weight, glu_bias.reshape(1, CHANNELS), out_weight, out_gain.reshape(1, D),
    )
    return pl.pallas_call(
        final_kernel,
        name="final",
        in_specs=[spec] * len(args),
        out_specs=spec,
        out_shape=sds((ROWS, D), BF16),
        scratch_shapes=[VMEM((2, 4, 16, 128), F32), VMEM((ROWS, CHANNELS), F32)],
        compiler_params=params(12),
    )(*args)


def hbm(x):
    return pltpu.with_memory_space_constraint(x, pltpu.HBM)


def solution(mesh):
    finer = Mesh(mesh.devices.reshape(4, 4, 4, 2), AXES)
    split = P(AXES, None)
    placed = (split, P(AXES), P(), P(), P(), P(), P(), P(), P(), P(), P(), P(), P())
    return jax.shard_map(local, mesh=finer, in_specs=placed, out_specs=split, check_vma=False)
```

```python
import functools
import math

import jax
import jax.numpy as jnp
from jax import lax
from jax.experimental import pallas as pl
from jax.experimental.pallas import tpu as pltpu
from jax.sharding import Mesh
from jax.sharding import PartitionSpec as P

ROWS = 128
D = 2048
CHANNELS = 1024
TILES = 8
SPAN = 16
SPANS = ROWS // SPAN
PIECES = (1,) * 8
LOG2E = 1.0 / math.log(2.0)
EPSILON = 1e-06
AXES = ("z", "x", "y", "c")
VMEM = pltpu.VMEM
HIGHEST = lax.Precision.HIGHEST
F32 = jnp.float32
BF16 = jnp.bfloat16

SINE = (4.44288291, -7.30824512, 3.60634303, -0.84604096, 0.10968436)
COSINE = (1.4142135, -6.97885097, 5.73946067, -1.88355924, 0.31068962)
SINE_SHORT = (4.44287876, -7.30776104, 3.5971931, -0.7896682)
COSINE_SHORT = (1.41420407, -6.97764062, 5.71521917, -1.7282871)
DAMP = (
    9.99995989e-01,
    -2.49939726e-01,
    5.19269127e-02,
    -7.65257696e-03,
    7.74390930e-04,
    -4.89307841e-05,
    1.45423687e-06,
)


def horner(coefficients, x):
    value = coefficients[-1] * x + coefficients[-2]
    for c in coefficients[-3::-1]:
        value = value * x + c
    return value


def half_turn(turns, sine=SINE_SHORT, cosine=COSINE_SHORT):
    r = turns - jnp.round(turns)
    z = r * r
    return r * horner(sine, z), horner(cosine, z)


def unit_circle(turns, *tables):
    s, c = half_turn(turns, *tables)
    return 1.0 - s * s, s * c


def nt(a, b):
    return lax.dot_general(a, b, (((1,), (1,)), ((), ())), preferred_element_type=F32)


def mm(a, b):
    return jnp.dot(a, b, preferred_element_type=F32)


def iotas(shape):
    return lax.broadcasted_iota(jnp.int32, shape, 0), lax.broadcasted_iota(jnp.int32, shape, 1)


def column_of(row):
    return jnp.broadcast_to(row, (ROWS, ROWS)).T


def exact_mm(a, b):
    return jnp.dot(a, b, preferred_element_type=F32, precision=HIGHEST)


def pair_row(ref, k, pair):
    return jnp.concatenate([ref[k, pl.ds(2 * pair, 1), :], ref[k, pl.ds(2 * pair + 1, 1), :]], axis=1)


def end_kernel(
    tokens, elapsed, gain, weight, inputs, angle, rate,
    driven_ref, ends_ref, pars_ref, damp_ref, within_ref, normed, times,
):
    step = pl.program_id(0)

    @pl.when(step == 0)
    def _():
        x = tokens[...].astype(F32)
        scale = lax.rsqrt(jnp.mean(x * x, axis=-1, keepdims=True) + EPSILON)
        normed[...] = (x * scale * gain[...]).astype(BF16)
        steps = column_of(elapsed[...])
        row, col = iotas((ROWS, ROWS))
        same = row // SPAN == col // SPAN
        times[0] = exact_mm((col > row).astype(F32), steps)
        times[1] = exact_mm((col < row).astype(F32), steps)
        times[2] = jnp.sqrt(steps)
        times[3] = steps
        within_ref[0] = exact_mm(((col <= row) & same).astype(F32), steps)
        within_ref[1] = exact_mm(((col >= row) & same).astype(F32), steps)
        total = exact_mm(jnp.ones((8, ROWS), F32), steps)
        ends_ref[128:, :] = total

    driven = mm(normed[...], weight[...]).astype(BF16)
    driven_ref[...] = driven
    flipped = driven.astype(F32).T.astype(BF16)
    first = lax.broadcasted_iota(jnp.int32, (16, 128), 1) < 64
    for j in range(4):
        pair = step * 4 + j
        for k in range(2):
            f = pair_row(rate, k, pair)
            th = pair_row(angle, k, pair)
            pars_ref[k, 0, pl.ds(pair, 1), :] = th
            pars_ref[k, 1, pl.ds(pair, 1), :] = f
            f2 = f * 2.0
            root = jnp.sqrt(f2)
            after = times[k]
            s, c = half_turn(after * (th * (0.5 / math.pi)))
            damp = horner(DAMP, times[3] * f2) * times[2]
            damp_ref[j, k] = damp
            amp = jnp.exp2(after * (f * -LOG2E)) * damp
            tilted = amp * s
            pull = jnp.concatenate([(amp - tilted * s).astype(BF16), (tilted * c).astype(BF16)], axis=1)
            mixed = mm(flipped[32 * j : 32 * j + 32], pull)
            m_re = jnp.where(first, mixed[:16, :128], mixed[16:, :128])
            m_im = jnp.where(first, mixed[:16, 128:], mixed[16:, 128:])
            b_re, b_im = (
                jnp.concatenate([inputs[k, c, 2 * j].astype(F32), inputs[k, c, 2 * j + 1].astype(F32)], axis=1)
                for c in range(2)
            )
            at = 64 * k + pair
            ends_ref[pl.ds(at, 1), :] = root * jnp.sum(b_re * m_re - b_im * m_im, axis=0, keepdims=True)
            ends_ref[pl.ds(at + 32, 1), :] = root * jnp.sum(b_re * m_im + b_im * m_re, axis=0, keepdims=True)


def local_kernel(
    offset, within, damps, driven, inputs, readout, angle, rate, skip,
    out_ref, prefix_ref, table_ref,
):
    step = pl.program_id(0)
    row, col = iotas((ROWS, ROWS))
    same = row // SPAN == col // SPAN
    triangles = (((col <= row) & same).astype(BF16), ((col >= row) & same).astype(BF16))
    empty = jnp.zeros((16, 64), BF16)
    hole = jnp.zeros((16, 64), F32)
    x = driven[...]
    outs = []
    for j in range(4):
        pair = (step + offset) * 4 + j
        lhs = x[:, 32 * j : 32 * j + 32]
        total = None
        for k in range(2):
            f = pair_row(rate, k, pair)
            th = pair_row(angle, k, pair)
            root = jnp.sqrt(f * 2.0)
            b00, b01 = inputs[k, 0, 2 * j], inputs[k, 1, 2 * j]
            b10, b11 = inputs[k, 0, 2 * j + 1], inputs[k, 1, 2 * j + 1]
            rhs = jnp.concatenate(
                [
                    jnp.concatenate([b00, empty, b01, empty], axis=1),
                    jnp.concatenate([empty, b10, empty, b11], axis=1),
                ],
                axis=0,
            )
            proj = mm(lhs, rhs)
            p_re, p_im = proj[:, :128], proj[:, 128:]
            offs = within[k]
            cosine, sine = unit_circle(offs * (th * (0.5 / math.pi)))
            grow = jnp.exp2(offs * (f * LOG2E)) * damps[j, k]
            fade = jnp.exp2(offs * (f * -LOG2E))
            a_re, a_im = grow * cosine, grow * sine
            lift = jnp.concatenate(
                [(a_re * p_re + a_im * p_im).astype(BF16), (a_re * p_im - a_im * p_re).astype(BF16)], axis=1
            )
            part = mm(triangles[k], lift)
            e_re, e_im = fade * cosine, fade * sine
            c_re = c_im = jnp.zeros((1, 128), F32)
            d_re, d_im = jnp.ones((1, 128), F32), jnp.zeros((1, 128), F32)
            states, prefixes = [None] * SPANS, [None] * SPANS
            for n in range(SPANS) if k == 0 else range(SPANS - 1, -1, -1):
                cut = slice(SPAN * n, SPAN * n + SPAN)
                er, ei = e_re[cut], e_im[cut]
                wr, wi = part[cut, :128] + c_re, part[cut, 128:] + c_im
                sr, si = er * wr - ei * wi, er * wi + ei * wr
                pr, pi = er * d_re - ei * d_im, er * d_im + ei * d_re
                edge = slice(SPAN - 1, SPAN) if k == 0 else slice(0, 1)
                c_re, c_im, d_re, d_im = sr[edge], si[edge], pr[edge], pi[edge]
                states[n] = jnp.concatenate([sr.astype(BF16), si.astype(BF16)], axis=1)
                prefixes[n] = jnp.concatenate([pr.astype(BF16), pi.astype(BF16)], axis=1)
            prefix_ref[j, k] = jnp.concatenate(prefixes, axis=0)
            tables = []
            for c in range(2):
                upper = jnp.concatenate([readout[k, c, 2 * j], hole], axis=1)
                lower = jnp.concatenate([hole, readout[k, c, 2 * j + 1]], axis=1)
                table = jnp.concatenate([upper, lower], axis=0)
                table_ref[j, k, c] = table
                tables.append(table * root)
            y = nt(
                jnp.concatenate(states, axis=0),
                jnp.concatenate([tables[0].astype(BF16), (-tables[1]).astype(BF16)], axis=1),
            )
            total = y if total is None else total + y
        outs.append(total)
    out_ref[...] = jnp.concatenate(outs, axis=1) + skip[...] * x.astype(F32)


def times_of(a, b):
    return a[0] * b[0] - a[1] * b[1], a[0] * b[1] + a[1] * b[0]


def plus(a, b):
    return a[0] + b[0], a[1] + b[1]


def pick(condition, a, b):
    return tuple(jnp.where(condition, x, y) for x, y in zip(a, b))


def my_pars(pars):
    found = []
    for k in range(2):
        angle, rate = pars[k, 0], pars[k, 1]
        high = jnp.round(angle * (4096 * 0.5 / math.pi)) * (1.0 / 4096)
        coarse = 6433 / 1024
        low = ((angle - high * coarse) - high * (2 * math.pi - coarse)) * (0.5 / math.pi)
        found.append((high, low, rate * -LOG2E))
    return found


def decay_over(span, pars):
    high, low, level = pars
    u = span * high
    cosine, sine = unit_circle((u - jnp.round(u)) + span * low, SINE, COSINE)
    fade = jnp.exp2(span * level)
    return fade * cosine, fade * sine


def states_of(ref, k):
    return ref[64 * k : 64 * k + 32, :], ref[64 * k + 32 : 64 * k + 64, :]


def keep_states(ref, k, value):
    ref[64 * k : 64 * k + 32, :], ref[64 * k + 32 : 64 * k + 64, :] = value


def span_of(ref):
    return jnp.concatenate([ref[128:136, :]] * 4, axis=0)


def trail_of(trail, at):
    return trail[2 * at], trail[2 * at + 1]


def keep_trail(trail, at, value):
    trail[2 * at], trail[2 * at + 1] = value


def upper(stage):
    axis, kind = stage
    here = lax.axis_index(axis)
    return here >= 2 if kind == "high" else here % 2 == 1


def is_behind(stage, k):
    return upper(stage) if k == 0 else jnp.logical_not(upper(stage))


def pair_kernel(own, other, pars, total_ref, trail_ref):
    mine = my_pars(pars)
    zero = jnp.zeros((32, 128), F32)
    for k in range(2):
        decay, decay_other = decay_over(span_of(own), mine[k]), decay_over(span_of(other), mine[k])
        a, b = states_of(own, k), states_of(other, k)
        total = plus(times_of(decay, b), a) if k == 0 else plus(times_of(decay_other, a), b)
        keep_states(total_ref, k, total)
        keep_trail(trail_ref, k, (zero, zero))
        keep_trail(trail_ref, 2 + k, (zero + 1.0, zero))
        keep_trail(trail_ref, 4 + k, times_of(decay, decay_other))
    total_ref[128:136, :] = own[128:136, :] + other[128:136, :]


def stage_kernel(stage, own, other, trail, pars, total_ref, trail_ref):
    mine = my_pars(pars)
    for k in range(2):
        decay, decay_other = trail_of(trail, 4 + k), decay_over(span_of(other), mine[k])
        behind = is_behind(stage, k)
        a, b = states_of(own, k), states_of(other, k)
        early, late = pick(behind, b, a), pick(behind, a, b)
        keep_states(total_ref, k, plus(times_of(pick(behind, decay, decay_other), early), late))
        state, fade = trail_of(trail, k), trail_of(trail, 2 + k)
        keep_trail(trail_ref, k, pick(behind, plus(times_of(fade, b), state), state))
        keep_trail(trail_ref, 2 + k, pick(behind, times_of(fade, decay_other), fade))
        keep_trail(trail_ref, 4 + k, times_of(decay, decay_other))
    total_ref[128:136, :] = own[128:136, :] + other[128:136, :]


def enter_kernel(stage, last, trail, own, other, pars, mine_ref, theirs_ref):
    mine = my_pars(pars)
    for k in range(2):
        state, fade = trail_of(trail, k), trail_of(trail, 2 + k)
        state = pick(is_behind(stage, k), plus(times_of(fade, states_of(last, k)), state), state)
        early = other if k == 0 else own
        later = plus(times_of(decay_over(span_of(early), mine[k]), state), states_of(early, k))
        keep_states(mine_ref, k, later if k == 0 else state)
        keep_states(theirs_ref, k, state if k == 0 else later)


def final_kernel(*refs):
    count = len(PIECES)
    own, other = refs[:2]
    nears, prefixes, tables = (refs[2 + count * n : 2 + count * n + count] for n in range(3))
    glu, glu_bias, outw, out_gain, out_ref, entering, response = refs[2 + 3 * count :]
    entering[...] = jnp.where(lax.axis_index("c") == 1, own[...], other[...])
    start = 0
    for size, near, prefix, table in zip(PIECES, nears, prefixes, tables):

        def tile(i, _, start=start, near=near, prefix=prefix, table=table):
            outs = []
            for j in range(4):
                total = None
                for k in range(2):
                    pair = 4 * (start + i) + j
                    er = entering[pl.ds(64 * k + pair, 1), :]
                    ei = entering[pl.ds(64 * k + 32 + pair, 1), :]
                    cr, ci = table[4 * i + j, k, 0], table[4 * i + j, k, 1]
                    rhs = jnp.concatenate(
                        [(cr * er - ci * ei).astype(BF16), (-(cr * ei + ci * er)).astype(BF16)], axis=1
                    )
                    y = nt(prefix[4 * i + j, k], rhs)
                    total = y if total is None else total + y
                outs.append(total)
            at = pl.multiple_of(128 * i, 128)
            response[:, pl.ds(at + 128 * start, 128)] = jnp.concatenate(outs, axis=1) + near[:, pl.ds(at, 128)]
            return 0

        lax.fori_loop(0, size, tile, 0)
        start += size
    x = response[...]
    active = 0.5 * x * (1.0 + jnp.tanh(math.sqrt(2.0 / math.pi) * (x + 0.044715 * (x * x * x))))
    gate = mm(active.astype(BF16), glu[...]) + glu_bias[...]
    gated = (active * jax.nn.sigmoid(gate)).astype(BF16)
    projected = mm(gated, outw[...])
    scale = lax.rsqrt(jnp.mean(projected * projected, axis=-1, keepdims=True) + EPSILON)
    out_ref[...] = (projected * scale * out_gain[...]).astype(BF16)


def whole(shape):
    return pl.BlockSpec(shape, lambda *_: (0,) * len(shape))


def sds(shape, dtype=F32):
    return jax.ShapeDtypeStruct(shape, dtype)


def params(limit):
    return pltpu.CompilerParams(vmem_limit_bytes=limit * 1024 * 1024)


def run_local(start, size, within, damps, driven, inputs, state_output, angle, rate, skip_row):
    row_spec = whole((2, 64, 64))
    return pl.pallas_call(
        functools.partial(local_kernel, start),
        name=f"local_{start}",
        grid=(size,),
        in_specs=[
            whole((2, ROWS, ROWS)),
            pl.BlockSpec((4, 2, ROWS, ROWS), lambda i: (i + start, 0, 0, 0)),
            pl.BlockSpec((ROWS, 128), lambda i: (0, i + start)),
            pl.BlockSpec((2, 2, 8, 16, 64), lambda i: (0, 0, i + start, 0, 0)),
            pl.BlockSpec((2, 2, 8, 16, 64), lambda i: (0, 0, i + start, 0, 0)),
            row_spec, row_spec,
            pl.BlockSpec((1, 128), lambda i: (0, i + start)),
        ],
        out_specs=[
            pl.BlockSpec((ROWS, 128), lambda i: (0, i)),
            pl.BlockSpec((4, 2, ROWS, 256), lambda i: (i, 0, 0, 0)),
            pl.BlockSpec((4, 2, 2, 32, 128), lambda i: (i, 0, 0, 0, 0)),
        ],
        out_shape=[
            sds((ROWS, 128 * size)),
            sds((4 * size, 2, ROWS, 256), BF16),
            sds((4 * size, 2, 2, 32, 128)),
        ],
        compiler_params=params(10),
        cost_estimate=pl.CostEstimate(flops=size * 5 * 10**8, bytes_accessed=size * 2 * 2**20, transcendentals=0),
    )(within, damps, driven, inputs, state_output, angle, rate, skip_row)


def simple(kernel, name, shapes, args, scratch=()):
    spec = pl.BlockSpec(memory_space=VMEM)
    return pl.pallas_call(
        kernel,
        name=name,
        in_specs=[spec] * len(args),
        out_specs=[spec] * len(shapes),
        out_shape=[sds(shape) for shape in shapes],
        scratch_shapes=scratch,
        compiler_params=params(4),
    )(*args)


def local(
    tokens, elapsed, norm_gain, in_weight, state_input, state_output, forget_rate, decay_angle,
    skip_gain, glu_weight, glu_bias, out_weight, out_gain,
):
    elapsed_row = elapsed.reshape(1, ROWS)
    inputs = jnp.swapaxes(state_input, 3, 4)
    row_spec = whole((2, 64, 64))
    driven, ends, pars, damps, within = pl.pallas_call(
        end_kernel,
        name="ends",
        grid=(TILES,),
        in_specs=[
            whole((ROWS, D)),
            whole((1, ROWS)),
            whole((1, D)),
            pl.BlockSpec((D, 128), lambda i: (0, i)),
            pl.BlockSpec((2, 2, 8, 16, 64), lambda i: (0, 0, i, 0, 0)),
            row_spec, row_spec,
        ],
        out_specs=[
            pl.BlockSpec((ROWS, 128), lambda i: (0, i)),
            whole((136, 128)),
            whole((2, 2, 32, 128)),
            pl.BlockSpec((4, 2, ROWS, ROWS), lambda i: (i, 0, 0, 0)),
            whole((2, ROWS, ROWS)),
        ],
        out_shape=[
            sds((ROWS, CHANNELS), BF16), sds((136, 128)), sds((2, 2, 32, 128)),
            sds((32, 2, ROWS, ROWS)), sds((2, ROWS, ROWS)),
        ],
        scratch_shapes=[VMEM((ROWS, D), BF16), VMEM((4, ROWS, ROWS), F32)],
        compiler_params=params(10),
    )(
        *(hbm(a) for a in (tokens, elapsed_row, norm_gain.reshape(1, D), in_weight, inputs, decay_angle, forget_rate))
    )

    skip_row = skip_gain.reshape(1, CHANNELS)
    pieces, start = [], 0

    def piece_between(before, after):
        index = len(pieces)
        start = sum(PIECES[:index])
        driven_now, _ = lax.optimization_barrier((driven, before))
        piece = run_local(
            start, PIECES[index], within, damps, driven_now, inputs, state_output, decay_angle, forget_rate, skip_row
        )
        *piece, after = lax.optimization_barrier((*piece, after))
        pieces.append(piece)
        return after

    pairings = {"low": (1, 0, 3, 2), "high": (3, 2, 1, 0)}
    stages = [(axis, kind) for axis in ("y", "x", "z") for kind in ("low", "high")]
    partner = piece_between(ends, lax.ppermute(ends, "c", [(0, 1)]))
    total, trail = simple(pair_kernel, "pair", [(136, 128), (12, 32, 128)], (ends, partner, pars))
    for stage in stages:
        axis, kind = stage
        pairs = [(2 * i + 1, 2 * j + 1) for i, j in enumerate(pairings[kind])]
        other = piece_between(total, lax.ppermute(total, (axis, "c"), pairs))
        if stage == stages[-1]:
            mine, theirs = simple(
                functools.partial(enter_kernel, stage), "enter", [(128, 128), (128, 128)],
                (other, trail, ends, partner, pars),
            )
        else:
            total, trail = simple(
                functools.partial(stage_kernel, stage), f"stage_{axis}_{kind}", [(136, 128), (12, 32, 128)],
                (total, other, trail, pars),
            )
    other = piece_between(theirs, lax.ppermute(theirs, "c", [(1, 0)]))

    spec = pl.BlockSpec(memory_space=VMEM)
    args = (
        mine, other, *(p[0] for p in pieces), *(p[1] for p in pieces), *(p[2] for p in pieces),
        glu_weight, glu_bias.reshape(1, CHANNELS), out_weight, out_gain.reshape(1, D),
    )
    return pl.pallas_call(
        final_kernel,
        name="final",
        in_specs=[spec] * len(args),
        out_specs=spec,
        out_shape=sds((ROWS, D), BF16),
        scratch_shapes=[VMEM((128, 128), F32), VMEM((ROWS, CHANNELS), F32)],
        compiler_params=params(12),
    )(*args)


def hbm(x):
    return pltpu.with_memory_space_constraint(x, pltpu.HBM)


def solution(mesh):
    finer = Mesh(mesh.devices.reshape(4, 4, 4, 2), AXES)
    split = P(AXES, None)
    placed = (split, P(AXES), P(), P(), P(), P(), P(), P(), P(), P(), P(), P(), P())
    return jax.shard_map(local, mesh=finer, in_specs=placed, out_specs=split, check_vma=False)
```

```python
import functools
import math

import jax
import jax.numpy as jnp
from jax import lax
from jax.experimental import pallas as pl
from jax.experimental.pallas import tpu as pltpu
from jax.sharding import Mesh
from jax.sharding import PartitionSpec as P

ROWS = 128
D = 2048
CHANNELS = 1024
TILES = 8
SPAN = 16
SPANS = ROWS // SPAN
PIECES = (1,) * 8
LOG2E = 1.0 / math.log(2.0)
TINY = 1e-37
EPSILON = 1e-06
AXES = ("z", "x", "y", "c")
VMEM = pltpu.VMEM
F32 = jnp.float32
BF16 = jnp.bfloat16

SINE = (4.44288291, -7.30824512, 3.60634303, -0.84604096, 0.10968436)
COSINE = (1.4142135, -6.97885097, 5.73946067, -1.88355924, 0.31068962)
SINE_SHORT = (4.44287876, -7.30776104, 3.5971931, -0.7896682)
COSINE_SHORT = (1.41420407, -6.97764062, 5.71521917, -1.7282871)


def horner(coefficients, x):
    value = coefficients[-1] * x + coefficients[-2]
    for c in coefficients[-3::-1]:
        value = value * x + c
    return value


def half_turn(turns, sine=SINE_SHORT, cosine=COSINE_SHORT):
    r = turns - jnp.round(turns)
    z = r * r
    return r * horner(sine, z), horner(cosine, z)


def unit_circle(turns, *tables):
    s, c = half_turn(turns, *tables)
    return 1.0 - s * s, s * c


def nt(a, b):
    return lax.dot_general(a, b, (((1,), (1,)), ((), ())), preferred_element_type=F32)


def mm(a, b):
    return jnp.dot(a, b, preferred_element_type=F32)


def iotas(shape):
    return lax.broadcasted_iota(jnp.int32, shape, 0), lax.broadcasted_iota(jnp.int32, shape, 1)


def column_of(row):
    return jnp.broadcast_to(row, (ROWS, ROWS)).T


def in_parts(x):
    high = x.astype(BF16)
    rest = x - high.astype(F32)
    middle = rest.astype(BF16)
    return high, middle, (rest - middle.astype(F32)).astype(BF16)


def sums_of(chosen, parts):
    return sum(mm(chosen.astype(BF16), part) for part in parts)


def pair_row(ref, k, pair):
    return jnp.concatenate([ref[k, pl.ds(2 * pair, 1), :], ref[k, pl.ds(2 * pair + 1, 1), :]], axis=1)


def end_kernel(
    tokens, elapsed, gain, weight, inputs, angle, rate,
    driven_ref, ends_ref, pars_ref, damp_ref, within_ref, normed, times,
):
    step = pl.program_id(0)

    @pl.when(step == 0)
    def _():
        x = tokens[...].astype(F32)
        scale = lax.rsqrt(jnp.mean(x * x, axis=-1, keepdims=True) + EPSILON)
        normed[...] = (x * scale * gain[...]).astype(BF16)
        steps = column_of(elapsed[...])
        parts = in_parts(steps)
        row, col = iotas((ROWS, ROWS))
        same = row // SPAN == col // SPAN
        times[0] = sums_of(col > row, parts)
        times[1] = sums_of(col < row, parts)
        times[2] = steps
        within_ref[0] = sums_of((col <= row) & same, parts)
        within_ref[1] = sums_of((col >= row) & same, parts)
        total = sums_of(jnp.ones((8, ROWS), F32), parts)
        ends_ref[128:, :] = total

    driven = mm(normed[...], weight[...]).astype(BF16)
    driven_ref[...] = driven
    flipped = driven.astype(F32).T.astype(BF16)
    first = lax.broadcasted_iota(jnp.int32, (16, 128), 1) < 64
    for j in range(4):
        pair = step * 4 + j
        for k in range(2):
            f = pair_row(rate, k, pair)
            th = pair_row(angle, k, pair)
            pars_ref[k, 0, pl.ds(pair, 1), :] = th
            pars_ref[k, 1, pl.ds(pair, 1), :] = f
            after = times[k]
            s, c = half_turn(after * (th * (0.5 / math.pi)))
            bend = jnp.tanh(times[2] * f)
            damp = bend * lax.rsqrt(bend * (0.5 + 0.5 * bend) + TINY)
            damp_ref[j, k] = damp
            amp = jnp.exp2(after * (f * -LOG2E)) * damp
            tilted = amp * s
            pull = jnp.concatenate([(amp - tilted * s).astype(BF16), (tilted * c).astype(BF16)], axis=1)
            mixed = mm(flipped[32 * j : 32 * j + 32], pull)
            m_re = jnp.where(first, mixed[:16, :128], mixed[16:, :128])
            m_im = jnp.where(first, mixed[:16, 128:], mixed[16:, 128:])
            b_re, b_im = (
                jnp.concatenate([inputs[k, c, 2 * j].astype(F32), inputs[k, c, 2 * j + 1].astype(F32)], axis=1)
                for c in range(2)
            )
            at = 64 * k + pair
            ends_ref[pl.ds(at, 1), :] = jnp.sum(b_re * m_re - b_im * m_im, axis=0, keepdims=True)
            ends_ref[pl.ds(at + 32, 1), :] = jnp.sum(b_re * m_im + b_im * m_re, axis=0, keepdims=True)


def local_kernel(
    offset, within, damps, driven, inputs, readout, angle, rate, skip,
    out_ref, prefix_ref, table_ref,
):
    step = pl.program_id(0)
    row, col = iotas((ROWS, ROWS))
    same = row // SPAN == col // SPAN
    triangles = (((col <= row) & same).astype(BF16), ((col >= row) & same).astype(BF16))
    empty = jnp.zeros((16, 64), BF16)
    hole = jnp.zeros((16, 64), F32)
    x = driven[...]
    outs = []
    for j in range(4):
        pair = (step + offset) * 4 + j
        lhs = x[:, 32 * j : 32 * j + 32]
        total = None
        for k in range(2):
            f = pair_row(rate, k, pair)
            th = pair_row(angle, k, pair)
            b00, b01 = inputs[k, 0, 2 * j], inputs[k, 1, 2 * j]
            b10, b11 = inputs[k, 0, 2 * j + 1], inputs[k, 1, 2 * j + 1]
            rhs = jnp.concatenate(
                [
                    jnp.concatenate([b00, empty, b01, empty], axis=1),
                    jnp.concatenate([empty, b10, empty, b11], axis=1),
                ],
                axis=0,
            )
            proj = mm(lhs, rhs)
            p_re, p_im = proj[:, :128], proj[:, 128:]
            offs = within[k]
            cosine, sine = unit_circle(offs * (th * (0.5 / math.pi)))
            grow = jnp.exp2(offs * (f * LOG2E)) * damps[j, k]
            fade = jnp.exp2(offs * (f * -LOG2E))
            a_re, a_im = grow * cosine, grow * sine
            lift = jnp.concatenate(
                [(a_re * p_re + a_im * p_im).astype(BF16), (a_re * p_im - a_im * p_re).astype(BF16)], axis=1
            )
            part = mm(triangles[k], lift)
            e_re, e_im = fade * cosine, fade * sine
            c_re = c_im = jnp.zeros((1, 128), F32)
            d_re, d_im = jnp.ones((1, 128), F32), jnp.zeros((1, 128), F32)
            states, prefixes = [None] * SPANS, [None] * SPANS
            for n in range(SPANS) if k == 0 else range(SPANS - 1, -1, -1):
                cut = slice(SPAN * n, SPAN * n + SPAN)
                er, ei = e_re[cut], e_im[cut]
                wr, wi = part[cut, :128] + c_re, part[cut, 128:] + c_im
                sr, si = er * wr - ei * wi, er * wi + ei * wr
                pr, pi = er * d_re - ei * d_im, er * d_im + ei * d_re
                edge = slice(SPAN - 1, SPAN) if k == 0 else slice(0, 1)
                c_re, c_im, d_re, d_im = sr[edge], si[edge], pr[edge], pi[edge]
                states[n] = jnp.concatenate([sr.astype(BF16), si.astype(BF16)], axis=1)
                prefixes[n] = jnp.concatenate([pr.astype(BF16), pi.astype(BF16)], axis=1)
            prefix_ref[j, k] = jnp.concatenate(prefixes, axis=0)
            tables = []
            for c in range(2):
                upper = jnp.concatenate([readout[k, c, 2 * j], hole], axis=1)
                lower = jnp.concatenate([hole, readout[k, c, 2 * j + 1]], axis=1)
                table = jnp.concatenate([upper, lower], axis=0)
                table_ref[j, k, c] = table
                tables.append(table)
            y = nt(
                jnp.concatenate(states, axis=0),
                jnp.concatenate([tables[0].astype(BF16), (-tables[1]).astype(BF16)], axis=1),
            )
            total = y if total is None else total + y
        outs.append(total)
    out_ref[...] = jnp.concatenate(outs, axis=1) + skip[...] * x.astype(F32)


def times_of(a, b):
    return a[0] * b[0] - a[1] * b[1], a[0] * b[1] + a[1] * b[0]


def plus(a, b):
    return a[0] + b[0], a[1] + b[1]


def pick(condition, a, b):
    return tuple(jnp.where(condition, x, y) for x, y in zip(a, b))


def my_pars(pars):
    found = []
    for k in range(2):
        angle, rate = pars[k, 0], pars[k, 1]
        high = jnp.round(angle * (4096 * 0.5 / math.pi)) * (1.0 / 4096)
        coarse = 6433 / 1024
        low = ((angle - high * coarse) - high * (2 * math.pi - coarse)) * (0.5 / math.pi)
        found.append((high, low, rate * -LOG2E))
    return found


def decay_over(span, pars):
    high, low, level = pars
    u = span * high
    cosine, sine = unit_circle((u - jnp.round(u)) + span * low, SINE, COSINE)
    fade = jnp.exp2(span * level)
    return fade * cosine, fade * sine


def states_of(ref, k):
    return ref[64 * k : 64 * k + 32, :], ref[64 * k + 32 : 64 * k + 64, :]


def keep_states(ref, k, value):
    ref[64 * k : 64 * k + 32, :], ref[64 * k + 32 : 64 * k + 64, :] = value


def span_of(ref):
    return jnp.concatenate([ref[128:136, :]] * 4, axis=0)


def trail_of(trail, at):
    return trail[2 * at], trail[2 * at + 1]


def keep_trail(trail, at, value):
    trail[2 * at], trail[2 * at + 1] = value


def upper(stage):
    axis, kind = stage
    here = lax.axis_index(axis)
    return here >= 2 if kind == "high" else here % 2 == 1


def is_behind(stage, k):
    return upper(stage) if k == 0 else jnp.logical_not(upper(stage))


def pair_kernel(own, other, pars, total_ref, trail_ref):
    mine = my_pars(pars)
    zero = jnp.zeros((32, 128), F32)
    for k in range(2):
        decay, decay_other = decay_over(span_of(own), mine[k]), decay_over(span_of(other), mine[k])
        a, b = states_of(own, k), states_of(other, k)
        total = plus(times_of(decay, b), a) if k == 0 else plus(times_of(decay_other, a), b)
        keep_states(total_ref, k, total)
        keep_trail(trail_ref, k, (zero, zero))
        keep_trail(trail_ref, 2 + k, (zero + 1.0, zero))
        keep_trail(trail_ref, 4 + k, times_of(decay, decay_other))
    total_ref[128:136, :] = own[128:136, :] + other[128:136, :]


def stage_kernel(stage, own, other, trail, pars, total_ref, trail_ref):
    mine = my_pars(pars)
    for k in range(2):
        decay, decay_other = trail_of(trail, 4 + k), decay_over(span_of(other), mine[k])
        behind = is_behind(stage, k)
        a, b = states_of(own, k), states_of(other, k)
        early, late = pick(behind, b, a), pick(behind, a, b)
        keep_states(total_ref, k, plus(times_of(pick(behind, decay, decay_other), early), late))
        state, fade = trail_of(trail, k), trail_of(trail, 2 + k)
        keep_trail(trail_ref, k, pick(behind, plus(times_of(fade, b), state), state))
        keep_trail(trail_ref, 2 + k, pick(behind, times_of(fade, decay_other), fade))
        keep_trail(trail_ref, 4 + k, times_of(decay, decay_other))
    total_ref[128:136, :] = own[128:136, :] + other[128:136, :]


def enter_kernel(stage, last, trail, own, other, pars, mine_ref, theirs_ref):
    mine = my_pars(pars)
    for k in range(2):
        state, fade = trail_of(trail, k), trail_of(trail, 2 + k)
        state = pick(is_behind(stage, k), plus(times_of(fade, states_of(last, k)), state), state)
        early = other if k == 0 else own
        later = plus(times_of(decay_over(span_of(early), mine[k]), state), states_of(early, k))
        keep_states(mine_ref, k, later if k == 0 else state)
        keep_states(theirs_ref, k, state if k == 0 else later)


def final_kernel(*refs):
    count = len(PIECES)
    own, other = refs[:2]
    nears, prefixes, tables = (refs[2 + count * n : 2 + count * n + count] for n in range(3))
    glu, glu_bias, outw, out_gain, out_ref, entering, response = refs[2 + 3 * count :]
    entering[...] = jnp.where(lax.axis_index("c") == 1, own[...], other[...])
    start = 0
    for size, near, prefix, table in zip(PIECES, nears, prefixes, tables):

        def tile(i, _, start=start, near=near, prefix=prefix, table=table):
            outs = []
            for j in range(4):
                total = None
                for k in range(2):
                    pair = 4 * (start + i) + j
                    er = entering[pl.ds(64 * k + pair, 1), :]
                    ei = entering[pl.ds(64 * k + 32 + pair, 1), :]
                    cr, ci = table[4 * i + j, k, 0], table[4 * i + j, k, 1]
                    rhs = jnp.concatenate(
                        [(cr * er - ci * ei).astype(BF16), (-(cr * ei + ci * er)).astype(BF16)], axis=1
                    )
                    y = nt(prefix[4 * i + j, k], rhs)
                    total = y if total is None else total + y
                outs.append(total)
            at = pl.multiple_of(128 * i, 128)
            response[:, pl.ds(at + 128 * start, 128)] = jnp.concatenate(outs, axis=1) + near[:, pl.ds(at, 128)]
            return 0

        lax.fori_loop(0, size, tile, 0)
        start += size
    x = response[...]
    active = 0.5 * x * (1.0 + jnp.tanh(math.sqrt(2.0 / math.pi) * (x + 0.044715 * (x * x * x))))
    gate = mm(active.astype(BF16), glu[...]) + glu_bias[...]
    gated = (active * jax.nn.sigmoid(gate)).astype(BF16)
    projected = mm(gated, outw[...])
    scale = lax.rsqrt(jnp.mean(projected * projected, axis=-1, keepdims=True) + EPSILON)
    out_ref[...] = (projected * scale * out_gain[...]).astype(BF16)


def whole(shape):
    return pl.BlockSpec(shape, lambda *_: (0,) * len(shape))


def sds(shape, dtype=F32):
    return jax.ShapeDtypeStruct(shape, dtype)


def params(limit):
    return pltpu.CompilerParams(vmem_limit_bytes=limit * 1024 * 1024)


def run_local(start, size, within, damps, driven, inputs, state_output, angle, rate, skip_row):
    row_spec = whole((2, 64, 64))
    return pl.pallas_call(
        functools.partial(local_kernel, start),
        name=f"local_{start}",
        grid=(size,),
        in_specs=[
            whole((2, ROWS, ROWS)),
            pl.BlockSpec((4, 2, ROWS, ROWS), lambda i: (i + start, 0, 0, 0)),
            pl.BlockSpec((ROWS, 128), lambda i: (0, i + start)),
            pl.BlockSpec((2, 2, 8, 16, 64), lambda i: (0, 0, i + start, 0, 0)),
            pl.BlockSpec((2, 2, 8, 16, 64), lambda i: (0, 0, i + start, 0, 0)),
            row_spec, row_spec,
            pl.BlockSpec((1, 128), lambda i: (0, i + start)),
        ],
        out_specs=[
            pl.BlockSpec((ROWS, 128), lambda i: (0, i)),
            pl.BlockSpec((4, 2, ROWS, 256), lambda i: (i, 0, 0, 0)),
            pl.BlockSpec((4, 2, 2, 32, 128), lambda i: (i, 0, 0, 0, 0)),
        ],
        out_shape=[
            sds((ROWS, 128 * size)),
            sds((4 * size, 2, ROWS, 256), BF16),
            sds((4 * size, 2, 2, 32, 128)),
        ],
        compiler_params=params(10),
        cost_estimate=pl.CostEstimate(flops=size * 5 * 10**8, bytes_accessed=size * 2 * 2**20, transcendentals=0),
    )(within, damps, driven, inputs, state_output, angle, rate, skip_row)


def simple(kernel, name, shapes, args, scratch=()):
    spec = pl.BlockSpec(memory_space=VMEM)
    return pl.pallas_call(
        kernel,
        name=name,
        in_specs=[spec] * len(args),
        out_specs=[spec] * len(shapes),
        out_shape=[sds(shape) for shape in shapes],
        scratch_shapes=scratch,
        compiler_params=params(4),
    )(*args)


def local(
    tokens, elapsed, norm_gain, in_weight, state_input, state_output, forget_rate, decay_angle,
    skip_gain, glu_weight, glu_bias, out_weight, out_gain,
):
    elapsed_row = elapsed.reshape(1, ROWS)
    inputs = jnp.swapaxes(state_input, 3, 4)
    row_spec = whole((2, 64, 64))
    driven, ends, pars, damps, within = pl.pallas_call(
        end_kernel,
        name="ends",
        grid=(TILES,),
        in_specs=[
            whole((ROWS, D)),
            whole((1, ROWS)),
            whole((1, D)),
            pl.BlockSpec((D, 128), lambda i: (0, i)),
            pl.BlockSpec((2, 2, 8, 16, 64), lambda i: (0, 0, i, 0, 0)),
            row_spec, row_spec,
        ],
        out_specs=[
            pl.BlockSpec((ROWS, 128), lambda i: (0, i)),
            whole((136, 128)),
            whole((2, 2, 32, 128)),
            pl.BlockSpec((4, 2, ROWS, ROWS), lambda i: (i, 0, 0, 0)),
            whole((2, ROWS, ROWS)),
        ],
        out_shape=[
            sds((ROWS, CHANNELS), BF16), sds((136, 128)), sds((2, 2, 32, 128)),
            sds((32, 2, ROWS, ROWS)), sds((2, ROWS, ROWS)),
        ],
        scratch_shapes=[VMEM((ROWS, D), BF16), VMEM((3, ROWS, ROWS), F32)],
        compiler_params=params(10),
    )(
        *(hbm(a) for a in (tokens, elapsed_row, norm_gain.reshape(1, D), in_weight, inputs, decay_angle, forget_rate))
    )

    skip_row = skip_gain.reshape(1, CHANNELS)
    pieces, start = [], 0

    def piece_between(before, after):
        index = len(pieces)
        start = sum(PIECES[:index])
        driven_now, _ = lax.optimization_barrier((driven, before))
        piece = run_local(
            start, PIECES[index], within, damps, driven_now, inputs, state_output, decay_angle, forget_rate, skip_row
        )
        *piece, after = lax.optimization_barrier((*piece, after))
        pieces.append(piece)
        return after

    swap = [(0, 1), (1, 0)]
    pairings = {"low": (1, 0, 3, 2), "high": (3, 2, 1, 0)}
    stages = [(axis, kind) for axis in ("y", "x", "z") for kind in ("low", "high")]
    partner = piece_between(ends, lax.ppermute(ends, "c", swap))
    total, trail = simple(pair_kernel, "pair", [(136, 128), (12, 32, 128)], (ends, partner, pars))
    for stage in stages:
        axis, kind = stage
        pairs = [pair for i, j in enumerate(pairings[kind]) for pair in ((2 * i, 2 * i), (2 * i + 1, 2 * j + 1))]
        other = piece_between(total, lax.ppermute(total, (axis, "c"), pairs))
        if stage == stages[-1]:
            mine, theirs = simple(
                functools.partial(enter_kernel, stage), "enter", [(128, 128), (128, 128)],
                (other, trail, ends, partner, pars),
            )
        else:
            total, trail = simple(
                functools.partial(stage_kernel, stage), f"stage_{axis}_{kind}", [(136, 128), (12, 32, 128)],
                (total, other, trail, pars),
            )
    other = piece_between(theirs, lax.ppermute(theirs, "c", swap))

    spec = pl.BlockSpec(memory_space=VMEM)
    args = (
        mine, other, *(p[0] for p in pieces), *(p[1] for p in pieces), *(p[2] for p in pieces),
        glu_weight, glu_bias.reshape(1, CHANNELS), out_weight, out_gain.reshape(1, D),
    )
    return pl.pallas_call(
        final_kernel,
        name="final",
        in_specs=[spec] * len(args),
        out_specs=spec,
        out_shape=sds((ROWS, D), BF16),
        scratch_shapes=[VMEM((128, 128), F32), VMEM((ROWS, CHANNELS), F32)],
        compiler_params=params(12),
    )(*args)


def hbm(x):
    return pltpu.with_memory_space_constraint(x, pltpu.HBM)


def solution(mesh):
    finer = Mesh(mesh.devices.reshape(4, 4, 4, 2), AXES)
    split = P(AXES, None)
    placed = (split, P(AXES), P(), P(), P(), P(), P(), P(), P(), P(), P(), P(), P())
    return jax.shard_map(local, mesh=finer, in_specs=placed, out_specs=split, check_vma=False)
```

```python
import functools
import math

import jax
import jax.numpy as jnp
from jax import lax
from jax.experimental import pallas as pl
from jax.experimental.pallas import tpu as pltpu
from jax.sharding import Mesh
from jax.sharding import PartitionSpec as P

ROWS = 128
D = 2048
CHANNELS = 1024
TILES = 8
SPAN = 16
SPANS = ROWS // SPAN
PIECES = (1,) * 8
LOG2E = 1.0 / math.log(2.0)
TINY = 1e-37
EPSILON = 1e-06
AXES = ("z", "x", "y", "c")
VMEM = pltpu.VMEM
F32 = jnp.float32
BF16 = jnp.bfloat16

SINE = (4.44288291, -7.30824512, 3.60634303, -0.84604096, 0.10968436)
COSINE = (1.4142135, -6.97885097, 5.73946067, -1.88355924, 0.31068962)
SINE_SHORT = (4.44287876, -7.30776104, 3.5971931, -0.7896682)
COSINE_SHORT = (1.41420407, -6.97764062, 5.71521917, -1.7282871)


def horner(coefficients, x):
    value = coefficients[-1] * x + coefficients[-2]
    for c in coefficients[-3::-1]:
        value = value * x + c
    return value


def half_turn(turns, sine=SINE_SHORT, cosine=COSINE_SHORT):
    r = turns - jnp.round(turns)
    z = r * r
    return r * horner(sine, z), horner(cosine, z)


def unit_circle(turns, *tables):
    s, c = half_turn(turns, *tables)
    return 1.0 - s * s, s * c


def nt(a, b):
    return lax.dot_general(a, b, (((1,), (1,)), ((), ())), preferred_element_type=F32)


def mm(a, b):
    return jnp.dot(a, b, preferred_element_type=F32)


def iotas(shape):
    return lax.broadcasted_iota(jnp.int32, shape, 0), lax.broadcasted_iota(jnp.int32, shape, 1)


def column_of(row):
    return jnp.broadcast_to(row, (ROWS, ROWS)).T


def in_parts(x):
    high = x.astype(BF16)
    rest = x - high.astype(F32)
    middle = rest.astype(BF16)
    return high, middle, (rest - middle.astype(F32)).astype(BF16)


def sums_of(chosen, parts):
    return sum(mm(chosen.astype(BF16), part) for part in parts)


def pair_row(ref, k, pair):
    return jnp.concatenate([ref[k, pl.ds(2 * pair, 1), :], ref[k, pl.ds(2 * pair + 1, 1), :]], axis=1)


def end_kernel(
    tokens, elapsed, gain, weight, inputs, angle, rate,
    driven_ref, ends_ref, pars_ref, damp_ref, within_ref, inputs_ref, normed, times, chunks, weight_sems, input_sems,
):
    core = lax.axis_index("c")

    def fetch(i):
        return (
            pltpu.make_async_copy(
                weight.at[:, pl.ds(pl.multiple_of(128 * i, 128), 128)], chunks.at[i], weight_sems.at[i]
            ),
            pltpu.make_async_copy(inputs.at[:, :, pl.ds(8 * i, 8)], inputs_ref.at[:, :, pl.ds(8 * i, 8)], input_sems.at[i]),
        )

    for i in range(TILES):
        for copy in fetch(i):
            copy.start()
    steps = column_of(elapsed[...])
    parts = in_parts(steps)
    row, col = iotas((ROWS, ROWS))
    same = row // SPAN == col // SPAN
    times[0] = sums_of(col > row, parts)
    times[1] = sums_of(col < row, parts)
    times[2] = steps
    within_ref[0] = sums_of((col <= row) & same, parts)
    within_ref[1] = sums_of((col >= row) & same, parts)
    total = sums_of(jnp.ones((8, ROWS), F32), parts)
    ends_ref[0, 64:] = total
    ends_ref[1, 64:] = total
    x = tokens[...].astype(F32)
    scale = lax.rsqrt(jnp.mean(x * x, axis=-1, keepdims=True) + EPSILON)
    normed[...] = (x * scale * gain[...]).astype(BF16)
    first = lax.broadcasted_iota(jnp.int32, (16, 128), 1) < 64

    def tile(step, _):
        for copy in fetch(step):
            copy.wait()
        driven = mm(normed[...], chunks[step]).astype(BF16)
        driven_ref[:, pl.ds(pl.multiple_of(128 * step, 128), 128)] = driven
        flipped = driven.astype(F32).T.astype(BF16)
        away = jnp.where((step // 4) == core, 0, 1)
        for j in range(4):
            pair = step * 4 + j
            for k in range(2):
                f = pair_row(rate, k, pair)
                th = pair_row(angle, k, pair)
                pars_ref[k, 0, pl.ds(pair, 1), :] = th
                pars_ref[k, 1, pl.ds(pair, 1), :] = f
                after = times[k]
                s, c = half_turn(after * (th * (0.5 / math.pi)))
                bend = jnp.tanh(times[2] * f)
                damp = bend * lax.rsqrt(bend * (0.5 + 0.5 * bend) + TINY)
                damp_ref[pair, k] = damp
                amp = jnp.exp2(after * (f * -LOG2E)) * damp
                tilted = amp * s
                pull = jnp.concatenate([(amp - tilted * s).astype(BF16), (tilted * c).astype(BF16)], axis=1)
                mixed = mm(flipped[32 * j : 32 * j + 32], pull)
                m_re = jnp.where(first, mixed[:16, :128], mixed[16:, :128])
                m_im = jnp.where(first, mixed[:16, 128:], mixed[16:, 128:])
                b_re, b_im = (
                    jnp.concatenate([inputs_ref[k, c, 2 * pair].astype(F32), inputs_ref[k, c, 2 * pair + 1].astype(F32)], axis=1)
                    for c in range(2)
                )
                at = 32 * k + 4 * (step % 4) + j
                ends_ref[away, pl.ds(at, 1), :] = jnp.sum(b_re * m_re - b_im * m_im, axis=0, keepdims=True)
                ends_ref[away, pl.ds(at + 16, 1), :] = jnp.sum(b_re * m_im + b_im * m_re, axis=0, keepdims=True)
        return 0

    lax.fori_loop(0, TILES, tile, 0)


def local_kernel(
    start, size, within, damps, driven, inputs, readout, angle, rate, skip,
    out_ref, prefix_ref, table_ref,
):
    row, col = iotas((ROWS, ROWS))
    same = row // SPAN == col // SPAN
    triangles = (((col <= row) & same).astype(BF16), ((col >= row) & same).astype(BF16))
    empty = jnp.zeros((16, 64), BF16)
    hole = jnp.zeros((16, 64), F32)
    x = driven[:, 32 * start : 32 * (start + size)]
    outs = []
    for j in range(size):
        pair = start + j
        lhs = x[:, 32 * j : 32 * j + 32]
        total = None
        for k in range(2):
            f = pair_row(rate, k, pair)
            th = pair_row(angle, k, pair)
            b00, b01 = inputs[k, 0, 2 * pair], inputs[k, 1, 2 * pair]
            b10, b11 = inputs[k, 0, 2 * pair + 1], inputs[k, 1, 2 * pair + 1]
            rhs = jnp.concatenate(
                [
                    jnp.concatenate([b00, empty, b01, empty], axis=1),
                    jnp.concatenate([empty, b10, empty, b11], axis=1),
                ],
                axis=0,
            )
            proj = mm(lhs, rhs)
            p_re, p_im = proj[:, :128], proj[:, 128:]
            offs = within[k]
            cosine, sine = unit_circle(offs * (th * (0.5 / math.pi)))
            grow = jnp.exp2(offs * (f * LOG2E)) * damps[pair, k]
            fade = jnp.exp2(offs * (f * -LOG2E))
            a_re, a_im = grow * cosine, grow * sine
            lift = jnp.concatenate(
                [(a_re * p_re + a_im * p_im).astype(BF16), (a_re * p_im - a_im * p_re).astype(BF16)], axis=1
            )
            part = mm(triangles[k], lift)
            e_re, e_im = fade * cosine, fade * sine
            c_re = c_im = jnp.zeros((1, 128), F32)
            d_re, d_im = jnp.ones((1, 128), F32), jnp.zeros((1, 128), F32)
            states, prefixes = [None] * SPANS, [None] * SPANS
            for n in range(SPANS) if k == 0 else range(SPANS - 1, -1, -1):
                cut = slice(SPAN * n, SPAN * n + SPAN)
                er, ei = e_re[cut], e_im[cut]
                wr, wi = part[cut, :128] + c_re, part[cut, 128:] + c_im
                sr, si = er * wr - ei * wi, er * wi + ei * wr
                pr, pi = er * d_re - ei * d_im, er * d_im + ei * d_re
                edge = slice(SPAN - 1, SPAN) if k == 0 else slice(0, 1)
                c_re, c_im, d_re, d_im = sr[edge], si[edge], pr[edge], pi[edge]
                states[n] = jnp.concatenate([sr.astype(BF16), si.astype(BF16)], axis=1)
                prefixes[n] = jnp.concatenate([pr.astype(BF16), pi.astype(BF16)], axis=1)
            prefix_ref[j, k] = jnp.concatenate(prefixes, axis=0)
            tables = []
            for c in range(2):
                upper = jnp.concatenate([readout[k, c, 2 * pair], hole], axis=1)
                lower = jnp.concatenate([hole, readout[k, c, 2 * pair + 1]], axis=1)
                table = jnp.concatenate([upper, lower], axis=0)
                table_ref[j, k, c] = table
                tables.append(table)
            y = nt(
                jnp.concatenate(states, axis=0),
                jnp.concatenate([tables[0].astype(BF16), (-tables[1]).astype(BF16)], axis=1),
            )
            total = y if total is None else total + y
        outs.append(total)
    out_ref[...] = jnp.concatenate(outs, axis=1) + skip[:, 32 * start : 32 * (start + size)] * x.astype(F32)


def times_of(a, b):
    return a[0] * b[0] - a[1] * b[1], a[0] * b[1] + a[1] * b[0]


def plus(a, b):
    return a[0] + b[0], a[1] + b[1]


def pick(condition, a, b):
    return tuple(jnp.where(condition, x, y) for x, y in zip(a, b))


def my_pars(pars):
    core = lax.axis_index("c")
    found = []
    for k in range(2):
        angle = pars[k, 0, pl.ds(16 * core, 16), :]
        rate = pars[k, 1, pl.ds(16 * core, 16), :]
        high = jnp.round(angle * (4096 * 0.5 / math.pi)) * (1.0 / 4096)
        coarse = 6433 / 1024
        low = ((angle - high * coarse) - high * (2 * math.pi - coarse)) * (0.5 / math.pi)
        found.append((high, low, rate * -LOG2E))
    return found


def decay_over(span, pars):
    high, low, level = pars
    u = span * high
    cosine, sine = unit_circle((u - jnp.round(u)) + span * low, SINE, COSINE)
    fade = jnp.exp2(span * level)
    return fade * cosine, fade * sine


def states_of(ref, k):
    return ref[32 * k : 32 * k + 16, :], ref[32 * k + 16 : 32 * k + 32, :]


def span_of(ref):
    span = ref[64:72, :]
    return jnp.concatenate([span, span], axis=0)


def keep_at(ref, at, value):
    ref[2 * at], ref[2 * at + 1] = value


def upper(stage):
    axis, kind = stage
    here = lax.axis_index(axis)
    return here >= 2 if kind == "high" else here % 2 == 1


def merge(stage, own, other, mine, total_ref, k, decay, decay_other):
    behind = upper(stage) if k == 0 else jnp.logical_not(upper(stage))
    a, b = states_of(own, k), states_of(other, k)
    early, late = pick(behind, b, a), pick(behind, a, b)
    total = plus(times_of(pick(behind, decay, decay_other), early), late)
    if total_ref is not None:
        total_ref[32 * k : 32 * k + 16, :], total_ref[32 * k + 16 : 32 * k + 32, :] = total
    return behind, b


def pair_kernel(own, other, pars, total_ref, trail_ref):
    mine = my_pars(pars)
    zero = jnp.zeros((16, 128), F32)
    for k in range(2):
        decay, decay_other = decay_over(span_of(own), mine[k]), decay_over(span_of(other), mine[k])
        merge(("c", "low"), own, other, mine, total_ref, k, decay, decay_other)
        keep_at(trail_ref, k, (zero, zero))
        keep_at(trail_ref, 2 + k, (zero + 1.0, zero))
        keep_at(trail_ref, 4 + k, times_of(decay, decay_other))
    total_ref[64:72, :] = own[64:72, :] + other[64:72, :]


def trail_of(trail, at):
    return trail[2 * at], trail[2 * at + 1]


def stage_kernel(stage, own, other, trail, pars, total_ref, trail_ref):
    mine = my_pars(pars)
    for k in range(2):
        decay, decay_other = trail_of(trail, 4 + k), decay_over(span_of(other), mine[k])
        behind, theirs = merge(stage, own, other, mine, total_ref, k, decay, decay_other)
        state, fade = trail_of(trail, k), trail_of(trail, 2 + k)
        keep_at(trail_ref, k, pick(behind, plus(times_of(fade, theirs), state), state))
        keep_at(trail_ref, 2 + k, pick(behind, times_of(fade, decay_other), fade))
        keep_at(trail_ref, 4 + k, times_of(decay, decay_other))
    total_ref[64:72, :] = own[64:72, :] + other[64:72, :]


def enter_kernel(stage, last, trail, own, other, pars, mine_ref, theirs_ref):
    core = lax.axis_index("c")
    mine = my_pars(pars)
    for k in range(2):
        behind = upper(stage) if k == 0 else jnp.logical_not(upper(stage))
        state, fade = trail_of(trail, k), trail_of(trail, 2 + k)
        state = pick(behind, plus(times_of(fade, states_of(last, k)), state), state)
        ahead = core == k
        early = pick(ahead, states_of(own, k), states_of(other, k))
        later = plus(times_of(decay_over(jnp.where(ahead, span_of(own), span_of(other)), mine[k]), state), early)
        keep_at(mine_ref, k, pick(ahead, state, later))
        keep_at(theirs_ref, k, pick(ahead, later, state))


def final_kernel(*refs):
    count = len(PIECES)
    own, other = refs[:2]
    nears, prefixes, tables = (refs[2 + count * n : 2 + count * n + count] for n in range(3))
    glu, glu_bias, outw, out_gain, out_ref, entering, response = refs[2 + 3 * count :]
    core = lax.axis_index("c")
    entering[core] = own[...]
    entering[1 - core] = other[...]
    start = 0
    for size, near, prefix, table in zip(PIECES, nears, prefixes, tables):

        def tile(i, _, start=start, near=near, prefix=prefix, table=table):
            outs = []
            for j in range(4):
                total = None
                for k in range(2):
                    pair = 4 * (start + i) + j
                    er = entering[pair // 16, 2 * k, pl.ds(pair % 16, 1), :]
                    ei = entering[pair // 16, 2 * k + 1, pl.ds(pair % 16, 1), :]
                    cr, ci = table[4 * i + j, k, 0], table[4 * i + j, k, 1]
                    rhs = jnp.concatenate(
                        [(cr * er - ci * ei).astype(BF16), (-(cr * ei + ci * er)).astype(BF16)], axis=1
                    )
                    y = nt(prefix[4 * i + j, k], rhs)
                    total = y if total is None else total + y
                outs.append(total)
            at = pl.multiple_of(128 * i, 128)
            response[:, pl.ds(at + 128 * start, 128)] = jnp.concatenate(outs, axis=1) + near[:, pl.ds(at, 128)]
            return 0

        lax.fori_loop(0, size, tile, 0)
        start += size
    x = response[...]
    active = 0.5 * x * (1.0 + jnp.tanh(math.sqrt(2.0 / math.pi) * (x + 0.044715 * (x * x * x))))
    gate = mm(active.astype(BF16), glu[...]) + glu_bias[...]
    gated = (active * jax.nn.sigmoid(gate)).astype(BF16)
    projected = mm(gated, outw[...])
    scale = lax.rsqrt(jnp.mean(projected * projected, axis=-1, keepdims=True) + EPSILON)
    out_ref[...] = (projected * scale * out_gain[...]).astype(BF16)


def sds(shape, dtype=F32):
    return jax.ShapeDtypeStruct(shape, dtype)


def params(limit):
    return pltpu.CompilerParams(vmem_limit_bytes=limit * 1024 * 1024)


def run_local(start, size, args):
    spec = pl.BlockSpec(memory_space=VMEM)
    return pl.pallas_call(
        functools.partial(local_kernel, 4 * start, 4 * size),
        name=f"local_{start}",
        in_specs=[spec] * len(args),
        out_specs=[spec] * 3,
        out_shape=[
            sds((ROWS, 128 * size)),
            sds((4 * size, 2, ROWS, 256), BF16),
            sds((4 * size, 2, 2, 32, 128)),
        ],
        compiler_params=params(6),
        cost_estimate=pl.CostEstimate(flops=size * 5 * 10**8, bytes_accessed=size * 2 * 2**20, transcendentals=0),
    )(*args)


def simple(kernel, name, shapes, args, scratch=()):
    spec = pl.BlockSpec(memory_space=VMEM)
    return pl.pallas_call(
        kernel,
        name=name,
        in_specs=[spec] * len(args),
        out_specs=[spec] * len(shapes),
        out_shape=[sds(shape) for shape in shapes],
        scratch_shapes=scratch,
        compiler_params=params(4),
    )(*args)


def local(
    tokens, elapsed, norm_gain, in_weight, state_input, state_output, forget_rate, decay_angle,
    skip_gain, glu_weight, glu_bias, out_weight, out_gain,
):
    elapsed_row = elapsed.reshape(1, ROWS)
    inputs = jnp.swapaxes(state_input, 3, 4)
    spec, distant = pl.BlockSpec(memory_space=VMEM), pl.BlockSpec(memory_space=pltpu.HBM)
    driven, ends, pars, damps, within, inputs_here = pl.pallas_call(
        end_kernel,
        name="ends",
        in_specs=[spec, spec, spec, distant, distant, spec, spec],
        out_specs=[spec] * 6,
        out_shape=[
            sds((ROWS, CHANNELS), BF16), sds((2, 72, 128)), sds((2, 2, 32, 128)),
            sds((32, 2, ROWS, ROWS)), sds((2, ROWS, ROWS)), sds((2, 2, 64, 16, 64), BF16),
        ],
        scratch_shapes=[
            VMEM((ROWS, D), BF16), VMEM((3, ROWS, ROWS), F32), VMEM((TILES, D, 128), BF16),
            pltpu.SemaphoreType.DMA((TILES,)), pltpu.SemaphoreType.DMA((TILES,)),
        ],
        compiler_params=params(12),
    )(
        *(hbm(a) for a in (tokens, elapsed_row, norm_gain.reshape(1, D), in_weight, inputs, decay_angle, forget_rate))
    )

    skip_row = skip_gain.reshape(1, CHANNELS)
    pieces, start = [], 0

    def piece_between(before, after):
        index = len(pieces)
        start = sum(PIECES[:index])
        driven_now, _ = lax.optimization_barrier((driven, before))
        piece = run_local(
            start, PIECES[index],
            (within, damps, driven_now, inputs_here, state_output, decay_angle, forget_rate, skip_row),
        )
        *piece, after = lax.optimization_barrier((*piece, after))
        pieces.append(piece)
        return after

    swap = [(0, 1), (1, 0)]
    pairings = {"low": [(0, 1), (1, 0), (2, 3), (3, 2)], "high": [(0, 3), (3, 0), (1, 2), (2, 1)]}
    stages = [(axis, kind) for axis in ("y", "x", "z") for kind in ("low", "high")]
    keep = ends[0]
    partner = piece_between(keep, lax.ppermute(ends[1], "c", swap))
    total, trail = simple(pair_kernel, "pair", [(72, 128), (12, 16, 128)], (keep, partner, pars))
    for stage in stages:
        axis, kind = stage
        other = piece_between(total, lax.ppermute(total, axis, pairings[kind]))
        if stage == stages[-1]:
            mine, theirs = simple(
                functools.partial(enter_kernel, stage), "enter", [(4, 16, 128), (4, 16, 128)],
                (other, trail, keep, partner, pars),
            )
        else:
            total, trail = simple(
                functools.partial(stage_kernel, stage), f"stage_{axis}_{kind}", [(72, 128), (12, 16, 128)],
                (total, other, trail, pars),
            )
    other = piece_between(theirs, lax.ppermute(theirs, "c", swap))

    spec = pl.BlockSpec(memory_space=VMEM)
    args = (
        mine, other, *(p[0] for p in pieces), *(p[1] for p in pieces), *(p[2] for p in pieces),
        glu_weight, glu_bias.reshape(1, CHANNELS), out_weight, out_gain.reshape(1, D),
    )
    return pl.pallas_call(
        final_kernel,
        name="final",
        in_specs=[spec] * len(args),
        out_specs=spec,
        out_shape=sds((ROWS, D), BF16),
        scratch_shapes=[VMEM((2, 4, 16, 128), F32), VMEM((ROWS, CHANNELS), F32)],
        compiler_params=params(12),
    )(*args)


def hbm(x):
    return pltpu.with_memory_space_constraint(x, pltpu.HBM)


def solution(mesh):
    finer = Mesh(mesh.devices.reshape(4, 4, 4, 2), AXES)
    split = P(AXES, None)
    placed = (split, P(AXES), P(), P(), P(), P(), P(), P(), P(), P(), P(), P(), P())
    return jax.shard_map(local, mesh=finer, in_specs=placed, out_specs=split, check_vma=False)
```

```python
import functools
import math

import jax
import jax.numpy as jnp
from jax import lax
from jax.experimental import pallas as pl
from jax.experimental.pallas import tpu as pltpu
from jax.sharding import Mesh
from jax.sharding import PartitionSpec as P

ROWS = 128
D = 2048
CHANNELS = 1024
TILES = 8
SPAN = 16
SPANS = ROWS // SPAN
PIECES = (1, 2, 2, 2, 1)
LOG2E = 1.0 / math.log(2.0)
TINY = 1e-37
EPSILON = 1e-06
AXES = ("z", "x", "y", "c")
VMEM = pltpu.VMEM
F32 = jnp.float32
BF16 = jnp.bfloat16

SINE = (4.44288291, -7.30824512, 3.60634303, -0.84604096, 0.10968436)
COSINE = (1.4142135, -6.97885097, 5.73946067, -1.88355924, 0.31068962)
SINE_SHORT = (4.44287876, -7.30776104, 3.5971931, -0.7896682)
COSINE_SHORT = (1.41420407, -6.97764062, 5.71521917, -1.7282871)


def horner(coefficients, x):
    value = coefficients[-1] * x + coefficients[-2]
    for c in coefficients[-3::-1]:
        value = value * x + c
    return value


def half_turn(turns, sine=SINE_SHORT, cosine=COSINE_SHORT):
    r = turns - jnp.round(turns)
    z = r * r
    return r * horner(sine, z), horner(cosine, z)


def unit_circle(turns, *tables):
    s, c = half_turn(turns, *tables)
    return 1.0 - s * s, s * c


def nt(a, b):
    return lax.dot_general(a, b, (((1,), (1,)), ((), ())), preferred_element_type=F32)


def mm(a, b):
    return jnp.dot(a, b, preferred_element_type=F32)


def iotas(shape):
    return lax.broadcasted_iota(jnp.int32, shape, 0), lax.broadcasted_iota(jnp.int32, shape, 1)


def column_of(row):
    return jnp.broadcast_to(row, (ROWS, ROWS)).T


def in_parts(x):
    high = x.astype(BF16)
    rest = x - high.astype(F32)
    middle = rest.astype(BF16)
    return high, middle, (rest - middle.astype(F32)).astype(BF16)


def sums_of(chosen, parts):
    return sum(mm(chosen.astype(BF16), part) for part in parts)


def pair_row(ref, k, pair):
    return jnp.concatenate([ref[k, pl.ds(2 * pair, 1), :], ref[k, pl.ds(2 * pair + 1, 1), :]], axis=1)


def end_kernel(
    tokens, elapsed, gain, weight, inputs, angle, rate,
    driven_ref, pairs_ref, ends_ref, pars_ref, damp_ref, within_ref, inputs_ref, normed, times, chunks, weight_sems, input_sems,
):
    core = lax.axis_index("c")

    def fetch(i):
        return (
            pltpu.make_async_copy(
                weight.at[:, pl.ds(pl.multiple_of(128 * i, 128), 128)], chunks.at[i], weight_sems.at[i]
            ),
            pltpu.make_async_copy(inputs.at[:, :, pl.ds(8 * i, 8)], inputs_ref.at[:, :, pl.ds(8 * i, 8)], input_sems.at[i]),
        )

    for i in range(TILES):
        for copy in fetch(i):
            copy.start()
    steps = column_of(elapsed[...])
    parts = in_parts(steps)
    row, col = iotas((ROWS, ROWS))
    same = row // SPAN == col // SPAN
    times[0] = sums_of(col > row, parts)
    times[1] = sums_of(col < row, parts)
    times[2] = steps
    within_ref[0] = sums_of((col <= row) & same, parts)
    within_ref[1] = sums_of((col >= row) & same, parts)
    total = sums_of(jnp.ones((8, ROWS), F32), parts)
    ends_ref[0, 64:] = total
    ends_ref[1, 64:] = total
    x = tokens[...].astype(F32)
    scale = lax.rsqrt(jnp.mean(x * x, axis=-1, keepdims=True) + EPSILON)
    normed[...] = (x * scale * gain[...]).astype(BF16)
    first = lax.broadcasted_iota(jnp.int32, (16, 128), 1) < 64

    def tile(step, _):
        for copy in fetch(step):
            copy.wait()
        driven = mm(normed[...], chunks[step]).astype(BF16)
        driven_ref[:, pl.ds(pl.multiple_of(128 * step, 128), 128)] = driven
        flipped = driven.astype(F32).T.astype(BF16)
        away = jnp.where((step // 4) == core, 0, 1)
        for j in range(4):
            pair = step * 4 + j
            pairs_ref[pair] = driven[:, 32 * j : 32 * j + 32]
            for k in range(2):
                f = pair_row(rate, k, pair)
                th = pair_row(angle, k, pair)
                pars_ref[k, 0, pl.ds(pair, 1), :] = th
                pars_ref[k, 1, pl.ds(pair, 1), :] = f
                after = times[k]
                s, c = half_turn(after * (th * (0.5 / math.pi)))
                bend = jnp.tanh(times[2] * f)
                damp = bend * lax.rsqrt(bend * (0.5 + 0.5 * bend) + TINY)
                damp_ref[pair, k] = damp
                amp = jnp.exp2(after * (f * -LOG2E)) * damp
                tilted = amp * s
                pull = jnp.concatenate([(amp - tilted * s).astype(BF16), (tilted * c).astype(BF16)], axis=1)
                mixed = mm(flipped[32 * j : 32 * j + 32], pull)
                m_re = jnp.where(first, mixed[:16, :128], mixed[16:, :128])
                m_im = jnp.where(first, mixed[:16, 128:], mixed[16:, 128:])
                b_re, b_im = (
                    jnp.concatenate([inputs_ref[k, c, 2 * pair].astype(F32), inputs_ref[k, c, 2 * pair + 1].astype(F32)], axis=1)
                    for c in range(2)
                )
                at = 32 * k + 4 * (step % 4) + j
                ends_ref[away, pl.ds(at, 1), :] = jnp.sum(b_re * m_re - b_im * m_im, axis=0, keepdims=True)
                ends_ref[away, pl.ds(at + 16, 1), :] = jnp.sum(b_re * m_im + b_im * m_re, axis=0, keepdims=True)
        return 0

    lax.fori_loop(0, TILES, tile, 0)


def local_kernel(
    start, size, within, damps, driven, inputs, readout, pars, out_ref, prefix_ref, table_ref, triangles,
):
    row, col = iotas((ROWS, ROWS))
    same = row // SPAN == col // SPAN
    triangles[0] = ((col <= row) & same).astype(BF16)
    triangles[1] = ((col >= row) & same).astype(BF16)
    empty = jnp.zeros((16, 64), BF16)
    hole = jnp.zeros((16, 64), F32)

    def both(j, _):
        pair = start + j
        lhs = driven[pair]
        total = None
        for k in range(2):
            th, f = pars[k, 0, pl.ds(pair, 1), :], pars[k, 1, pl.ds(pair, 1), :]
            b00, b01 = inputs[k, 0, 2 * pair], inputs[k, 1, 2 * pair]
            b10, b11 = inputs[k, 0, 2 * pair + 1], inputs[k, 1, 2 * pair + 1]
            rhs = jnp.concatenate(
                [
                    jnp.concatenate([b00, empty, b01, empty], axis=1),
                    jnp.concatenate([empty, b10, empty, b11], axis=1),
                ],
                axis=0,
            )
            proj = mm(lhs, rhs)
            p_re, p_im = proj[:, :128], proj[:, 128:]
            offs = within[k]
            cosine, sine = unit_circle(offs * (th * (0.5 / math.pi)))
            grow = jnp.exp2(offs * (f * LOG2E)) * damps[pair, k]
            fade = jnp.exp2(offs * (f * -LOG2E))
            a_re, a_im = grow * cosine, grow * sine
            lift = jnp.concatenate(
                [(a_re * p_re + a_im * p_im).astype(BF16), (a_re * p_im - a_im * p_re).astype(BF16)], axis=1
            )
            part = mm(triangles[k], lift)
            e_re, e_im = fade * cosine, fade * sine
            c_re = c_im = jnp.zeros((1, 128), F32)
            d_re, d_im = jnp.ones((1, 128), F32), jnp.zeros((1, 128), F32)
            states = [None] * SPANS
            for n in range(SPANS) if k == 0 else range(SPANS - 1, -1, -1):
                cut = slice(SPAN * n, SPAN * n + SPAN)
                er, ei = e_re[cut], e_im[cut]
                wr, wi = part[cut, :128] + c_re, part[cut, 128:] + c_im
                sr, si = er * wr - ei * wi, er * wi + ei * wr
                pr, pi = er * d_re - ei * d_im, er * d_im + ei * d_re
                edge = slice(SPAN - 1, SPAN) if k == 0 else slice(0, 1)
                c_re, c_im, d_re, d_im = sr[edge], si[edge], pr[edge], pi[edge]
                states[n] = jnp.concatenate([sr.astype(BF16), si.astype(BF16)], axis=1)
                prefix_ref[j, k, cut, :] = jnp.concatenate([pr.astype(BF16), pi.astype(BF16)], axis=1)
            tables = []
            for c in range(2):
                upper = jnp.concatenate([readout[k, c, 2 * pair], hole], axis=1)
                lower = jnp.concatenate([hole, readout[k, c, 2 * pair + 1]], axis=1)
                table = jnp.concatenate([upper, lower], axis=0)
                table_ref[j, k, c] = table
                tables.append(table)
            y = nt(
                jnp.concatenate(states, axis=0),
                jnp.concatenate([tables[0].astype(BF16), (-tables[1]).astype(BF16)], axis=1),
            )
            total = y if total is None else total + y
        out_ref[j] = total
        return 0

    lax.fori_loop(0, size, both, 0)


def times_of(a, b):
    return a[0] * b[0] - a[1] * b[1], a[0] * b[1] + a[1] * b[0]


def plus(a, b):
    return a[0] + b[0], a[1] + b[1]


def pick(condition, a, b):
    return tuple(jnp.where(condition, x, y) for x, y in zip(a, b))


def my_pars(pars):
    core = lax.axis_index("c")
    found = []
    for k in range(2):
        angle = pars[k, 0, pl.ds(16 * core, 16), :]
        rate = pars[k, 1, pl.ds(16 * core, 16), :]
        high = jnp.round(angle * (4096 * 0.5 / math.pi)) * (1.0 / 4096)
        coarse = 6433 / 1024
        low = ((angle - high * coarse) - high * (2 * math.pi - coarse)) * (0.5 / math.pi)
        found.append((high, low, rate * -LOG2E))
    return found


def decay_over(span, pars):
    high, low, level = pars
    u = span * high
    cosine, sine = unit_circle((u - jnp.round(u)) + span * low, SINE, COSINE)
    fade = jnp.exp2(span * level)
    return fade * cosine, fade * sine


def states_of(ref, k):
    return ref[32 * k : 32 * k + 16, :], ref[32 * k + 16 : 32 * k + 32, :]


def span_of(ref):
    span = ref[64:72, :]
    return jnp.concatenate([span, span], axis=0)


def keep_states(ref, k, value):
    ref[32 * k : 32 * k + 16, :], ref[32 * k + 16 : 32 * k + 32, :] = value


def keep_at(ref, at, value):
    ref[2 * at], ref[2 * at + 1] = value


def pair_kernel(own, other, pars, total_ref):
    core = lax.axis_index("c")
    mine = my_pars(pars)
    for k in range(2):
        ahead = core == k
        a, b = states_of(own, k), states_of(other, k)
        early, late = pick(ahead, a, b), pick(ahead, b, a)
        step = decay_over(jnp.where(ahead, span_of(other), span_of(own)), mine[k])
        keep_states(total_ref, k, plus(times_of(step, early), late))
    total_ref[64:72, :] = own[64:72, :] + other[64:72, :]


def gather_four(axis, own, one, two, three, data):
    here = lax.axis_index(axis)
    data[here] = own[...]
    data[here + 1 - 2 * (here % 2)] = one[...]
    data[(here + 2) % 4] = two[...]
    data[3 - here] = three[...]
    return here


def run_over(here, data, mine, k):
    zero = jnp.zeros((16, 128), F32)
    state, decay = (zero, zero), (zero + 1.0, zero)
    before, before_decay = state, decay
    for n in range(4) if k == 0 else range(3, -1, -1):
        before = pick(n == here, state, before)
        before_decay = pick(n == here, decay, before_decay)
        step = decay_over(span_of(data.at[n]), mine[k])
        state = plus(times_of(step, state), states_of(data.at[n], k))
        decay = times_of(step, decay)
    return state, before, before_decay


def group_kernel(axis, own, one, two, three, pars, total_ref, before_ref, data):
    here = gather_four(axis, own, one, two, three, data)
    mine = my_pars(pars)
    for k in range(2):
        total, before, decay = run_over(here, data, mine, k)
        keep_states(total_ref, k, total)
        keep_at(before_ref, k, before)
        keep_at(before_ref, 2 + k, decay)
    total_ref[64:72, :] = own[64:72, :] + one[64:72, :] + two[64:72, :] + three[64:72, :]


def enter_kernel(across, one, two, three, before_x, before_y, own, other, pars, mine_ref, theirs_ref, data):
    here = gather_four("z", across, one, two, three, data)
    core = lax.axis_index("c")
    mine = my_pars(pars)
    for k in range(2):
        _, state, _ = run_over(here, data, mine, k)
        for before in (before_x, before_y):
            state = plus(times_of((before[4 + 2 * k], before[5 + 2 * k]), state), (before[2 * k], before[2 * k + 1]))
        ahead = core == k
        early = pick(ahead, states_of(own, k), states_of(other, k))
        later = plus(times_of(decay_over(jnp.where(ahead, span_of(own), span_of(other)), mine[k]), state), early)
        keep_at(mine_ref, k, pick(ahead, state, later))
        keep_at(theirs_ref, k, pick(ahead, later, state))


def final_kernel(*refs):
    count = len(PIECES)
    own, other = refs[:2]
    nears, prefixes, tables = (refs[2 + count * n : 2 + count * n + count] for n in range(3))
    driven, skip, glu, glu_bias, outw, out_gain, out_ref, entering, response = refs[2 + 3 * count :]
    core = lax.axis_index("c")
    entering[core] = own[...]
    entering[1 - core] = other[...]
    start = 0
    for size, near, prefix, table in zip(PIECES, nears, prefixes, tables):

        def tile(i, _, start=start, near=near, prefix=prefix, table=table):
            outs = []
            for j in range(4):
                total = None
                for k in range(2):
                    pair = 4 * (start + i) + j
                    er = entering[pair // 16, 2 * k, pl.ds(pair % 16, 1), :]
                    ei = entering[pair // 16, 2 * k + 1, pl.ds(pair % 16, 1), :]
                    cr, ci = table[4 * i + j, k, 0], table[4 * i + j, k, 1]
                    rhs = jnp.concatenate(
                        [(cr * er - ci * ei).astype(BF16), (-(cr * ei + ci * er)).astype(BF16)], axis=1
                    )
                    y = nt(prefix[4 * i + j, k], rhs)
                    total = y if total is None else total + y
                outs.append(total + near[4 * i + j])
            at = pl.multiple_of(128 * i, 128)
            response[:, pl.ds(at + 128 * start, 128)] = jnp.concatenate(outs, axis=1)
            return 0

        lax.fori_loop(0, size, tile, 0)
        start += size
    x = response[...] + skip[...] * driven[...].astype(F32)
    active = 0.5 * x * (1.0 + jnp.tanh(math.sqrt(2.0 / math.pi) * (x + 0.044715 * (x * x * x))))
    gate = mm(active.astype(BF16), glu[...]) + glu_bias[...]
    gated = (active * jax.nn.sigmoid(gate)).astype(BF16)
    projected = mm(gated, outw[...])
    scale = lax.rsqrt(jnp.mean(projected * projected, axis=-1, keepdims=True) + EPSILON)
    out_ref[...] = (projected * scale * out_gain[...]).astype(BF16)


def sds(shape, dtype=F32):
    return jax.ShapeDtypeStruct(shape, dtype)


def params(limit):
    return pltpu.CompilerParams(vmem_limit_bytes=limit * 1024 * 1024)


def run_local(start, size, args):
    spec = pl.BlockSpec(memory_space=VMEM)
    return pl.pallas_call(
        functools.partial(local_kernel, 4 * start, 4 * size),
        name=f"local_{start}",
        in_specs=[spec] * len(args),
        out_specs=[spec] * 3,
        out_shape=[
            sds((4 * size, ROWS, 32)),
            sds((4 * size, 2, ROWS, 256), BF16),
            sds((4 * size, 2, 2, 32, 128)),
        ],
        scratch_shapes=[VMEM((2, ROWS, ROWS), BF16)],
        compiler_params=params(6),
        cost_estimate=pl.CostEstimate(flops=size * 5 * 10**8, bytes_accessed=size * 2 * 2**20, transcendentals=0),
    )(*args)


def simple(kernel, name, shapes, args, scratch=()):
    spec = pl.BlockSpec(memory_space=VMEM)
    return pl.pallas_call(
        kernel,
        name=name,
        in_specs=[spec] * len(args),
        out_specs=[spec] * len(shapes),
        out_shape=[sds(shape) for shape in shapes],
        scratch_shapes=scratch,
        compiler_params=params(4),
    )(*args)


def local(
    tokens, elapsed, norm_gain, in_weight, state_input, state_output, forget_rate, decay_angle,
    skip_gain, glu_weight, glu_bias, out_weight, out_gain,
):
    elapsed_row = elapsed.reshape(1, ROWS)
    inputs = jnp.swapaxes(state_input, 3, 4)
    spec, distant = pl.BlockSpec(memory_space=VMEM), pl.BlockSpec(memory_space=pltpu.HBM)
    driven, pairs, ends, pars, damps, within, inputs_here = pl.pallas_call(
        end_kernel,
        name="ends",
        in_specs=[spec, spec, spec, distant, distant, spec, spec],
        out_specs=[spec] * 7,
        out_shape=[
            sds((ROWS, CHANNELS), BF16), sds((32, ROWS, 32), BF16), sds((2, 72, 128)), sds((2, 2, 32, 128)),
            sds((32, 2, ROWS, ROWS)), sds((2, ROWS, ROWS)), sds((2, 2, 64, 16, 64), BF16),
        ],
        scratch_shapes=[
            VMEM((ROWS, D), BF16), VMEM((3, ROWS, ROWS), F32), VMEM((TILES, D, 128), BF16),
            pltpu.SemaphoreType.DMA((TILES,)), pltpu.SemaphoreType.DMA((TILES,)),
        ],
        compiler_params=params(12),
    )(
        *(hbm(a) for a in (tokens, elapsed_row, norm_gain.reshape(1, D), in_weight, inputs, decay_angle, forget_rate))
    )

    pieces, start = [], 0

    def piece_between(before, after):
        index = len(pieces)
        start = sum(PIECES[:index])
        pairs_now, _ = lax.optimization_barrier((pairs, before))
        piece = run_local(
            start, PIECES[index],
            (within, damps, pairs_now, inputs_here, state_output, pars),
        )
        *piece, after = lax.optimization_barrier((*piece, after))
        pieces.append(piece)
        return after

    swap = [(0, 1), (1, 0)]
    swaps = ([(0, 1), (1, 0), (2, 3), (3, 2)], [(0, 2), (2, 0), (1, 3), (3, 1)], [(0, 3), (3, 0), (1, 2), (2, 1)])
    four = VMEM((4, 72, 128), F32)
    keep = ends[0]
    partner = piece_between(keep, lax.ppermute(ends[1], "c", swap))
    (total,) = simple(pair_kernel, "pair", [(72, 128)], (keep, partner, pars))
    befores = []
    for axis in ("y", "x"):
        others = piece_between(total, tuple(lax.ppermute(total, axis, pairs) for pairs in swaps))
        total, before = simple(
            functools.partial(group_kernel, axis), f"group_{axis}", [(72, 128), (8, 16, 128)],
            (total, *others, pars), [four],
        )
        befores.append(before)
    others = piece_between(total, tuple(lax.ppermute(total, "z", pairs) for pairs in swaps))
    mine, theirs = simple(
        enter_kernel, "enter", [(4, 16, 128), (4, 16, 128)],
        (total, *others, befores[1], befores[0], keep, partner, pars), [four],
    )
    other = piece_between(theirs, lax.ppermute(theirs, "c", swap))

    spec = pl.BlockSpec(memory_space=VMEM)
    args = (
        mine, other, *(p[0] for p in pieces), *(p[1] for p in pieces), *(p[2] for p in pieces),
        driven, skip_gain.reshape(1, CHANNELS), glu_weight, glu_bias.reshape(1, CHANNELS), out_weight, out_gain.reshape(1, D),
    )
    return pl.pallas_call(
        final_kernel,
        name="final",
        in_specs=[spec] * len(args),
        out_specs=spec,
        out_shape=sds((ROWS, D), BF16),
        scratch_shapes=[VMEM((2, 4, 16, 128), F32), VMEM((ROWS, CHANNELS), F32)],
        compiler_params=params(12),
    )(*args)


def hbm(x):
    return pltpu.with_memory_space_constraint(x, pltpu.HBM)


def solution(mesh):
    finer = Mesh(mesh.devices.reshape(4, 4, 4, 2), AXES)
    split = P(AXES, None)
    placed = (split, P(AXES), P(), P(), P(), P(), P(), P(), P(), P(), P(), P(), P())
    return jax.shard_map(local, mesh=finer, in_specs=placed, out_specs=split, check_vma=False)
```

```python
import functools
import math

import jax
import jax.numpy as jnp
from jax import lax
from jax.experimental import pallas as pl
from jax.experimental.pallas import tpu as pltpu
from jax.sharding import Mesh
from jax.sharding import PartitionSpec as P

ROWS = 128
D = 2048
CHANNELS = 1024
CHUNKS = 4
LAG = 10
DRIVE_AT = (6, 16, 32, 48)
SPAN = 16
SPANS = ROWS // SPAN
SLOTS = 6
PIECES = (1, 2, 2, 2, 1)
LOG2E = 1.0 / math.log(2.0)
TINY = 1e-37
EPSILON = 1e-06
AXES = ("z", "x", "y", "c")
VMEM = pltpu.VMEM
F32 = jnp.float32
BF16 = jnp.bfloat16

SINE = (4.44288291, -7.30824512, 3.60634303, -0.84604096, 0.10968436)
COSINE = (1.4142135, -6.97885097, 5.73946067, -1.88355924, 0.31068962)
SINE_SHORT = (4.44287876, -7.30776104, 3.5971931, -0.7896682)
COSINE_SHORT = (1.41420407, -6.97764062, 5.71521917, -1.7282871)


def horner(coefficients, x):
    value = coefficients[-1] * x + coefficients[-2]
    for c in coefficients[-3::-1]:
        value = value * x + c
    return value


def half_turn(turns, sine=SINE_SHORT, cosine=COSINE_SHORT):
    r = turns - jnp.round(turns)
    z = r * r
    return r * horner(sine, z), horner(cosine, z)


def unit_circle(turns, *tables):
    s, c = half_turn(turns, *tables)
    return 1.0 - s * s, s * c


def nt(a, b):
    return lax.dot_general(a, b, (((1,), (1,)), ((), ())), preferred_element_type=F32)


def mm(a, b):
    return jnp.dot(a, b, preferred_element_type=F32)


def iotas(shape):
    return lax.broadcasted_iota(jnp.int32, shape, 0), lax.broadcasted_iota(jnp.int32, shape, 1)


def column_of(row):
    return jnp.broadcast_to(row, (ROWS, ROWS)).T


def in_parts(x):
    high = x.astype(BF16)
    rest = x - high.astype(F32)
    middle = rest.astype(BF16)
    return high, middle, (rest - middle.astype(F32)).astype(BF16)


def sums_of(chosen, parts):
    return sum(mm(chosen.astype(BF16), part) for part in parts)


def pair_row(ref, k, pair):
    return jnp.concatenate([ref[k, pl.ds(2 * pair, 1), :], ref[k, pl.ds(2 * pair + 1, 1), :]], axis=1)


def end_kernel(
    tokens, elapsed, gain, weight, inputs, angle, rate,
    driven_ref, pairs_ref, ends_ref, pars_ref, damp_ref, within_ref, inputs_ref, normed, times, chunks, flipped, pulls, weight_sems, input_sems,
):
    core = lax.axis_index("c")

    def fetch(i):
        return (
            pltpu.make_async_copy(
                weight.at[:, pl.ds(256 * i, 256)], chunks.at[i], weight_sems.at[i]
            ),
            pltpu.make_async_copy(inputs.at[:, :, pl.ds(16 * i, 16)], inputs_ref.at[:, :, pl.ds(16 * i, 16)], input_sems.at[i]),
        )

    for i in range(CHUNKS):
        for copy in fetch(i):
            copy.start()
    steps = column_of(elapsed[...])
    parts = in_parts(steps)
    row, col = iotas((ROWS, ROWS))
    same = row // SPAN == col // SPAN
    times[0] = sums_of(col > row, parts)
    times[1] = sums_of(col < row, parts)
    times[2] = steps
    within_ref[0] = sums_of((col <= row) & same, parts)
    within_ref[1] = sums_of((col >= row) & same, parts)
    total = sums_of(jnp.ones((8, ROWS), F32), parts)
    ends_ref[0, 64:] = total
    ends_ref[1, 64:] = total
    x = tokens[...].astype(F32)
    scale = lax.rsqrt(jnp.mean(x * x, axis=-1, keepdims=True) + EPSILON)
    normed[...] = (x * scale * gain[...]).astype(BF16)
    first = lax.broadcasted_iota(jnp.int32, (16, 128), 1) < 64

    def drive(step):
        for copy in fetch(step):
            copy.wait()
        driven = mm(normed[...], chunks[step]).astype(BF16)
        driven_ref[:, 256 * step : 256 * step + 256] = driven
        for j in range(8):
            pairs_ref[8 * step + j] = driven[:, 32 * j : 32 * j + 32]
        flipped[step % 2] = driven.astype(F32).T.astype(BF16)

    def pull(pair, k):
        f = pair_row(rate, k, pair)
        th = pair_row(angle, k, pair)
        pars_ref[k, 0, pair : pair + 1, :] = th
        pars_ref[k, 1, pair : pair + 1, :] = f
        after = times[k]
        s, c = half_turn(after * (th * (0.5 / math.pi)))
        bend = jnp.tanh(times[2] * f)
        damp = bend * lax.rsqrt(bend * (0.5 + 0.5 * bend) + TINY)
        damp_ref[pair, k] = damp
        amp = jnp.exp2(after * (f * -LOG2E)) * damp
        tilted = amp * s
        pulls[pair % 8, k, :, :128] = (amp - tilted * s).astype(BF16)
        pulls[pair % 8, k, :, 128:] = (tilted * c).astype(BF16)

    def finish(pair, k):
        mixed = mm(flipped[pair // 8 % 2, 32 * (pair % 8) : 32 * (pair % 8) + 32], pulls[pair % 8, k])
        m_re = jnp.where(first, mixed[:16, :128], mixed[16:, :128])
        m_im = jnp.where(first, mixed[:16, 128:], mixed[16:, 128:])
        b_re, b_im = (
            jnp.concatenate([inputs_ref[k, c, 2 * pair].astype(F32), inputs_ref[k, c, 2 * pair + 1].astype(F32)], axis=1)
            for c in range(2)
        )
        away = jnp.where(pair // 16 == core, 0, 1)
        at = 32 * k + pair % 16
        ends_ref[away, at : at + 1, :] = jnp.sum(b_re * m_re - b_im * m_im, axis=0, keepdims=True)
        ends_ref[away, at + 16 : at + 17, :] = jnp.sum(b_re * m_im + b_im * m_re, axis=0, keepdims=True)

    units = [(pair, k) for pair in range(32) for k in range(2)]
    for n in range(len(units) + LAG):
        if n in DRIVE_AT:
            drive(DRIVE_AT.index(n))
        if n < len(units):
            pull(*units[n])
        if n >= LAG:
            finish(*units[n - LAG])


def shifted_rows(x, by, fill):
    row = lax.broadcasted_iota(jnp.int32, (SPANS, 128), 0)
    moved = pltpu.roll(x, by % SPANS, 0)
    return jnp.where(row >= by if by > 0 else row < SPANS + by, moved, fill)


def local_kernel(
    start, size, within, damps, driven, inputs, readout, pars, out_ref, prefix_ref, table_ref,
    triangles, proj, turn, lifts, part, states, carry,
):
    row, col = iotas((ROWS, ROWS))
    same = row // SPAN == col // SPAN
    triangles[0] = ((col <= row) & same).astype(BF16)
    triangles[1] = ((col >= row) & same).astype(BF16)
    empty = jnp.zeros((16, 64), BF16)
    hole = jnp.zeros((16, 64), F32)

    def project(j, k, slot):
        pair = start + j
        b00, b01 = inputs[k, 0, 2 * pair], inputs[k, 1, 2 * pair]
        b10, b11 = inputs[k, 0, 2 * pair + 1], inputs[k, 1, 2 * pair + 1]
        rhs = jnp.concatenate(
            [
                jnp.concatenate([b00, empty, b01, empty], axis=1),
                jnp.concatenate([empty, b10, empty, b11], axis=1),
            ],
            axis=0,
        )
        proj[slot] = mm(driven[pair], rhs)

    def lift(j, k, slot):
        pair = start + j
        th, f = pars[k, 0, pair : pair + 1, :], pars[k, 1, pair : pair + 1, :]
        offs = within[k]
        cosine, sine = unit_circle(offs * (th * (0.5 / math.pi)))
        grow = jnp.exp2(offs * (f * LOG2E)) * damps[pair, k]
        fade = jnp.exp2(offs * (f * -LOG2E))
        turn[slot, 0], turn[slot, 1] = fade * cosine, fade * sine
        a_re, a_im = grow * cosine, grow * sine
        p_re, p_im = proj[slot, :, :128], proj[slot, :, 128:]
        lifts[slot, :, :128] = (a_re * p_re + a_im * p_im).astype(BF16)
        lifts[slot, :, 128:] = (a_re * p_im - a_im * p_re).astype(BF16)

    def add_up(j, k, slot):
        total = mm(triangles[k], lifts[slot])
        part[slot, 0], part[slot, 1] = total[:, :128], total[:, 128:]

    def carry_on(j, k, slot):
        edge = pl.ds(SPAN - 1 if k == 0 else 0, SPANS, stride=SPAN)
        d = turn[slot, 0, edge, :], turn[slot, 1, edge, :]
        s = times_of(d, (part[slot, 0, edge, :], part[slot, 1, edge, :]))
        sign = 1 if k == 0 else -1
        for by in (1, 2, 4):
            s_old = tuple(shifted_rows(x, sign * by, 0.0) for x in s)
            d_old = shifted_rows(d[0], sign * by, 1.0), shifted_rows(d[1], sign * by, 0.0)
            s = plus(times_of(d, s_old), s)
            d = times_of(d, d_old)
        carry[slot, 0], carry[slot, 1] = (shifted_rows(x, sign, 0.0) for x in s)
        carry[slot, 2], carry[slot, 3] = shifted_rows(d[0], sign, 1.0), shifted_rows(d[1], sign, 0.0)

    def spread(j, k, slot):
        for n in range(SPANS):
            cut = slice(SPAN * n, SPAN * n + SPAN)
            e = turn[slot, 0, cut, :], turn[slot, 1, cut, :]
            c_re, c_im, d_re, d_im = (jnp.broadcast_to(carry[slot, i, n : n + 1, :], (SPAN, 128)) for i in range(4))
            state = times_of(e, (part[slot, 0, cut, :] + c_re, part[slot, 1, cut, :] + c_im))
            states[j % 2, cut, 256 * k : 256 * k + 128] = state[0].astype(BF16)
            states[j % 2, cut, 256 * k + 128 : 256 * k + 256] = state[1].astype(BF16)
            prefix = times_of(e, (d_re, d_im))
            prefix_ref[j, k, cut, :128] = prefix[0].astype(BF16)
            prefix_ref[j, k, cut, 128:] = prefix[1].astype(BF16)

    def read(j):
        pair = start + j
        tables = []
        for k in range(2):
            for c in range(2):
                upper = jnp.concatenate([readout[k, c, 2 * pair], hole], axis=1)
                lower = jnp.concatenate([hole, readout[k, c, 2 * pair + 1]], axis=1)
                table = jnp.concatenate([upper, lower], axis=0)
                table_ref[j, k, c] = table
                tables.append((table if c == 0 else -table).astype(BF16))
        out_ref[j] = nt(states[j % 2], jnp.concatenate(tables, axis=1))

    units = [(j, k) for j in range(size) for k in range(2)]
    for turn_of in range(len(units) + 6):
        for late, act in ((0, project), (1, lift), (2, add_up), (3, carry_on), (4, spread)):
            at = turn_of - late
            if 0 <= at < len(units):
                act(*units[at], at % SLOTS)
        at = turn_of - 5
        if 0 <= at < len(units) and units[at][1] == 1:
            read(units[at][0])


def times_of(a, b):
    return a[0] * b[0] - a[1] * b[1], a[0] * b[1] + a[1] * b[0]


def plus(a, b):
    return a[0] + b[0], a[1] + b[1]


def pick(condition, a, b):
    return tuple(jnp.where(condition, x, y) for x, y in zip(a, b))


def my_pars(pars):
    core = lax.axis_index("c")
    found = []
    for k in range(2):
        angle = pars[k, 0, pl.ds(16 * core, 16), :]
        rate = pars[k, 1, pl.ds(16 * core, 16), :]
        high = jnp.round(angle * (4096 * 0.5 / math.pi)) * (1.0 / 4096)
        coarse = 6433 / 1024
        low = ((angle - high * coarse) - high * (2 * math.pi - coarse)) * (0.5 / math.pi)
        found.append((high, low, rate * -LOG2E))
    return found


def decay_over(span, pars):
    high, low, level = pars
    u = span * high
    cosine, sine = unit_circle((u - jnp.round(u)) + span * low, SINE, COSINE)
    fade = jnp.exp2(span * level)
    return fade * cosine, fade * sine


def states_of(ref, k):
    return ref[32 * k : 32 * k + 16, :], ref[32 * k + 16 : 32 * k + 32, :]


def span_of(ref):
    span = ref[64:72, :]
    return jnp.concatenate([span, span], axis=0)


def keep_states(ref, k, value):
    ref[32 * k : 32 * k + 16, :], ref[32 * k + 16 : 32 * k + 32, :] = value


def keep_at(ref, at, value):
    ref[2 * at], ref[2 * at + 1] = value


def pair_kernel(own, other, pars, total_ref):
    core = lax.axis_index("c")
    mine = my_pars(pars)
    for k in range(2):
        ahead = core == k
        a, b = states_of(own, k), states_of(other, k)
        early, late = pick(ahead, a, b), pick(ahead, b, a)
        step = decay_over(jnp.where(ahead, span_of(other), span_of(own)), mine[k])
        keep_states(total_ref, k, plus(times_of(step, early), late))
    total_ref[64:72, :] = own[64:72, :] + other[64:72, :]


def gather_four(axis, own, one, two, three, data):
    here = lax.axis_index(axis)
    data[here] = own[...]
    data[here + 1 - 2 * (here % 2)] = one[...]
    data[(here + 2) % 4] = two[...]
    data[3 - here] = three[...]
    return here


def run_over(here, data, mine, k):
    zero = jnp.zeros((16, 128), F32)
    state, decay = (zero, zero), (zero + 1.0, zero)
    before, before_decay = state, decay
    for n in range(4) if k == 0 else range(3, -1, -1):
        before = pick(n == here, state, before)
        before_decay = pick(n == here, decay, before_decay)
        step = decay_over(span_of(data.at[n]), mine[k])
        state = plus(times_of(step, state), states_of(data.at[n], k))
        decay = times_of(step, decay)
    return state, before, before_decay


def group_kernel(axis, own, one, two, three, pars, total_ref, before_ref, data):
    here = gather_four(axis, own, one, two, three, data)
    mine = my_pars(pars)
    for k in range(2):
        total, before, decay = run_over(here, data, mine, k)
        keep_states(total_ref, k, total)
        keep_at(before_ref, k, before)
        keep_at(before_ref, 2 + k, decay)
    total_ref[64:72, :] = own[64:72, :] + one[64:72, :] + two[64:72, :] + three[64:72, :]


def enter_kernel(across, one, two, three, before_x, before_y, own, other, pars, mine_ref, theirs_ref, data):
    here = gather_four("z", across, one, two, three, data)
    core = lax.axis_index("c")
    mine = my_pars(pars)
    for k in range(2):
        _, state, _ = run_over(here, data, mine, k)
        for before in (before_x, before_y):
            state = plus(times_of((before[4 + 2 * k], before[5 + 2 * k]), state), (before[2 * k], before[2 * k + 1]))
        ahead = core == k
        early = pick(ahead, states_of(own, k), states_of(other, k))
        later = plus(times_of(decay_over(jnp.where(ahead, span_of(own), span_of(other)), mine[k]), state), early)
        keep_at(mine_ref, k, pick(ahead, state, later))
        keep_at(theirs_ref, k, pick(ahead, later, state))


def final_kernel(*refs):
    count = len(PIECES)
    own, other = refs[:2]
    nears, prefixes, tables = (refs[2 + count * n : 2 + count * n + count] for n in range(3))
    driven, skip, glu, glu_bias, outw, out_gain, out_ref, entering, response = refs[2 + 3 * count :]
    core = lax.axis_index("c")
    entering[core] = own[...]
    entering[1 - core] = other[...]
    start = 0
    for size, near, prefix, table in zip(PIECES, nears, prefixes, tables):

        def tile(i, start=start, near=near, prefix=prefix, table=table):
            outs = []
            for j in range(4):
                total = None
                for k in range(2):
                    pair = 4 * (start + i) + j
                    er = entering[pair // 16, 2 * k, pl.ds(pair % 16, 1), :]
                    ei = entering[pair // 16, 2 * k + 1, pl.ds(pair % 16, 1), :]
                    cr, ci = table[4 * i + j, k, 0], table[4 * i + j, k, 1]
                    rhs = jnp.concatenate(
                        [(cr * er - ci * ei).astype(BF16), (-(cr * ei + ci * er)).astype(BF16)], axis=1
                    )
                    y = nt(prefix[4 * i + j, k], rhs)
                    total = y if total is None else total + y
                outs.append(total + near[4 * i + j])
            at = 128 * i
            response[:, pl.ds(at + 128 * start, 128)] = jnp.concatenate(outs, axis=1)

        for i in range(size):
            tile(i)
        start += size
    x = response[...] + skip[...] * driven[...].astype(F32)
    active = 0.5 * x * (1.0 + jnp.tanh(math.sqrt(2.0 / math.pi) * (x + 0.044715 * (x * x * x))))
    gate = mm(active.astype(BF16), glu[...]) + glu_bias[...]
    gated = (active * jax.nn.sigmoid(gate)).astype(BF16)
    projected = mm(gated, outw[...])
    scale = lax.rsqrt(jnp.mean(projected * projected, axis=-1, keepdims=True) + EPSILON)
    out_ref[...] = (projected * scale * out_gain[...]).astype(BF16)


def sds(shape, dtype=F32):
    return jax.ShapeDtypeStruct(shape, dtype)


def params(limit):
    return pltpu.CompilerParams(vmem_limit_bytes=limit * 1024 * 1024)


def run_local(start, size, args):
    spec = pl.BlockSpec(memory_space=VMEM)
    return pl.pallas_call(
        functools.partial(local_kernel, 4 * start, 4 * size),
        name=f"local_{start}",
        in_specs=[spec] * len(args),
        out_specs=[spec] * 3,
        out_shape=[
            sds((4 * size, ROWS, 32)),
            sds((4 * size, 2, ROWS, 256), BF16),
            sds((4 * size, 2, 2, 32, 128)),
        ],
        scratch_shapes=[
            VMEM((2, ROWS, ROWS), BF16), VMEM((SLOTS, ROWS, 256), F32), VMEM((SLOTS, 2, ROWS, 128), F32),
            VMEM((SLOTS, ROWS, 256), BF16), VMEM((SLOTS, 2, ROWS, 128), F32), VMEM((2, ROWS, 512), BF16),
            VMEM((SLOTS, 4, SPANS, 128), F32),
        ],
        compiler_params=params(8),
        cost_estimate=pl.CostEstimate(flops=size * 5 * 10**8, bytes_accessed=size * 2 * 2**20, transcendentals=0),
    )(*args)


def simple(kernel, name, shapes, args, scratch=()):
    spec = pl.BlockSpec(memory_space=VMEM)
    return pl.pallas_call(
        kernel,
        name=name,
        in_specs=[spec] * len(args),
        out_specs=[spec] * len(shapes),
        out_shape=[sds(shape) for shape in shapes],
        scratch_shapes=scratch,
        compiler_params=params(4),
    )(*args)


def local(
    tokens, elapsed, norm_gain, in_weight, state_input, state_output, forget_rate, decay_angle,
    skip_gain, glu_weight, glu_bias, out_weight, out_gain,
):
    elapsed_row = elapsed.reshape(1, ROWS)
    inputs = jnp.swapaxes(state_input, 3, 4)
    spec, distant = pl.BlockSpec(memory_space=VMEM), pl.BlockSpec(memory_space=pltpu.HBM)
    driven, pairs, ends, pars, damps, within, inputs_here = pl.pallas_call(
        end_kernel,
        name="ends",
        in_specs=[spec, spec, spec, distant, distant, spec, spec],
        out_specs=[spec] * 7,
        out_shape=[
            sds((ROWS, CHANNELS), BF16), sds((32, ROWS, 32), BF16), sds((2, 72, 128)), sds((2, 2, 32, 128)),
            sds((32, 2, ROWS, ROWS)), sds((2, ROWS, ROWS)), sds((2, 2, 64, 16, 64), BF16),
        ],
        scratch_shapes=[
            VMEM((ROWS, D), BF16), VMEM((3, ROWS, ROWS), F32), VMEM((CHUNKS, D, 256), BF16), VMEM((2, 256, ROWS), BF16),
            VMEM((8, 2, ROWS, 256), BF16),
            pltpu.SemaphoreType.DMA((CHUNKS,)), pltpu.SemaphoreType.DMA((CHUNKS,)),
        ],
        compiler_params=params(12),
    )(
        *(hbm(a) for a in (tokens, elapsed_row, norm_gain.reshape(1, D), in_weight, inputs, decay_angle, forget_rate))
    )

    pieces, start = [], 0

    def piece_between(before, after):
        index = len(pieces)
        start = sum(PIECES[:index])
        pairs_now, _ = lax.optimization_barrier((pairs, before))
        piece = run_local(
            start, PIECES[index],
            (within, damps, pairs_now, inputs_here, state_output, pars),
        )
        *piece, after = lax.optimization_barrier((*piece, after))
        pieces.append(piece)
        return after

    swap = [(0, 1), (1, 0)]
    swaps = ([(0, 1), (1, 0), (2, 3), (3, 2)], [(0, 2), (2, 0), (1, 3), (3, 1)], [(0, 3), (3, 0), (1, 2), (2, 1)])
    four = VMEM((4, 72, 128), F32)
    keep = ends[0]
    partner = piece_between(keep, lax.ppermute(ends[1], "c", swap))
    (total,) = simple(pair_kernel, "pair", [(72, 128)], (keep, partner, pars))
    befores = []
    for axis in ("y", "x"):
        others = piece_between(total, tuple(lax.ppermute(total, axis, pairs) for pairs in swaps))
        total, before = simple(
            functools.partial(group_kernel, axis), f"group_{axis}", [(72, 128), (8, 16, 128)],
            (total, *others, pars), [four],
        )
        befores.append(before)
    others = piece_between(total, tuple(lax.ppermute(total, "z", pairs) for pairs in swaps))
    mine, theirs = simple(
        enter_kernel, "enter", [(4, 16, 128), (4, 16, 128)],
        (total, *others, befores[1], befores[0], keep, partner, pars), [four],
    )
    other = piece_between(theirs, lax.ppermute(theirs, "c", swap))

    spec = pl.BlockSpec(memory_space=VMEM)
    args = (
        mine, other, *(p[0] for p in pieces), *(p[1] for p in pieces), *(p[2] for p in pieces),
        driven, skip_gain.reshape(1, CHANNELS), glu_weight, glu_bias.reshape(1, CHANNELS), out_weight, out_gain.reshape(1, D),
    )
    return pl.pallas_call(
        final_kernel,
        name="final",
        in_specs=[spec] * len(args),
        out_specs=spec,
        out_shape=sds((ROWS, D), BF16),
        scratch_shapes=[VMEM((2, 4, 16, 128), F32), VMEM((ROWS, CHANNELS), F32)],
        compiler_params=params(12),
    )(*args)


def hbm(x):
    return pltpu.with_memory_space_constraint(x, pltpu.HBM)


def solution(mesh):
    finer = Mesh(mesh.devices.reshape(4, 4, 4, 2), AXES)
    split = P(AXES, None)
    placed = (split, P(AXES), P(), P(), P(), P(), P(), P(), P(), P(), P(), P(), P())
    return jax.shard_map(local, mesh=finer, in_specs=placed, out_specs=split, check_vma=False)
```

```python
import functools
import math

import jax
import jax.numpy as jnp
from jax import lax
from jax.experimental import pallas as pl
from jax.experimental.pallas import tpu as pltpu
from jax.sharding import Mesh
from jax.sharding import PartitionSpec as P

ROWS = 128
D = 2048
CHANNELS = 1024
CHUNKS = 4
LAG = 10
DRIVE_AT = (6, 16, 32, 48)
SPAN = 16
SPANS = ROWS // SPAN
SLOTS = 6
PIECES = (1, 2, 2, 2, 1)
LOG2E = 1.0 / math.log(2.0)
TINY = 1e-37
EPSILON = 1e-06
AXES = ("z", "x", "y", "c")
VMEM = pltpu.VMEM
F32 = jnp.float32
BF16 = jnp.bfloat16

SINE = (4.44288291, -7.30824512, 3.60634303, -0.84604096, 0.10968436)
COSINE = (1.4142135, -6.97885097, 5.73946067, -1.88355924, 0.31068962)
SINE_SHORT = (4.44287876, -7.30776104, 3.5971931, -0.7896682)
COSINE_SHORT = (1.41420407, -6.97764062, 5.71521917, -1.7282871)


def horner(coefficients, x):
    value = coefficients[-1] * x + coefficients[-2]
    for c in coefficients[-3::-1]:
        value = value * x + c
    return value


def half_turn(turns, sine=SINE_SHORT, cosine=COSINE_SHORT):
    r = turns - jnp.round(turns)
    z = r * r
    return r * horner(sine, z), horner(cosine, z)


def unit_circle(turns, *tables):
    s, c = half_turn(turns, *tables)
    return 1.0 - s * s, s * c


def nt(a, b):
    return lax.dot_general(a, b, (((1,), (1,)), ((), ())), preferred_element_type=F32)


def mm(a, b):
    return jnp.dot(a, b, preferred_element_type=F32)


def iotas(shape):
    return lax.broadcasted_iota(jnp.int32, shape, 0), lax.broadcasted_iota(jnp.int32, shape, 1)


def column_of(row):
    return jnp.broadcast_to(row, (ROWS, ROWS)).T


def in_parts(x):
    high = x.astype(BF16)
    rest = x - high.astype(F32)
    middle = rest.astype(BF16)
    return high, middle, (rest - middle.astype(F32)).astype(BF16)


def sums_of(chosen, parts):
    return sum(mm(chosen.astype(BF16), part) for part in parts)


def pair_row(ref, k, pair):
    return jnp.concatenate([ref[k, pl.ds(2 * pair, 1), :], ref[k, pl.ds(2 * pair + 1, 1), :]], axis=1)


def end_kernel(
    tokens, elapsed, gain, weight, inputs, angle, rate,
    driven_ref, pairs_ref, ends_ref, pars_ref, damp_ref, within_ref, inputs_ref, normed, times, chunks, flipped, pulls, weight_sems, input_sems,
):
    core = lax.axis_index("c")

    def fetch(i):
        return (
            pltpu.make_async_copy(
                weight.at[:, pl.ds(256 * i, 256)], chunks.at[i], weight_sems.at[i]
            ),
            pltpu.make_async_copy(inputs.at[:, :, pl.ds(16 * i, 16)], inputs_ref.at[:, :, pl.ds(16 * i, 16)], input_sems.at[i]),
        )

    for i in range(CHUNKS):
        for copy in fetch(i):
            copy.start()
    steps = column_of(elapsed[...])
    parts = in_parts(steps)
    row, col = iotas((ROWS, ROWS))
    same = row // SPAN == col // SPAN
    times[0] = sums_of(col > row, parts)
    times[1] = sums_of(col < row, parts)
    times[2] = steps
    within_ref[0] = sums_of((col <= row) & same, parts)
    within_ref[1] = sums_of((col >= row) & same, parts)
    total = sums_of(jnp.ones((8, ROWS), F32), parts)
    ends_ref[0, 64:] = total
    ends_ref[1, 64:] = total
    for r in range(0, ROWS, 16):
        x = tokens[r : r + 16, :].astype(F32)
        scale = lax.rsqrt(jnp.mean(x * x, axis=-1, keepdims=True) + EPSILON)
        normed[r : r + 16, :] = (x * scale * gain[...]).astype(BF16)
    first = lax.broadcasted_iota(jnp.int32, (16, 128), 1) < 64

    def drive(step):
        for copy in fetch(step):
            copy.wait()
        driven = mm(normed[...], chunks[step]).astype(BF16)
        driven_ref[:, 256 * step : 256 * step + 256] = driven
        for j in range(8):
            pairs_ref[8 * step + j] = driven[:, 32 * j : 32 * j + 32]
        flipped[step % 2] = driven.astype(F32).T.astype(BF16)

    def pull(pair, k):
        f = pair_row(rate, k, pair)
        th = pair_row(angle, k, pair)
        pars_ref[k, 0, pair : pair + 1, :] = th
        pars_ref[k, 1, pair : pair + 1, :] = f
        after = times[k]
        s, c = half_turn(after * (th * (0.5 / math.pi)))
        bend = jnp.tanh(times[2] * f)
        damp = bend * lax.rsqrt(bend * (0.5 + 0.5 * bend) + TINY)
        damp_ref[pair, k] = damp
        amp = jnp.exp2(after * (f * -LOG2E)) * damp
        tilted = amp * s
        pulls[pair % 8, k, :, :128] = (amp - tilted * s).astype(BF16)
        pulls[pair % 8, k, :, 128:] = (tilted * c).astype(BF16)

    def finish(pair, k):
        mixed = mm(flipped[pair // 8 % 2, 32 * (pair % 8) : 32 * (pair % 8) + 32], pulls[pair % 8, k])
        m_re = jnp.where(first, mixed[:16, :128], mixed[16:, :128])
        m_im = jnp.where(first, mixed[:16, 128:], mixed[16:, 128:])
        b_re, b_im = (
            jnp.concatenate([inputs_ref[k, c, 2 * pair].astype(F32), inputs_ref[k, c, 2 * pair + 1].astype(F32)], axis=1)
            for c in range(2)
        )
        away = jnp.where(pair // 16 == core, 0, 1)
        at = 32 * k + pair % 16
        ends_ref[away, at : at + 1, :] = jnp.sum(b_re * m_re - b_im * m_im, axis=0, keepdims=True)
        ends_ref[away, at + 16 : at + 17, :] = jnp.sum(b_re * m_im + b_im * m_re, axis=0, keepdims=True)

    units = [(pair, k) for pair in range(32) for k in range(2)]
    for n in range(len(units) + LAG):
        if n in DRIVE_AT:
            drive(DRIVE_AT.index(n))
        if n < len(units):
            pull(*units[n])
        if n >= LAG:
            finish(*units[n - LAG])


def shifted_rows(x, by, fill):
    row = lax.broadcasted_iota(jnp.int32, (SPANS, 128), 0)
    moved = pltpu.roll(x, by % SPANS, 0)
    return jnp.where(row >= by if by > 0 else row < SPANS + by, moved, fill)


def local_kernel(start, size, fetching, within, damps, driven, inputs, readout, pars, *refs):
    copies = []
    if fetching:
        *refs, sems = refs
        sources, refs = refs[:fetching], refs[fetching:]
        out_ref, prefix_ref, table_ref, *refs = refs
        targets, refs = refs[:fetching], refs[fetching:]
        for n in range(fetching):
            copies.append(pltpu.make_async_copy(sources[n], targets[n], sems.at[n]))
            copies[n].start()
    else:
        out_ref, prefix_ref, table_ref, *refs = refs
    triangles, proj, turn, lifts, part, states, carry = refs
    row, col = iotas((ROWS, ROWS))
    same = row // SPAN == col // SPAN
    triangles[0] = ((col <= row) & same).astype(BF16)
    triangles[1] = ((col >= row) & same).astype(BF16)
    empty = jnp.zeros((16, 64), BF16)
    hole = jnp.zeros((16, 64), F32)

    def project(j, k, slot):
        pair = start + j
        b00, b01 = inputs[k, 0, 2 * pair], inputs[k, 1, 2 * pair]
        b10, b11 = inputs[k, 0, 2 * pair + 1], inputs[k, 1, 2 * pair + 1]
        rhs = jnp.concatenate(
            [
                jnp.concatenate([b00, empty, b01, empty], axis=1),
                jnp.concatenate([empty, b10, empty, b11], axis=1),
            ],
            axis=0,
        )
        proj[slot] = mm(driven[pair], rhs)

    def lift(j, k, slot):
        pair = start + j
        th, f = pars[k, 0, pair : pair + 1, :], pars[k, 1, pair : pair + 1, :]
        offs = within[k]
        cosine, sine = unit_circle(offs * (th * (0.5 / math.pi)))
        grow = jnp.exp2(offs * (f * LOG2E)) * damps[pair, k]
        fade = jnp.exp2(offs * (f * -LOG2E))
        turn[slot, 0], turn[slot, 1] = fade * cosine, fade * sine
        a_re, a_im = grow * cosine, grow * sine
        p_re, p_im = proj[slot, :, :128], proj[slot, :, 128:]
        lifts[slot, :, :128] = (a_re * p_re + a_im * p_im).astype(BF16)
        lifts[slot, :, 128:] = (a_re * p_im - a_im * p_re).astype(BF16)

    def add_up(j, k, slot):
        total = mm(triangles[k], lifts[slot])
        part[slot, 0], part[slot, 1] = total[:, :128], total[:, 128:]

    def carry_on(j, k, slot):
        edge = pl.ds(SPAN - 1 if k == 0 else 0, SPANS, stride=SPAN)
        d = turn[slot, 0, edge, :], turn[slot, 1, edge, :]
        s = times_of(d, (part[slot, 0, edge, :], part[slot, 1, edge, :]))
        sign = 1 if k == 0 else -1
        for by in (1, 2, 4):
            s_old = tuple(shifted_rows(x, sign * by, 0.0) for x in s)
            d_old = shifted_rows(d[0], sign * by, 1.0), shifted_rows(d[1], sign * by, 0.0)
            s = plus(times_of(d, s_old), s)
            d = times_of(d, d_old)
        carry[slot, 0], carry[slot, 1] = (shifted_rows(x, sign, 0.0) for x in s)
        carry[slot, 2], carry[slot, 3] = shifted_rows(d[0], sign, 1.0), shifted_rows(d[1], sign, 0.0)

    def spread(j, k, slot):
        for n in range(SPANS):
            cut = slice(SPAN * n, SPAN * n + SPAN)
            e = turn[slot, 0, cut, :], turn[slot, 1, cut, :]
            c_re, c_im, d_re, d_im = (jnp.broadcast_to(carry[slot, i, n : n + 1, :], (SPAN, 128)) for i in range(4))
            state = times_of(e, (part[slot, 0, cut, :] + c_re, part[slot, 1, cut, :] + c_im))
            states[j % 2, cut, 256 * k : 256 * k + 128] = state[0].astype(BF16)
            states[j % 2, cut, 256 * k + 128 : 256 * k + 256] = state[1].astype(BF16)
            prefix = times_of(e, (d_re, d_im))
            prefix_ref[j, k, cut, :128] = prefix[0].astype(BF16)
            prefix_ref[j, k, cut, 128:] = prefix[1].astype(BF16)

    def read(j):
        pair = start + j
        tables = []
        for k in range(2):
            for c in range(2):
                upper = jnp.concatenate([readout[k, c, 2 * pair], hole], axis=1)
                lower = jnp.concatenate([hole, readout[k, c, 2 * pair + 1]], axis=1)
                table = jnp.concatenate([upper, lower], axis=0)
                table_ref[j, k, c] = table
                tables.append((table if c == 0 else -table).astype(BF16))
        out_ref[j] = nt(states[j % 2], jnp.concatenate(tables, axis=1))

    units = [(j, k) for j in range(size) for k in range(2)]
    for turn_of in range(len(units) + 6):
        for late, act in ((0, project), (1, lift), (2, add_up), (3, carry_on), (4, spread)):
            at = turn_of - late
            if 0 <= at < len(units):
                act(*units[at], at % SLOTS)
        at = turn_of - 5
        if 0 <= at < len(units) and units[at][1] == 1:
            read(units[at][0])
    for copy in copies:
        copy.wait()


def times_of(a, b):
    return a[0] * b[0] - a[1] * b[1], a[0] * b[1] + a[1] * b[0]


def plus(a, b):
    return a[0] + b[0], a[1] + b[1]


def pick(condition, a, b):
    return tuple(jnp.where(condition, x, y) for x, y in zip(a, b))


def my_pars(pars):
    core = lax.axis_index("c")
    found = []
    for k in range(2):
        angle = pars[k, 0, pl.ds(16 * core, 16), :]
        rate = pars[k, 1, pl.ds(16 * core, 16), :]
        high = jnp.round(angle * (4096 * 0.5 / math.pi)) * (1.0 / 4096)
        coarse = 6433 / 1024
        low = ((angle - high * coarse) - high * (2 * math.pi - coarse)) * (0.5 / math.pi)
        found.append((high, low, rate * -LOG2E))
    return found


def decay_over(span, pars):
    high, low, level = pars
    u = span * high
    cosine, sine = unit_circle((u - jnp.round(u)) + span * low, SINE, COSINE)
    fade = jnp.exp2(span * level)
    return fade * cosine, fade * sine


def states_of(ref, k):
    return ref[32 * k : 32 * k + 16, :], ref[32 * k + 16 : 32 * k + 32, :]


def span_of(ref):
    span = ref[64:72, :]
    return jnp.concatenate([span, span], axis=0)


def keep_states(ref, k, value):
    ref[32 * k : 32 * k + 16, :], ref[32 * k + 16 : 32 * k + 32, :] = value


def keep_at(ref, at, value):
    ref[2 * at], ref[2 * at + 1] = value


def pair_kernel(own, other, pars, total_ref):
    core = lax.axis_index("c")
    mine = my_pars(pars)
    for k in range(2):
        ahead = core == k
        a, b = states_of(own, k), states_of(other, k)
        early, late = pick(ahead, a, b), pick(ahead, b, a)
        step = decay_over(jnp.where(ahead, span_of(other), span_of(own)), mine[k])
        keep_states(total_ref, k, plus(times_of(step, early), late))
    total_ref[64:72, :] = own[64:72, :] + other[64:72, :]


def gather_four(axis, own, one, two, three, data):
    here = lax.axis_index(axis)
    data[here] = own[...]
    data[here + 1 - 2 * (here % 2)] = one[...]
    data[(here + 2) % 4] = two[...]
    data[3 - here] = three[...]
    return here


def run_over(here, data, mine, k):
    zero = jnp.zeros((16, 128), F32)
    state, decay = (zero, zero), (zero + 1.0, zero)
    before, before_decay = state, decay
    for n in range(4) if k == 0 else range(3, -1, -1):
        before = pick(n == here, state, before)
        before_decay = pick(n == here, decay, before_decay)
        step = decay_over(span_of(data.at[n]), mine[k])
        state = plus(times_of(step, state), states_of(data.at[n], k))
        decay = times_of(step, decay)
    return state, before, before_decay


def group_kernel(axis, own, one, two, three, pars, *refs):
    *sends, before_ref, data = refs
    here = gather_four(axis, own, one, two, three, data)
    mine = my_pars(pars)
    totals = []
    for k in range(2):
        total, before, decay = run_over(here, data, mine, k)
        totals.append(total)
        keep_at(before_ref, k, before)
        keep_at(before_ref, 2 + k, decay)
    span = own[64:72, :] + one[64:72, :] + two[64:72, :] + three[64:72, :]
    if len(sends) == 1:
        for k in range(2):
            keep_states(sends[0], k, totals[k])
        sends[0][64:72, :] = span
        return
    here = lax.axis_index("z")
    partners = (here + 1 - 2 * (here % 2), (here + 2) % 4, 3 - here)
    for partner, send in zip(partners, sends):
        keep_states(send, 0, pick(partner > here, totals[0], totals[1]))
        send[32:40, :] = span


def enter_kernel(one, two, three, before_x, before_y, own, other, pars, mine_ref, theirs_ref, data):
    here = lax.axis_index("z")
    data[here] = one[...]
    data[here + 1 - 2 * (here % 2)] = one[...]
    data[(here + 2) % 4] = two[...]
    data[3 - here] = three[...]
    core = lax.axis_index("c")
    mine = my_pars(pars)
    zero = jnp.zeros((16, 128), F32)
    for k in range(2):
        state = (zero, zero)
        for n in range(3) if k == 0 else range(3, 0, -1):
            span = jnp.concatenate([data[n, 32:40, :]] * 2, axis=0)
            new = plus(times_of(decay_over(span, mine[k]), state), states_of(data.at[n], 0))
            state = pick(n < here if k == 0 else n > here, new, state)
        for before in (before_x, before_y):
            state = plus(times_of((before[4 + 2 * k], before[5 + 2 * k]), state), (before[2 * k], before[2 * k + 1]))
        ahead = core == k
        early = pick(ahead, states_of(own, k), states_of(other, k))
        later = plus(times_of(decay_over(jnp.where(ahead, span_of(own), span_of(other)), mine[k]), state), early)
        keep_at(mine_ref, k, pick(ahead, state, later))
        keep_at(theirs_ref, k, pick(ahead, later, state))


def final_kernel(*refs):
    count = len(PIECES)
    own, other = refs[:2]
    nears, prefixes, tables = (refs[2 + count * n : 2 + count * n + count] for n in range(3))
    driven, skip, glu, glu_bias, outw, out_gain, out_ref, entering, response = refs[2 + 3 * count :]
    core = lax.axis_index("c")
    entering[core] = own[...]
    entering[1 - core] = other[...]
    start = 0
    for size, near, prefix, table in zip(PIECES, nears, prefixes, tables):

        def tile(i, start=start, near=near, prefix=prefix, table=table):
            outs = []
            for j in range(4):
                total = None
                for k in range(2):
                    pair = 4 * (start + i) + j
                    er = entering[pair // 16, 2 * k, pl.ds(pair % 16, 1), :]
                    ei = entering[pair // 16, 2 * k + 1, pl.ds(pair % 16, 1), :]
                    cr, ci = table[4 * i + j, k, 0], table[4 * i + j, k, 1]
                    rhs = jnp.concatenate(
                        [(cr * er - ci * ei).astype(BF16), (-(cr * ei + ci * er)).astype(BF16)], axis=1
                    )
                    y = nt(prefix[4 * i + j, k], rhs)
                    total = y if total is None else total + y
                outs.append(total + near[4 * i + j])
            at = 128 * i
            response[:, pl.ds(at + 128 * start, 128)] = jnp.concatenate(outs, axis=1)

        for i in range(size):
            tile(i)
        start += size
    x = response[...] + skip[...] * driven[...].astype(F32)
    active = 0.5 * x * (1.0 + jnp.tanh(math.sqrt(2.0 / math.pi) * (x + 0.044715 * (x * x * x))))
    gate = mm(active.astype(BF16), glu[...]) + glu_bias[...]
    gated = (active * jax.nn.sigmoid(gate)).astype(BF16)
    projected = mm(gated, outw[...])
    scale = lax.rsqrt(jnp.mean(projected * projected, axis=-1, keepdims=True) + EPSILON)
    out_ref[...] = (projected * scale * out_gain[...]).astype(BF16)


def sds(shape, dtype=F32):
    return jax.ShapeDtypeStruct(shape, dtype)


def params(limit):
    return pltpu.CompilerParams(vmem_limit_bytes=limit * 1024 * 1024)


def run_local(start, size, args, weights):
    spec, distant = pl.BlockSpec(memory_space=VMEM), pl.BlockSpec(memory_space=pltpu.HBM)
    count = len(weights)
    return pl.pallas_call(
        functools.partial(local_kernel, 4 * start, 4 * size, count),
        name=f"local_{start}",
        in_specs=[spec] * len(args) + [distant] * count,
        out_specs=[spec] * (3 + count),
        out_shape=[
            sds((4 * size, ROWS, 32)),
            sds((4 * size, 2, ROWS, 256), BF16),
            sds((4 * size, 2, 2, 32, 128)),
            *(sds(weight.shape, BF16) for weight in weights),
        ],
        scratch_shapes=[
            VMEM((2, ROWS, ROWS), BF16), VMEM((SLOTS, ROWS, 256), F32), VMEM((SLOTS, 2, ROWS, 128), F32),
            VMEM((SLOTS, ROWS, 256), BF16), VMEM((SLOTS, 2, ROWS, 128), F32), VMEM((2, ROWS, 512), BF16),
            VMEM((SLOTS, 4, SPANS, 128), F32),
            *([pltpu.SemaphoreType.DMA((count,))] if count else []),
        ],
        compiler_params=params(8),
        cost_estimate=pl.CostEstimate(flops=size * 5 * 10**8, bytes_accessed=size * 2 * 2**20, transcendentals=0),
    )(*args, *weights)


def simple(kernel, name, shapes, args, scratch=()):
    spec = pl.BlockSpec(memory_space=VMEM)
    return pl.pallas_call(
        kernel,
        name=name,
        in_specs=[spec] * len(args),
        out_specs=[spec] * len(shapes),
        out_shape=[sds(shape) for shape in shapes],
        scratch_shapes=scratch,
        compiler_params=params(4),
    )(*args)


def local(
    tokens, elapsed, norm_gain, in_weight, state_input, state_output, forget_rate, decay_angle,
    skip_gain, glu_weight, glu_bias, out_weight, out_gain,
):
    elapsed_row = elapsed.reshape(1, ROWS)
    inputs = jnp.swapaxes(state_input, 3, 4)
    spec, distant = pl.BlockSpec(memory_space=VMEM), pl.BlockSpec(memory_space=pltpu.HBM)
    driven, pairs, ends, pars, damps, within, inputs_here = pl.pallas_call(
        end_kernel,
        name="ends",
        in_specs=[spec, spec, spec, distant, distant, spec, spec],
        out_specs=[spec] * 7,
        out_shape=[
            sds((ROWS, CHANNELS), BF16), sds((32, ROWS, 32), BF16), sds((2, 72, 128)), sds((2, 2, 32, 128)),
            sds((32, 2, ROWS, ROWS)), sds((2, ROWS, ROWS)), sds((2, 2, 64, 16, 64), BF16),
        ],
        scratch_shapes=[
            VMEM((ROWS, D), BF16), VMEM((3, ROWS, ROWS), F32), VMEM((CHUNKS, D, 256), BF16), VMEM((2, 256, ROWS), BF16),
            VMEM((8, 2, ROWS, 256), BF16),
            pltpu.SemaphoreType.DMA((CHUNKS,)), pltpu.SemaphoreType.DMA((CHUNKS,)),
        ],
        compiler_params=params(12),
    )(
        *(hbm(a) for a in (tokens, elapsed_row, norm_gain.reshape(1, D), in_weight, inputs, decay_angle, forget_rate))
    )

    pieces, start = [], 0

    def piece_between(before, after, weights=()):
        index = len(pieces)
        start = sum(PIECES[:index])
        pairs_now, _ = lax.optimization_barrier((pairs, before))
        piece = run_local(
            start, PIECES[index],
            (within, damps, pairs_now, inputs_here, state_output, pars), weights,
        )
        *piece, after = lax.optimization_barrier((*piece, after))
        pieces.append(piece)
        return after

    swap = [(0, 1), (1, 0)]
    swaps = ([(0, 1), (1, 0), (2, 3), (3, 2)], [(0, 2), (2, 0), (1, 3), (3, 1)], [(0, 3), (3, 0), (1, 2), (2, 1)])
    four = VMEM((4, 72, 128), F32)
    keep = ends[0]
    partner = piece_between(keep, lax.ppermute(ends[1], "c", swap))
    (total,) = simple(pair_kernel, "pair", [(72, 128)], (keep, partner, pars))
    befores = []
    for axis in ("y", "x"):
        others = piece_between(total, tuple(lax.ppermute(total, axis, pairs) for pairs in swaps))
        *totals, before = simple(
            functools.partial(group_kernel, axis), f"group_{axis}",
            [(72, 128)] * (axis == "y") + [(40, 128)] * (3 * (axis == "x")) + [(8, 16, 128)],
            (total, *others, pars), [four],
        )
        total = totals[0]
        befores.append(before)
    others = piece_between(
        total, tuple(lax.ppermute(value, "z", pairs) for value, pairs in zip(totals, swaps)),
        (hbm(glu_weight), hbm(out_weight)),
    )
    glu_here, outw_here = pieces[-1][3:]
    mine, theirs = simple(
        enter_kernel, "enter", [(4, 16, 128), (4, 16, 128)],
        (*others, befores[1], befores[0], keep, partner, pars), [VMEM((4, 40, 128), F32)],
    )
    other = piece_between(theirs, lax.ppermute(theirs, "c", swap))

    spec = pl.BlockSpec(memory_space=VMEM)
    args = (
        mine, other, *(p[0] for p in pieces), *(p[1] for p in pieces), *(p[2] for p in pieces),
        driven, skip_gain.reshape(1, CHANNELS), glu_here, glu_bias.reshape(1, CHANNELS), outw_here, out_gain.reshape(1, D),
    )
    return pl.pallas_call(
        final_kernel,
        name="final",
        in_specs=[spec] * len(args),
        out_specs=spec,
        out_shape=sds((ROWS, D), BF16),
        scratch_shapes=[VMEM((2, 4, 16, 128), F32), VMEM((ROWS, CHANNELS), F32)],
        compiler_params=params(12),
    )(*args)


def hbm(x):
    return pltpu.with_memory_space_constraint(x, pltpu.HBM)


def solution(mesh):
    finer = Mesh(mesh.devices.reshape(4, 4, 4, 2), AXES)
    split = P(AXES, None)
    placed = (split, P(AXES), P(), P(), P(), P(), P(), P(), P(), P(), P(), P(), P())
    return jax.shard_map(local, mesh=finer, in_specs=placed, out_specs=split, check_vma=False)
```

```python
import functools
import math

import jax
import jax.numpy as jnp
from jax import lax
from jax.experimental import pallas as pl
from jax.experimental.pallas import tpu as pltpu
from jax.sharding import Mesh
from jax.sharding import PartitionSpec as P

ROWS = 128
D = 2048
CHANNELS = 1024
CHUNKS = 4
LAG = 12
DRIVE_AT = (6, 7, 8, 9, 13, 16, 19, 22, 29, 32, 35, 38, 45, 48, 51, 54)
SPAN = 16
SPANS = ROWS // SPAN
SLOTS = 6
PIECES = (1, 2, 2, 2, 1)
LOG2E = 1.0 / math.log(2.0)
TINY = 1e-37
EPSILON = 1e-06
AXES = ("z", "x", "y", "c")
VMEM = pltpu.VMEM
F32 = jnp.float32
BF16 = jnp.bfloat16

SINE = (4.44288291, -7.30824512, 3.60634303, -0.84604096, 0.10968436)
COSINE = (1.4142135, -6.97885097, 5.73946067, -1.88355924, 0.31068962)
SINE_SHORT = (4.44287876, -7.30776104, 3.5971931, -0.7896682)
COSINE_SHORT = (1.41420407, -6.97764062, 5.71521917, -1.7282871)


def horner(coefficients, x):
    value = coefficients[-1] * x + coefficients[-2]
    for c in coefficients[-3::-1]:
        value = value * x + c
    return value


def half_turn(turns, sine=SINE_SHORT, cosine=COSINE_SHORT):
    r = turns - jnp.round(turns)
    z = r * r
    return r * horner(sine, z), horner(cosine, z)


def unit_circle(turns, *tables):
    s, c = half_turn(turns, *tables)
    return 1.0 - s * s, s * c


def nt(a, b):
    return lax.dot_general(a, b, (((1,), (1,)), ((), ())), preferred_element_type=F32)


def mm(a, b):
    return jnp.dot(a, b, preferred_element_type=F32)


def iotas(shape):
    return lax.broadcasted_iota(jnp.int32, shape, 0), lax.broadcasted_iota(jnp.int32, shape, 1)


def column_of(row):
    return jnp.broadcast_to(row, (ROWS, ROWS)).T


def in_parts(x):
    high = x.astype(BF16)
    rest = x - high.astype(F32)
    middle = rest.astype(BF16)
    return high, middle, (rest - middle.astype(F32)).astype(BF16)


def sums_of(chosen, parts):
    return sum(mm(chosen.astype(BF16), part) for part in parts)


def pair_row(ref, k, pair):
    return jnp.concatenate([ref[k, pl.ds(2 * pair, 1), :], ref[k, pl.ds(2 * pair + 1, 1), :]], axis=1)


def end_kernel(
    tokens, elapsed, gain, weight, inputs, angle, rate,
    driven_ref, pairs_ref, ends_ref, pars_ref, damp_ref, within_ref, inputs_ref, normed, times, chunks, flipped, summed, pulls, weight_sems, input_sems,
):
    core = lax.axis_index("c")

    def fetch(i):
        return (
            pltpu.make_async_copy(
                weight.at[:, pl.ds(256 * i, 256)], chunks.at[i], weight_sems.at[i]
            ),
            pltpu.make_async_copy(inputs.at[:, :, pl.ds(16 * i, 16)], inputs_ref.at[:, :, pl.ds(16 * i, 16)], input_sems.at[i]),
        )

    for i in range(CHUNKS):
        for copy in fetch(i):
            copy.start()
    steps = column_of(elapsed[...])
    parts = in_parts(steps)
    row, col = iotas((ROWS, ROWS))
    same = row // SPAN == col // SPAN
    times[0] = sums_of(col > row, parts)
    times[1] = sums_of(col < row, parts)
    times[2] = steps
    within_ref[0] = sums_of((col <= row) & same, parts)
    within_ref[1] = sums_of((col >= row) & same, parts)
    total = sums_of(jnp.ones((8, ROWS), F32), parts)
    ends_ref[0, 64:] = total
    ends_ref[1, 64:] = total
    for r in range(0, ROWS, 16):
        x = tokens[r : r + 16, :].astype(F32)
        scale = lax.rsqrt(jnp.mean(x * x, axis=-1, keepdims=True) + EPSILON)
        normed[r : r + 16, :] = (x * scale * gain[...]).astype(BF16)
    first = lax.broadcasted_iota(jnp.int32, (16, 128), 1) < 64

    def gather_in(step, quarter):
        if quarter == 0:
            for copy in fetch(step):
                copy.wait()
        cut = slice(512 * quarter, 512 * quarter + 512)
        value = mm(normed[:, cut], chunks[step, cut, :])
        summed[...] = value if quarter == 0 else summed[...] + value
        if quarter == 3:
            drive(step)

    def drive(step):
        driven = summed[...].astype(BF16)
        driven_ref[:, 256 * step : 256 * step + 256] = driven
        for j in range(8):
            pairs_ref[8 * step + j] = driven[:, 32 * j : 32 * j + 32]
        flipped[step % 2] = driven.astype(F32).T.astype(BF16)

    def pull(pair, k):
        f = pair_row(rate, k, pair)
        th = pair_row(angle, k, pair)
        pars_ref[k, 0, pair : pair + 1, :] = th
        pars_ref[k, 1, pair : pair + 1, :] = f
        after = times[k]
        s, c = half_turn(after * (th * (0.5 / math.pi)))
        bend = jnp.tanh(times[2] * f)
        damp = bend * lax.rsqrt(bend * (0.5 + 0.5 * bend) + TINY)
        damp_ref[pair, k] = damp
        amp = jnp.exp2(after * (f * -LOG2E)) * damp
        tilted = amp * s
        pulls[pair % 8, k, :, :128] = (amp - tilted * s).astype(BF16)
        pulls[pair % 8, k, :, 128:] = (tilted * c).astype(BF16)

    def finish(pair, k):
        mixed = mm(flipped[pair // 8 % 2, 32 * (pair % 8) : 32 * (pair % 8) + 32], pulls[pair % 8, k])
        m_re = jnp.where(first, mixed[:16, :128], mixed[16:, :128])
        m_im = jnp.where(first, mixed[:16, 128:], mixed[16:, 128:])
        b_re, b_im = (
            jnp.concatenate([inputs_ref[k, c, 2 * pair].astype(F32), inputs_ref[k, c, 2 * pair + 1].astype(F32)], axis=1)
            for c in range(2)
        )
        away = jnp.where(pair // 16 == core, 0, 1)
        at = 32 * k + pair % 16
        ends_ref[away, at : at + 1, :] = jnp.sum(b_re * m_re - b_im * m_im, axis=0, keepdims=True)
        ends_ref[away, at + 16 : at + 17, :] = jnp.sum(b_re * m_im + b_im * m_re, axis=0, keepdims=True)

    units = [(pair, k) for pair in range(32) for k in range(2)]
    for n in range(len(units) + LAG):
        if n in DRIVE_AT:
            gather_in(*divmod(DRIVE_AT.index(n), 4))
        if n < len(units):
            pull(*units[n])
        if n >= LAG:
            finish(*units[n - LAG])


def shifted_rows(x, by, fill):
    row = lax.broadcasted_iota(jnp.int32, (SPANS, 128), 0)
    moved = pltpu.roll(x, by % SPANS, 0)
    return jnp.where(row >= by if by > 0 else row < SPANS + by, moved, fill)


def local_kernel(start, size, fetching, within, damps, driven, inputs, readout, pars, *refs):
    copies = []
    if fetching:
        *refs, sems = refs
        sources, refs = refs[:fetching], refs[fetching:]
        out_ref, prefix_ref, table_ref, *refs = refs
        targets, refs = refs[:fetching], refs[fetching:]
        for n in range(fetching):
            copies.append(pltpu.make_async_copy(sources[n], targets[n], sems.at[n]))
            copies[n].start()
    else:
        out_ref, prefix_ref, table_ref, *refs = refs
    triangles, proj, turn, lifts, part, states, carry = refs
    row, col = iotas((ROWS, ROWS))
    same = row // SPAN == col // SPAN
    triangles[0] = ((col <= row) & same).astype(BF16)
    triangles[1] = ((col >= row) & same).astype(BF16)
    empty = jnp.zeros((16, 64), BF16)
    hole = jnp.zeros((16, 64), F32)

    def project(j, k, slot):
        pair = start + j
        b00, b01 = inputs[k, 0, 2 * pair], inputs[k, 1, 2 * pair]
        b10, b11 = inputs[k, 0, 2 * pair + 1], inputs[k, 1, 2 * pair + 1]
        rhs = jnp.concatenate(
            [
                jnp.concatenate([b00, empty, b01, empty], axis=1),
                jnp.concatenate([empty, b10, empty, b11], axis=1),
            ],
            axis=0,
        )
        proj[slot] = mm(driven[pair], rhs)

    def lift(j, k, slot):
        pair = start + j
        th, f = pars[k, 0, pair : pair + 1, :], pars[k, 1, pair : pair + 1, :]
        offs = within[k]
        cosine, sine = unit_circle(offs * (th * (0.5 / math.pi)))
        grow = jnp.exp2(offs * (f * LOG2E)) * damps[pair, k]
        fade = jnp.exp2(offs * (f * -LOG2E))
        turn[slot, 0], turn[slot, 1] = fade * cosine, fade * sine
        a_re, a_im = grow * cosine, grow * sine
        p_re, p_im = proj[slot, :, :128], proj[slot, :, 128:]
        lifts[slot, :, :128] = (a_re * p_re + a_im * p_im).astype(BF16)
        lifts[slot, :, 128:] = (a_re * p_im - a_im * p_re).astype(BF16)

    def add_up(j, k, slot):
        total = mm(triangles[k], lifts[slot])
        part[slot, 0], part[slot, 1] = total[:, :128], total[:, 128:]

    def carry_on(j, k, slot):
        edge = pl.ds(SPAN - 1 if k == 0 else 0, SPANS, stride=SPAN)
        d = turn[slot, 0, edge, :], turn[slot, 1, edge, :]
        s = times_of(d, (part[slot, 0, edge, :], part[slot, 1, edge, :]))
        sign = 1 if k == 0 else -1
        for by in (1, 2, 4):
            s_old = tuple(shifted_rows(x, sign * by, 0.0) for x in s)
            d_old = shifted_rows(d[0], sign * by, 1.0), shifted_rows(d[1], sign * by, 0.0)
            s = plus(times_of(d, s_old), s)
            d = times_of(d, d_old)
        carry[slot, 0], carry[slot, 1] = (shifted_rows(x, sign, 0.0) for x in s)
        carry[slot, 2], carry[slot, 3] = shifted_rows(d[0], sign, 1.0), shifted_rows(d[1], sign, 0.0)

    def spread(j, k, slot):
        for n in range(SPANS):
            cut = slice(SPAN * n, SPAN * n + SPAN)
            e = turn[slot, 0, cut, :], turn[slot, 1, cut, :]
            c_re, c_im, d_re, d_im = (jnp.broadcast_to(carry[slot, i, n : n + 1, :], (SPAN, 128)) for i in range(4))
            state = times_of(e, (part[slot, 0, cut, :] + c_re, part[slot, 1, cut, :] + c_im))
            states[j % 2, cut, 256 * k : 256 * k + 128] = state[0].astype(BF16)
            states[j % 2, cut, 256 * k + 128 : 256 * k + 256] = state[1].astype(BF16)
            prefix = times_of(e, (d_re, d_im))
            prefix_ref[j, k, cut, :128] = prefix[0].astype(BF16)
            prefix_ref[j, k, cut, 128:] = prefix[1].astype(BF16)

    def read(j):
        pair = start + j
        tables = []
        for k in range(2):
            for c in range(2):
                upper = jnp.concatenate([readout[k, c, 2 * pair], hole], axis=1)
                lower = jnp.concatenate([hole, readout[k, c, 2 * pair + 1]], axis=1)
                table = jnp.concatenate([upper, lower], axis=0)
                table_ref[j, k, c] = table
                tables.append((table if c == 0 else -table).astype(BF16))
        out_ref[j] = nt(states[j % 2], jnp.concatenate(tables, axis=1))

    units = [(j, k) for j in range(size) for k in range(2)]
    for turn_of in range(len(units) + 6):
        for late, act in ((0, project), (1, lift), (2, add_up), (3, carry_on), (4, spread)):
            at = turn_of - late
            if 0 <= at < len(units):
                act(*units[at], at % SLOTS)
        at = turn_of - 5
        if 0 <= at < len(units) and units[at][1] == 1:
            read(units[at][0])
    for copy in copies:
        copy.wait()


def times_of(a, b):
    return a[0] * b[0] - a[1] * b[1], a[0] * b[1] + a[1] * b[0]


def plus(a, b):
    return a[0] + b[0], a[1] + b[1]


def pick(condition, a, b):
    return tuple(jnp.where(condition, x, y) for x, y in zip(a, b))


def my_pars(pars):
    core = lax.axis_index("c")
    found = []
    for k in range(2):
        angle = pars[k, 0, pl.ds(16 * core, 16), :]
        rate = pars[k, 1, pl.ds(16 * core, 16), :]
        high = jnp.round(angle * (4096 * 0.5 / math.pi)) * (1.0 / 4096)
        coarse = 6433 / 1024
        low = ((angle - high * coarse) - high * (2 * math.pi - coarse)) * (0.5 / math.pi)
        found.append((high, low, rate * -LOG2E))
    return found


def decay_over(span, pars):
    high, low, level = pars
    u = span * high
    cosine, sine = unit_circle((u - jnp.round(u)) + span * low, SINE, COSINE)
    fade = jnp.exp2(span * level)
    return fade * cosine, fade * sine


def states_of(ref, k):
    return ref[32 * k : 32 * k + 16, :], ref[32 * k + 16 : 32 * k + 32, :]


def span_of(ref):
    span = ref[64:72, :]
    return jnp.concatenate([span, span], axis=0)


def keep_states(ref, k, value):
    ref[32 * k : 32 * k + 16, :], ref[32 * k + 16 : 32 * k + 32, :] = value


def keep_at(ref, at, value):
    ref[2 * at], ref[2 * at + 1] = value


def pair_kernel(own, other, pars, total_ref):
    core = lax.axis_index("c")
    mine = my_pars(pars)
    for k in range(2):
        ahead = core == k
        a, b = states_of(own, k), states_of(other, k)
        early, late = pick(ahead, a, b), pick(ahead, b, a)
        step = decay_over(jnp.where(ahead, span_of(other), span_of(own)), mine[k])
        keep_states(total_ref, k, plus(times_of(step, early), late))
    total_ref[64:72, :] = own[64:72, :] + other[64:72, :]


def gather_four(axis, own, one, two, three, data):
    here = lax.axis_index(axis)
    data[here] = own[...]
    data[here + 1 - 2 * (here % 2)] = one[...]
    data[(here + 2) % 4] = two[...]
    data[3 - here] = three[...]
    return here


def run_over(here, data, mine, k):
    zero = jnp.zeros((16, 128), F32)
    state, decay = (zero, zero), (zero + 1.0, zero)
    before, before_decay = state, decay
    for n in range(4) if k == 0 else range(3, -1, -1):
        before = pick(n == here, state, before)
        before_decay = pick(n == here, decay, before_decay)
        step = decay_over(span_of(data.at[n]), mine[k])
        state = plus(times_of(step, state), states_of(data.at[n], k))
        decay = times_of(step, decay)
    return state, before, before_decay


def group_kernel(axis, own, one, two, three, pars, *refs):
    *sends, before_ref, data = refs
    here = gather_four(axis, own, one, two, three, data)
    mine = my_pars(pars)
    totals = []
    for k in range(2):
        total, before, decay = run_over(here, data, mine, k)
        totals.append(total)
        keep_at(before_ref, k, before)
        keep_at(before_ref, 2 + k, decay)
    span = own[64:72, :] + one[64:72, :] + two[64:72, :] + three[64:72, :]
    if len(sends) == 1:
        for k in range(2):
            keep_states(sends[0], k, totals[k])
        sends[0][64:72, :] = span
        return
    here = lax.axis_index("z")
    partners = ((here + 2) % 4, 3 - here, here + 1 - 2 * (here % 2))
    for partner, send in zip(partners, sends):
        keep_states(send, 0, pick(partner > here, totals[0], totals[1]))
        send[32:40, :] = span


def enter_kernel(one, two, three, before_x, before_y, own, other, pars, mine_ref, theirs_ref, data):
    here = lax.axis_index("z")
    data[here] = one[...]
    data[here + 1 - 2 * (here % 2)] = one[...]
    data[(here + 2) % 4] = two[...]
    data[3 - here] = three[...]
    core = lax.axis_index("c")
    mine = my_pars(pars)
    zero = jnp.zeros((16, 128), F32)
    for k in range(2):
        state = (zero, zero)
        for n in range(3) if k == 0 else range(3, 0, -1):
            span = jnp.concatenate([data[n, 32:40, :]] * 2, axis=0)
            new = plus(times_of(decay_over(span, mine[k]), state), states_of(data.at[n], 0))
            state = pick(n < here if k == 0 else n > here, new, state)
        for before in (before_x, before_y):
            state = plus(times_of((before[4 + 2 * k], before[5 + 2 * k]), state), (before[2 * k], before[2 * k + 1]))
        ahead = core == k
        early = pick(ahead, states_of(own, k), states_of(other, k))
        later = plus(times_of(decay_over(jnp.where(ahead, span_of(own), span_of(other)), mine[k]), state), early)
        keep_at(mine_ref, k, pick(ahead, state, later))
        keep_at(theirs_ref, k, pick(ahead, later, state))


def final_kernel(*refs):
    count = len(PIECES)
    own, other = refs[:2]
    nears, prefixes, tables = (refs[2 + count * n : 2 + count * n + count] for n in range(3))
    driven, skip, glu, glu_bias, outw, out_gain, out_ref, entering, response = refs[2 + 3 * count :]
    core = lax.axis_index("c")
    entering[core] = own[...]
    entering[1 - core] = other[...]
    start = 0
    for size, near, prefix, table in zip(PIECES, nears, prefixes, tables):

        def tile(i, start=start, near=near, prefix=prefix, table=table):
            outs = []
            for j in range(4):
                total = None
                for k in range(2):
                    pair = 4 * (start + i) + j
                    er = entering[pair // 16, 2 * k, pl.ds(pair % 16, 1), :]
                    ei = entering[pair // 16, 2 * k + 1, pl.ds(pair % 16, 1), :]
                    cr, ci = table[4 * i + j, k, 0], table[4 * i + j, k, 1]
                    rhs = jnp.concatenate(
                        [(cr * er - ci * ei).astype(BF16), (-(cr * ei + ci * er)).astype(BF16)], axis=1
                    )
                    y = nt(prefix[4 * i + j, k], rhs)
                    total = y if total is None else total + y
                outs.append(total + near[4 * i + j])
            at = 128 * i
            response[:, pl.ds(at + 128 * start, 128)] = jnp.concatenate(outs, axis=1)

        for i in range(size):
            tile(i)
        start += size
    x = response[...] + skip[...] * driven[...].astype(F32)
    active = 0.5 * x * (1.0 + jnp.tanh(math.sqrt(2.0 / math.pi) * (x + 0.044715 * (x * x * x))))
    gate = mm(active.astype(BF16), glu[...]) + glu_bias[...]
    gated = (active * jax.nn.sigmoid(gate)).astype(BF16)
    projected = mm(gated, outw[...])
    scale = lax.rsqrt(jnp.mean(projected * projected, axis=-1, keepdims=True) + EPSILON)
    out_ref[...] = (projected * scale * out_gain[...]).astype(BF16)


def sds(shape, dtype=F32):
    return jax.ShapeDtypeStruct(shape, dtype)


def params(limit):
    return pltpu.CompilerParams(vmem_limit_bytes=limit * 1024 * 1024)


def run_local(start, size, args, weights):
    spec, distant = pl.BlockSpec(memory_space=VMEM), pl.BlockSpec(memory_space=pltpu.HBM)
    count = len(weights)
    return pl.pallas_call(
        functools.partial(local_kernel, 4 * start, 4 * size, count),
        name=f"local_{start}",
        in_specs=[spec] * len(args) + [distant] * count,
        out_specs=[spec] * (3 + count),
        out_shape=[
            sds((4 * size, ROWS, 32)),
            sds((4 * size, 2, ROWS, 256), BF16),
            sds((4 * size, 2, 2, 32, 128)),
            *(sds(weight.shape, BF16) for weight in weights),
        ],
        scratch_shapes=[
            VMEM((2, ROWS, ROWS), BF16), VMEM((SLOTS, ROWS, 256), F32), VMEM((SLOTS, 2, ROWS, 128), F32),
            VMEM((SLOTS, ROWS, 256), BF16), VMEM((SLOTS, 2, ROWS, 128), F32), VMEM((2, ROWS, 512), BF16),
            VMEM((SLOTS, 4, SPANS, 128), F32),
            *([pltpu.SemaphoreType.DMA((count,))] if count else []),
        ],
        compiler_params=params(8),
        cost_estimate=pl.CostEstimate(flops=size * 5 * 10**8, bytes_accessed=size * 2 * 2**20, transcendentals=0),
    )(*args, *weights)


def simple(kernel, name, shapes, args, scratch=()):
    spec = pl.BlockSpec(memory_space=VMEM)
    return pl.pallas_call(
        kernel,
        name=name,
        in_specs=[spec] * len(args),
        out_specs=[spec] * len(shapes),
        out_shape=[sds(shape) for shape in shapes],
        scratch_shapes=scratch,
        compiler_params=params(4),
    )(*args)


def local(
    tokens, elapsed, norm_gain, in_weight, state_input, state_output, forget_rate, decay_angle,
    skip_gain, glu_weight, glu_bias, out_weight, out_gain,
):
    elapsed_row = elapsed.reshape(1, ROWS)
    inputs = jnp.swapaxes(state_input, 3, 4)
    spec, distant = pl.BlockSpec(memory_space=VMEM), pl.BlockSpec(memory_space=pltpu.HBM)
    driven, pairs, ends, pars, damps, within, inputs_here = pl.pallas_call(
        end_kernel,
        name="ends",
        in_specs=[spec, spec, spec, distant, distant, spec, spec],
        out_specs=[spec] * 7,
        out_shape=[
            sds((ROWS, CHANNELS), BF16), sds((32, ROWS, 32), BF16), sds((2, 72, 128)), sds((2, 2, 32, 128)),
            sds((32, 2, ROWS, ROWS)), sds((2, ROWS, ROWS)), sds((2, 2, 64, 16, 64), BF16),
        ],
        scratch_shapes=[
            VMEM((ROWS, D), BF16), VMEM((3, ROWS, ROWS), F32), VMEM((CHUNKS, D, 256), BF16), VMEM((2, 256, ROWS), BF16),
            VMEM((ROWS, 256), F32), VMEM((8, 2, ROWS, 256), BF16),
            pltpu.SemaphoreType.DMA((CHUNKS,)), pltpu.SemaphoreType.DMA((CHUNKS,)),
        ],
        compiler_params=params(12),
    )(
        *(hbm(a) for a in (tokens, elapsed_row, norm_gain.reshape(1, D), in_weight, inputs, decay_angle, forget_rate))
    )

    pieces, start = [], 0

    def piece_between(before, after, weights=()):
        index = len(pieces)
        start = sum(PIECES[:index])
        pairs_now, _ = lax.optimization_barrier((pairs, before))
        piece = run_local(
            start, PIECES[index],
            (within, damps, pairs_now, inputs_here, state_output, pars), weights,
        )
        *piece, after = lax.optimization_barrier((*piece, after))
        pieces.append(piece)
        return after

    swap = [(0, 1), (1, 0)]
    swaps = ([(0, 1), (1, 0), (2, 3), (3, 2)], [(0, 2), (2, 0), (1, 3), (3, 1)], [(0, 3), (3, 0), (1, 2), (2, 1)])

    def trade(values, axis, order, weights=()):
        found = piece_between(values[order[0]], tuple(lax.ppermute(values[n], axis, swaps[n]) for n in order), weights)
        return tuple(found[order.index(n)] for n in range(3))

    four = VMEM((4, 72, 128), F32)
    keep = ends[0]
    partner = piece_between(keep, lax.ppermute(ends[1], "c", swap))
    (total,) = simple(pair_kernel, "pair", [(72, 128)], (keep, partner, pars))
    befores = []
    for axis in ("y", "x"):
        others = trade((total,) * 3, axis, (0, 2, 1))
        *totals, before = simple(
            functools.partial(group_kernel, axis), f"group_{axis}",
            [(72, 128)] * (axis == "y") + [(40, 128)] * (3 * (axis == "x")) + [(8, 16, 128)],
            (total, *others, pars), [four],
        )
        total = totals[0]
        befores.append(before)
    others = trade(totals[2:] + totals[:2], "z", (1, 2, 0), (hbm(glu_weight), hbm(out_weight)))
    glu_here, outw_here = pieces[-1][3:]
    mine, theirs = simple(
        enter_kernel, "enter", [(4, 16, 128), (4, 16, 128)],
        (*others, befores[1], befores[0], keep, partner, pars), [VMEM((4, 40, 128), F32)],
    )
    other = piece_between(theirs, lax.ppermute(theirs, "c", swap))

    spec = pl.BlockSpec(memory_space=VMEM)
    args = (
        mine, other, *(p[0] for p in pieces), *(p[1] for p in pieces), *(p[2] for p in pieces),
        driven, skip_gain.reshape(1, CHANNELS), glu_here, glu_bias.reshape(1, CHANNELS), outw_here, out_gain.reshape(1, D),
    )
    return pl.pallas_call(
        final_kernel,
        name="final",
        in_specs=[spec] * len(args),
        out_specs=spec,
        out_shape=sds((ROWS, D), BF16),
        scratch_shapes=[VMEM((2, 4, 16, 128), F32), VMEM((ROWS, CHANNELS), F32)],
        compiler_params=params(12),
    )(*args)


def hbm(x):
    return pltpu.with_memory_space_constraint(x, pltpu.HBM)


def solution(mesh):
    finer = Mesh(mesh.devices.reshape(4, 4, 4, 2), AXES)
    split = P(AXES, None)
    placed = (split, P(AXES), P(), P(), P(), P(), P(), P(), P(), P(), P(), P(), P())
    return jax.shard_map(local, mesh=finer, in_specs=placed, out_specs=split, check_vma=False)
```

```python
import functools
import math

import jax
import jax.numpy as jnp
from jax import lax
from jax.experimental import pallas as pl
from jax.experimental.pallas import tpu as pltpu
from jax.sharding import Mesh
from jax.sharding import PartitionSpec as P

ROWS = 128
D = 2048
CHANNELS = 1024
CHUNKS = 4
FINISH_AT = 24
LAG = 6
NORM_AT = 18
DRIVE_AT = (18, 19, 20, 21, 22, 24, 26, 28, 30, 33, 36, 39, 41, 44, 47, 50)
SPAN = 16
SPANS = ROWS // SPAN
SLOTS = 6
PIECES = (1, 2, 2, 2, 1)
LOG2E = 1.0 / math.log(2.0)
TINY = 1e-37
EPSILON = 1e-06
AXES = ("z", "x", "y", "c")
VMEM = pltpu.VMEM
F32 = jnp.float32
BF16 = jnp.bfloat16

SINE = (4.44288291, -7.30824512, 3.60634303, -0.84604096, 0.10968436)
COSINE = (1.4142135, -6.97885097, 5.73946067, -1.88355924, 0.31068962)
SINE_SHORT = (4.44287876, -7.30776104, 3.5971931, -0.7896682)
COSINE_SHORT = (1.41420407, -6.97764062, 5.71521917, -1.7282871)


def horner(coefficients, x):
    value = coefficients[-1] * x + coefficients[-2]
    for c in coefficients[-3::-1]:
        value = value * x + c
    return value


def half_turn(turns, sine=SINE_SHORT, cosine=COSINE_SHORT):
    r = turns - jnp.round(turns)
    z = r * r
    return r * horner(sine, z), horner(cosine, z)


def unit_circle(turns, *tables):
    s, c = half_turn(turns, *tables)
    return 1.0 - s * s, s * c


def nt(a, b):
    return lax.dot_general(a, b, (((1,), (1,)), ((), ())), preferred_element_type=F32)


def mm(a, b):
    return jnp.dot(a, b, preferred_element_type=F32)


def iotas(shape):
    return lax.broadcasted_iota(jnp.int32, shape, 0), lax.broadcasted_iota(jnp.int32, shape, 1)


def column_of(row):
    return jnp.broadcast_to(row, (ROWS, ROWS)).T


def in_parts(x):
    high = x.astype(BF16)
    rest = x - high.astype(F32)
    middle = rest.astype(BF16)
    return high, middle, (rest - middle.astype(F32)).astype(BF16)


def sums_of(chosen, parts):
    return sum(mm(chosen.astype(BF16), part) for part in parts)


def pair_row(ref, k, pair):
    return jnp.concatenate([ref[k, pl.ds(2 * pair, 1), :], ref[k, pl.ds(2 * pair + 1, 1), :]], axis=1)


def end_kernel(
    tokens, elapsed, gain, weight, inputs, angle, rate,
    driven_ref, pairs_ref, ends_ref, pars_ref, damp_ref, within_ref, inputs_ref, raw, normed, times, chunks, flipped, summed, pulls, weight_sems, input_sems, token_sem,
):
    core = lax.axis_index("c")

    def fetch(i):
        return (
            pltpu.make_async_copy(
                weight.at[:, pl.ds(256 * i, 256)], chunks.at[i], weight_sems.at[i]
            ),
            pltpu.make_async_copy(inputs.at[:, :, pl.ds(16 * i, 16)], inputs_ref.at[:, :, pl.ds(16 * i, 16)], input_sems.at[i]),
        )

    def norm():
        token_copy.wait()
        for r in range(0, ROWS, 16):
            x = raw[r : r + 16, :].astype(F32)
            scale = lax.rsqrt(jnp.mean(x * x, axis=-1, keepdims=True) + EPSILON)
            normed[r : r + 16, :] = (x * scale * gain[...]).astype(BF16)

    token_copy = pltpu.make_async_copy(tokens, raw, token_sem)
    token_copy.start()
    fetched = [fetch(i) for i in range(CHUNKS)]
    for n in range(2):
        for copies in fetched:
            copies[n].start()
    steps = column_of(elapsed[...])
    parts = in_parts(steps)
    row, col = iotas((ROWS, ROWS))
    same = row // SPAN == col // SPAN
    times[0] = sums_of(col > row, parts)
    times[1] = sums_of(col < row, parts)
    times[2] = steps
    within_ref[0] = sums_of((col <= row) & same, parts)
    within_ref[1] = sums_of((col >= row) & same, parts)
    total = sums_of(jnp.ones((8, ROWS), F32), parts)
    ends_ref[0, 64:] = total
    ends_ref[1, 64:] = total
    first = lax.broadcasted_iota(jnp.int32, (16, 128), 1) < 64

    def gather_in(step, quarter):
        if quarter == 0 and step == 0:
            for copies in fetched:
                copies[0].wait()
        cut = slice(512 * quarter, 512 * quarter + 512)
        value = mm(normed[:, cut], chunks[step, cut, :])
        summed[...] = value if quarter == 0 else summed[...] + value
        if quarter == 3:
            drive(step)

    def drive(step):
        driven = summed[...].astype(BF16)
        driven_ref[:, 256 * step : 256 * step + 256] = driven
        for j in range(8):
            pairs_ref[8 * step + j] = driven[:, 32 * j : 32 * j + 32]
        flipped[step % 2] = driven.astype(F32).T.astype(BF16)

    def pull(pair, k):
        f = pair_row(rate, k, pair)
        th = pair_row(angle, k, pair)
        pars_ref[k, 0, pair : pair + 1, :] = th
        pars_ref[k, 1, pair : pair + 1, :] = f
        after = times[k]
        s, c = half_turn(after * (th * (0.5 / math.pi)))
        bend = jnp.tanh(times[2] * f)
        damp = bend * lax.rsqrt(bend * (0.5 + 0.5 * bend) + TINY)
        damp_ref[pair, k] = damp
        amp = jnp.exp2(after * (f * -LOG2E)) * damp
        tilted = amp * s
        pulls[pair % 16, k, :, :128] = (amp - tilted * s).astype(BF16)
        pulls[pair % 16, k, :, 128:] = (tilted * c).astype(BF16)

    def finish(pair, k):
        mixed = mm(flipped[pair // 8 % 2, 32 * (pair % 8) : 32 * (pair % 8) + 32], pulls[pair % 16, k])
        m_re = jnp.where(first, mixed[:16, :128], mixed[16:, :128])
        m_im = jnp.where(first, mixed[:16, 128:], mixed[16:, 128:])
        b_re, b_im = (
            jnp.concatenate([inputs_ref[k, c, 2 * pair].astype(F32), inputs_ref[k, c, 2 * pair + 1].astype(F32)], axis=1)
            for c in range(2)
        )
        away = jnp.where(pair // 16 == core, 0, 1)
        at = 32 * k + pair % 16
        ends_ref[away, at : at + 1, :] = jnp.sum(b_re * m_re - b_im * m_im, axis=0, keepdims=True)
        ends_ref[away, at + 16 : at + 17, :] = jnp.sum(b_re * m_im + b_im * m_re, axis=0, keepdims=True)

    units = [(pair, k) for pair in range(32) for k in range(2)]
    done = 0
    for n in range(len(units) + LAG):
        if n == NORM_AT:
            norm()
        if n in DRIVE_AT:
            gather_in(*divmod(DRIVE_AT.index(n), 4))
        if n < len(units):
            pull(*units[n])
        if n == FINISH_AT:
            for copies in fetched:
                copies[1].wait()
        for _ in range(2):
            if done < len(units) and FINISH_AT <= n and done <= n - LAG:
                finish(*units[done])
                done += 1


def shifted_rows(x, by, fill):
    row = lax.broadcasted_iota(jnp.int32, (SPANS, 128), 0)
    moved = pltpu.roll(x, by % SPANS, 0)
    return jnp.where(row >= by if by > 0 else row < SPANS + by, moved, fill)


def local_kernel(start, size, fetching, within, damps, driven, inputs, readout, pars, *refs):
    copies = []
    if fetching:
        *refs, sems = refs
        sources, refs = refs[:fetching], refs[fetching:]
        out_ref, prefix_ref, table_ref, *refs = refs
        targets, refs = refs[:fetching], refs[fetching:]
        for n in range(fetching):
            copies.append(pltpu.make_async_copy(sources[n], targets[n], sems.at[n]))
            copies[n].start()
    else:
        out_ref, prefix_ref, table_ref, *refs = refs
    triangles, proj, turn, lifts, part, states, carry = refs
    row, col = iotas((ROWS, ROWS))
    same = row // SPAN == col // SPAN
    triangles[0] = ((col <= row) & same).astype(BF16)
    triangles[1] = ((col >= row) & same).astype(BF16)
    empty = jnp.zeros((16, 64), BF16)
    hole = jnp.zeros((16, 64), F32)

    def project(j, k, slot):
        pair = start + j
        b00, b01 = inputs[k, 0, 2 * pair], inputs[k, 1, 2 * pair]
        b10, b11 = inputs[k, 0, 2 * pair + 1], inputs[k, 1, 2 * pair + 1]
        rhs = jnp.concatenate(
            [
                jnp.concatenate([b00, empty, b01, empty], axis=1),
                jnp.concatenate([empty, b10, empty, b11], axis=1),
            ],
            axis=0,
        )
        proj[slot] = mm(driven[pair], rhs)

    def lift(j, k, slot):
        pair = start + j
        th, f = pars[k, 0, pair : pair + 1, :], pars[k, 1, pair : pair + 1, :]
        offs = within[k]
        cosine, sine = unit_circle(offs * (th * (0.5 / math.pi)))
        grow = jnp.exp2(offs * (f * LOG2E)) * damps[pair, k]
        fade = jnp.exp2(offs * (f * -LOG2E))
        turn[slot, 0], turn[slot, 1] = fade * cosine, fade * sine
        a_re, a_im = grow * cosine, grow * sine
        p_re, p_im = proj[slot, :, :128], proj[slot, :, 128:]
        lifts[slot, :, :128] = (a_re * p_re + a_im * p_im).astype(BF16)
        lifts[slot, :, 128:] = (a_re * p_im - a_im * p_re).astype(BF16)

    def add_up(j, k, slot):
        total = mm(triangles[k], lifts[slot])
        part[slot, 0], part[slot, 1] = total[:, :128], total[:, 128:]

    def carry_on(j, k, slot):
        edge = pl.ds(SPAN - 1 if k == 0 else 0, SPANS, stride=SPAN)
        d = turn[slot, 0, edge, :], turn[slot, 1, edge, :]
        s = times_of(d, (part[slot, 0, edge, :], part[slot, 1, edge, :]))
        sign = 1 if k == 0 else -1
        for by in (1, 2, 4):
            s_old = tuple(shifted_rows(x, sign * by, 0.0) for x in s)
            d_old = shifted_rows(d[0], sign * by, 1.0), shifted_rows(d[1], sign * by, 0.0)
            s = plus(times_of(d, s_old), s)
            d = times_of(d, d_old)
        carry[slot, 0], carry[slot, 1] = (shifted_rows(x, sign, 0.0) for x in s)
        carry[slot, 2], carry[slot, 3] = shifted_rows(d[0], sign, 1.0), shifted_rows(d[1], sign, 0.0)

    def spread(j, k, slot):
        for n in range(SPANS):
            cut = slice(SPAN * n, SPAN * n + SPAN)
            e = turn[slot, 0, cut, :], turn[slot, 1, cut, :]
            c_re, c_im, d_re, d_im = (jnp.broadcast_to(carry[slot, i, n : n + 1, :], (SPAN, 128)) for i in range(4))
            state = times_of(e, (part[slot, 0, cut, :] + c_re, part[slot, 1, cut, :] + c_im))
            states[j % 2, cut, 256 * k : 256 * k + 128] = state[0].astype(BF16)
            states[j % 2, cut, 256 * k + 128 : 256 * k + 256] = state[1].astype(BF16)
            prefix = times_of(e, (d_re, d_im))
            prefix_ref[j, k, cut, :128] = prefix[0].astype(BF16)
            prefix_ref[j, k, cut, 128:] = prefix[1].astype(BF16)

    def read(j):
        pair = start + j
        tables = []
        for k in range(2):
            for c in range(2):
                upper = jnp.concatenate([readout[k, c, 2 * pair], hole], axis=1)
                lower = jnp.concatenate([hole, readout[k, c, 2 * pair + 1]], axis=1)
                table = jnp.concatenate([upper, lower], axis=0)
                table_ref[j, k, c] = table
                tables.append((table if c == 0 else -table).astype(BF16))
        out_ref[j] = nt(states[j % 2], jnp.concatenate(tables, axis=1))

    units = [(j, k) for j in range(size) for k in range(2)]
    for turn_of in range(len(units) + 6):
        for late, act in ((0, project), (1, lift), (2, add_up), (3, carry_on), (4, spread)):
            at = turn_of - late
            if 0 <= at < len(units):
                act(*units[at], at % SLOTS)
        at = turn_of - 5
        if 0 <= at < len(units) and units[at][1] == 1:
            read(units[at][0])
    for copy in copies:
        copy.wait()


def times_of(a, b):
    return a[0] * b[0] - a[1] * b[1], a[0] * b[1] + a[1] * b[0]


def plus(a, b):
    return a[0] + b[0], a[1] + b[1]


def pick(condition, a, b):
    return tuple(jnp.where(condition, x, y) for x, y in zip(a, b))


def my_pars(pars):
    core = lax.axis_index("c")
    found = []
    for k in range(2):
        angle = pars[k, 0, pl.ds(16 * core, 16), :]
        rate = pars[k, 1, pl.ds(16 * core, 16), :]
        high = jnp.round(angle * (4096 * 0.5 / math.pi)) * (1.0 / 4096)
        coarse = 6433 / 1024
        low = ((angle - high * coarse) - high * (2 * math.pi - coarse)) * (0.5 / math.pi)
        found.append((high, low, rate * -LOG2E))
    return found


def decay_over(span, pars):
    high, low, level = pars
    u = span * high
    cosine, sine = unit_circle((u - jnp.round(u)) + span * low, SINE, COSINE)
    fade = jnp.exp2(span * level)
    return fade * cosine, fade * sine


def states_of(ref, k):
    return ref[32 * k : 32 * k + 16, :], ref[32 * k + 16 : 32 * k + 32, :]


def span_of(ref):
    span = ref[64:72, :]
    return jnp.concatenate([span, span], axis=0)


def keep_states(ref, k, value):
    ref[32 * k : 32 * k + 16, :], ref[32 * k + 16 : 32 * k + 32, :] = value


def keep_at(ref, at, value):
    ref[2 * at], ref[2 * at + 1] = value


def pair_kernel(own, other, pars, total_ref):
    core = lax.axis_index("c")
    mine = my_pars(pars)
    for k in range(2):
        ahead = core == k
        a, b = states_of(own, k), states_of(other, k)
        early, late = pick(ahead, a, b), pick(ahead, b, a)
        step = decay_over(jnp.where(ahead, span_of(other), span_of(own)), mine[k])
        keep_states(total_ref, k, plus(times_of(step, early), late))
    total_ref[64:72, :] = own[64:72, :] + other[64:72, :]


def gather_four(axis, own, one, two, three, data):
    here = lax.axis_index(axis)
    data[here] = own[...]
    data[here + 1 - 2 * (here % 2)] = one[...]
    data[(here + 2) % 4] = two[...]
    data[3 - here] = three[...]
    return here


def run_over(here, data, mine, k):
    zero = jnp.zeros((16, 128), F32)
    state, decay = (zero, zero), (zero + 1.0, zero)
    before, before_decay = state, decay
    for n in range(4) if k == 0 else range(3, -1, -1):
        before = pick(n == here, state, before)
        before_decay = pick(n == here, decay, before_decay)
        step = decay_over(span_of(data.at[n]), mine[k])
        state = plus(times_of(step, state), states_of(data.at[n], k))
        decay = times_of(step, decay)
    return state, before, before_decay


def group_kernel(axis, own, one, two, three, pars, *refs):
    *sends, before_ref, data = refs
    here = gather_four(axis, own, one, two, three, data)
    mine = my_pars(pars)
    totals = []
    for k in range(2):
        total, before, decay = run_over(here, data, mine, k)
        totals.append(total)
        keep_at(before_ref, k, before)
        keep_at(before_ref, 2 + k, decay)
    span = own[64:72, :] + one[64:72, :] + two[64:72, :] + three[64:72, :]
    if len(sends) == 1:
        for k in range(2):
            keep_states(sends[0], k, totals[k])
        sends[0][64:72, :] = span
        return
    here = lax.axis_index("z")
    partners = ((here + 2) % 4, 3 - here, here + 1 - 2 * (here % 2))
    for partner, send in zip(partners, sends):
        keep_states(send, 0, pick(partner > here, totals[0], totals[1]))
        send[32:40, :] = span


def enter_kernel(one, two, three, before_x, before_y, own, other, pars, mine_ref, theirs_ref, data):
    here = lax.axis_index("z")
    data[here] = one[...]
    data[here + 1 - 2 * (here % 2)] = one[...]
    data[(here + 2) % 4] = two[...]
    data[3 - here] = three[...]
    core = lax.axis_index("c")
    mine = my_pars(pars)
    zero = jnp.zeros((16, 128), F32)
    for k in range(2):
        state = (zero, zero)
        for n in range(3) if k == 0 else range(3, 0, -1):
            span = jnp.concatenate([data[n, 32:40, :]] * 2, axis=0)
            new = plus(times_of(decay_over(span, mine[k]), state), states_of(data.at[n], 0))
            state = pick(n < here if k == 0 else n > here, new, state)
        for before in (before_x, before_y):
            state = plus(times_of((before[4 + 2 * k], before[5 + 2 * k]), state), (before[2 * k], before[2 * k + 1]))
        ahead = core == k
        early = pick(ahead, states_of(own, k), states_of(other, k))
        later = plus(times_of(decay_over(jnp.where(ahead, span_of(own), span_of(other)), mine[k]), state), early)
        keep_at(mine_ref, k, pick(ahead, state, later))
        keep_at(theirs_ref, k, pick(ahead, later, state))


def final_kernel(*refs):
    count = len(PIECES)
    own, other = refs[:2]
    nears, prefixes, tables = (refs[2 + count * n : 2 + count * n + count] for n in range(3))
    driven, skip, glu, glu_bias, outw, out_gain, out_ref, entering, response = refs[2 + 3 * count :]
    core = lax.axis_index("c")
    entering[core] = own[...]
    entering[1 - core] = other[...]
    start = 0
    for size, near, prefix, table in zip(PIECES, nears, prefixes, tables):

        def tile(i, start=start, near=near, prefix=prefix, table=table):
            outs = []
            for j in range(4):
                total = None
                for k in range(2):
                    pair = 4 * (start + i) + j
                    er = entering[pair // 16, 2 * k, pl.ds(pair % 16, 1), :]
                    ei = entering[pair // 16, 2 * k + 1, pl.ds(pair % 16, 1), :]
                    cr, ci = table[4 * i + j, k, 0], table[4 * i + j, k, 1]
                    rhs = jnp.concatenate(
                        [(cr * er - ci * ei).astype(BF16), (-(cr * ei + ci * er)).astype(BF16)], axis=1
                    )
                    y = nt(prefix[4 * i + j, k], rhs)
                    total = y if total is None else total + y
                outs.append(total + near[4 * i + j])
            at = 128 * i
            response[:, pl.ds(at + 128 * start, 128)] = jnp.concatenate(outs, axis=1)

        for i in range(size):
            tile(i)
        start += size
    x = response[...] + skip[...] * driven[...].astype(F32)
    active = 0.5 * x * (1.0 + jnp.tanh(math.sqrt(2.0 / math.pi) * (x + 0.044715 * (x * x * x))))
    gate = mm(active.astype(BF16), glu[...]) + glu_bias[...]
    gated = (active * jax.nn.sigmoid(gate)).astype(BF16)
    projected = mm(gated, outw[...])
    scale = lax.rsqrt(jnp.mean(projected * projected, axis=-1, keepdims=True) + EPSILON)
    out_ref[...] = (projected * scale * out_gain[...]).astype(BF16)


def sds(shape, dtype=F32):
    return jax.ShapeDtypeStruct(shape, dtype)


def params(limit):
    return pltpu.CompilerParams(vmem_limit_bytes=limit * 1024 * 1024)


def run_local(start, size, args, weights):
    spec, distant = pl.BlockSpec(memory_space=VMEM), pl.BlockSpec(memory_space=pltpu.HBM)
    count = len(weights)
    return pl.pallas_call(
        functools.partial(local_kernel, 4 * start, 4 * size, count),
        name=f"local_{start}",
        in_specs=[spec] * len(args) + [distant] * count,
        out_specs=[spec] * (3 + count),
        out_shape=[
            sds((4 * size, ROWS, 32)),
            sds((4 * size, 2, ROWS, 256), BF16),
            sds((4 * size, 2, 2, 32, 128)),
            *(sds(weight.shape, BF16) for weight in weights),
        ],
        scratch_shapes=[
            VMEM((2, ROWS, ROWS), BF16), VMEM((SLOTS, ROWS, 256), F32), VMEM((SLOTS, 2, ROWS, 128), F32),
            VMEM((SLOTS, ROWS, 256), BF16), VMEM((SLOTS, 2, ROWS, 128), F32), VMEM((2, ROWS, 512), BF16),
            VMEM((SLOTS, 4, SPANS, 128), F32),
            *([pltpu.SemaphoreType.DMA((count,))] if count else []),
        ],
        compiler_params=params(8),
        cost_estimate=pl.CostEstimate(flops=size * 5 * 10**8, bytes_accessed=size * 2 * 2**20, transcendentals=0),
    )(*args, *weights)


def simple(kernel, name, shapes, args, scratch=()):
    spec = pl.BlockSpec(memory_space=VMEM)
    return pl.pallas_call(
        kernel,
        name=name,
        in_specs=[spec] * len(args),
        out_specs=[spec] * len(shapes),
        out_shape=[sds(shape) for shape in shapes],
        scratch_shapes=scratch,
        compiler_params=params(4),
    )(*args)


def local(
    tokens, elapsed, norm_gain, in_weight, state_input, state_output, forget_rate, decay_angle,
    skip_gain, glu_weight, glu_bias, out_weight, out_gain,
):
    elapsed_row = elapsed.reshape(1, ROWS)
    inputs = jnp.swapaxes(state_input, 3, 4)
    spec, distant = pl.BlockSpec(memory_space=VMEM), pl.BlockSpec(memory_space=pltpu.HBM)
    driven, pairs, ends, pars, damps, within, inputs_here = pl.pallas_call(
        end_kernel,
        name="ends",
        in_specs=[distant, spec, spec, distant, distant, spec, spec],
        out_specs=[spec] * 7,
        out_shape=[
            sds((ROWS, CHANNELS), BF16), sds((32, ROWS, 32), BF16), sds((2, 72, 128)), sds((2, 2, 32, 128)),
            sds((32, 2, ROWS, ROWS)), sds((2, ROWS, ROWS)), sds((2, 2, 64, 16, 64), BF16),
        ],
        scratch_shapes=[
            VMEM((ROWS, D), BF16), VMEM((ROWS, D), BF16), VMEM((3, ROWS, ROWS), F32), VMEM((CHUNKS, D, 256), BF16), VMEM((2, 256, ROWS), BF16),
            VMEM((ROWS, 256), F32), VMEM((16, 2, ROWS, 256), BF16),
            pltpu.SemaphoreType.DMA((CHUNKS,)), pltpu.SemaphoreType.DMA((CHUNKS,)), pltpu.SemaphoreType.DMA,
        ],
        compiler_params=params(12),
    )(
        *(hbm(a) for a in (tokens, elapsed_row, norm_gain.reshape(1, D), in_weight, inputs, decay_angle, forget_rate))
    )

    pieces, start = [], 0

    def piece_between(before, after, weights=()):
        index = len(pieces)
        start = sum(PIECES[:index])
        pairs_now, _ = lax.optimization_barrier((pairs, before))
        piece = run_local(
            start, PIECES[index],
            (within, damps, pairs_now, inputs_here, state_output, pars), weights,
        )
        *piece, after = lax.optimization_barrier((*piece, after))
        pieces.append(piece)
        return after

    swap = [(0, 1), (1, 0)]
    swaps = ([(0, 1), (1, 0), (2, 3), (3, 2)], [(0, 2), (2, 0), (1, 3), (3, 1)], [(0, 3), (3, 0), (1, 2), (2, 1)])

    def trade(values, axis, order, weights=()):
        found = piece_between(values[order[0]], tuple(lax.ppermute(values[n], axis, swaps[n]) for n in order), weights)
        return tuple(found[order.index(n)] for n in range(3))

    four = VMEM((4, 72, 128), F32)
    keep = ends[0]
    partner = piece_between(keep, lax.ppermute(ends[1], "c", swap))
    (total,) = simple(pair_kernel, "pair", [(72, 128)], (keep, partner, pars))
    befores = []
    for axis in ("y", "x"):
        others = trade((total,) * 3, axis, (0, 2, 1))
        *totals, before = simple(
            functools.partial(group_kernel, axis), f"group_{axis}",
            [(72, 128)] * (axis == "y") + [(40, 128)] * (3 * (axis == "x")) + [(8, 16, 128)],
            (total, *others, pars), [four],
        )
        total = totals[0]
        befores.append(before)
    others = trade(totals[2:] + totals[:2], "z", (1, 2, 0), (hbm(glu_weight), hbm(out_weight)))
    glu_here, outw_here = pieces[-1][3:]
    mine, theirs = simple(
        enter_kernel, "enter", [(4, 16, 128), (4, 16, 128)],
        (*others, befores[1], befores[0], keep, partner, pars), [VMEM((4, 40, 128), F32)],
    )
    other = piece_between(theirs, lax.ppermute(theirs, "c", swap))

    spec = pl.BlockSpec(memory_space=VMEM)
    args = (
        mine, other, *(p[0] for p in pieces), *(p[1] for p in pieces), *(p[2] for p in pieces),
        driven, skip_gain.reshape(1, CHANNELS), glu_here, glu_bias.reshape(1, CHANNELS), outw_here, out_gain.reshape(1, D),
    )
    return pl.pallas_call(
        final_kernel,
        name="final",
        in_specs=[spec] * len(args),
        out_specs=spec,
        out_shape=sds((ROWS, D), BF16),
        scratch_shapes=[VMEM((2, 4, 16, 128), F32), VMEM((ROWS, CHANNELS), F32)],
        compiler_params=params(12),
    )(*args)


def hbm(x):
    return pltpu.with_memory_space_constraint(x, pltpu.HBM)


def solution(mesh):
    finer = Mesh(mesh.devices.reshape(4, 4, 4, 2), AXES)
    split = P(AXES, None)
    placed = (split, P(AXES), P(), P(), P(), P(), P(), P(), P(), P(), P(), P(), P())
    return jax.shard_map(local, mesh=finer, in_specs=placed, out_specs=split, check_vma=False)
```

```python
import functools
import math

import jax
import jax.numpy as jnp
from jax import lax
from jax.experimental import pallas as pl
from jax.experimental.pallas import tpu as pltpu
from jax.sharding import Mesh
from jax.sharding import PartitionSpec as P

ROWS = 128
D = 2048
CHANNELS = 1024
CHUNKS = 4
FINISH_AT = 20
LAG = 6
NORM_AT = 14
DRIVE_AT = (14, 15, 16, 17, 18, 20, 22, 24, 26, 29, 32, 35, 37, 40, 43, 46)
SPAN = 16
SPANS = ROWS // SPAN
SLOTS = 6
PIECES = (1, 2, 2, 2, 1)
LOG2E = 1.0 / math.log(2.0)
TINY = 1e-37
EPSILON = 1e-06
AXES = ("z", "x", "y", "c")
VMEM = pltpu.VMEM
F32 = jnp.float32
BF16 = jnp.bfloat16

SINE = (4.44288291, -7.30824512, 3.60634303, -0.84604096, 0.10968436)
COSINE = (1.4142135, -6.97885097, 5.73946067, -1.88355924, 0.31068962)
SINE_SHORT = (4.44287876, -7.30776104, 3.5971931, -0.7896682)
COSINE_SHORT = (1.41420407, -6.97764062, 5.71521917, -1.7282871)


def horner(coefficients, x):
    value = coefficients[-1] * x + coefficients[-2]
    for c in coefficients[-3::-1]:
        value = value * x + c
    return value


def half_turn(turns, sine=SINE_SHORT, cosine=COSINE_SHORT):
    r = turns - jnp.round(turns)
    z = r * r
    return r * horner(sine, z), horner(cosine, z)


def unit_circle(turns, *tables):
    s, c = half_turn(turns, *tables)
    return 1.0 - s * s, s * c


def nt(a, b):
    return lax.dot_general(a, b, (((1,), (1,)), ((), ())), preferred_element_type=F32)


def mm(a, b):
    return jnp.dot(a, b, preferred_element_type=F32)


def iotas(shape):
    return lax.broadcasted_iota(jnp.int32, shape, 0), lax.broadcasted_iota(jnp.int32, shape, 1)


def column_of(row):
    return jnp.broadcast_to(row, (ROWS, ROWS)).T


def in_parts(x):
    high = x.astype(BF16)
    rest = x - high.astype(F32)
    middle = rest.astype(BF16)
    return high, middle, (rest - middle.astype(F32)).astype(BF16)


def sums_of(chosen, parts):
    return sum(mm(chosen.astype(BF16), part) for part in parts)


def pair_row(ref, k, pair):
    return jnp.concatenate([ref[k, pl.ds(2 * pair, 1), :], ref[k, pl.ds(2 * pair + 1, 1), :]], axis=1)


def end_kernel(
    tokens, elapsed, gain, weight, inputs, angle, rate,
    driven_ref, pairs_ref, ends_ref, pars_ref, damp_ref, within_ref, inputs_ref, raw, normed, times, chunks, flipped, summed, pulls, weight_sems, input_sems, token_sem,
):
    core = lax.axis_index("c")

    def fetch(i):
        return (
            pltpu.make_async_copy(
                weight.at[:, pl.ds(256 * i, 256)], chunks.at[i], weight_sems.at[i]
            ),
            pltpu.make_async_copy(inputs.at[:, :, pl.ds(16 * i, 16)], inputs_ref.at[:, :, pl.ds(16 * i, 16)], input_sems.at[i]),
        )

    def norm():
        token_copy.wait()
        for r in range(0, ROWS, 16):
            x = raw[r : r + 16, :].astype(F32)
            scale = lax.rsqrt(jnp.mean(x * x, axis=-1, keepdims=True) + EPSILON)
            normed[r : r + 16, :] = (x * scale * gain[...]).astype(BF16)

    token_copy = pltpu.make_async_copy(tokens, raw, token_sem)
    token_copy.start()
    fetched = [fetch(i) for i in range(CHUNKS)]
    for n in range(2):
        for copies in fetched:
            copies[n].start()
    steps = column_of(elapsed[...])
    parts = in_parts(steps)
    row, col = iotas((ROWS, ROWS))
    same = row // SPAN == col // SPAN
    times[0] = sums_of(col > row, parts)
    times[1] = sums_of(col < row, parts)
    times[2] = steps
    within_ref[0] = sums_of((col <= row) & same, parts)
    within_ref[1] = sums_of((col >= row) & same, parts)
    total = sums_of(jnp.ones((8, ROWS), F32), parts)
    ends_ref[0, 64:] = total
    ends_ref[1, 64:] = total
    first = lax.broadcasted_iota(jnp.int32, (16, 128), 1) < 64

    def gather_in(step, quarter):
        if quarter == 0 and step == 0:
            for copies in fetched:
                copies[0].wait()
        cut = slice(512 * quarter, 512 * quarter + 512)
        value = mm(normed[:, cut], chunks[step, cut, :])
        summed[...] = value if quarter == 0 else summed[...] + value
        if quarter == 3:
            drive(step)

    def drive(step):
        driven = summed[...].astype(BF16)
        driven_ref[:, 256 * step : 256 * step + 256] = driven
        for j in range(8):
            pairs_ref[8 * step + j] = driven[:, 32 * j : 32 * j + 32]
        flipped[step % 2] = driven.astype(F32).T.astype(BF16)

    def pull(pair, k):
        f = pair_row(rate, k, pair)
        th = pair_row(angle, k, pair)
        pars_ref[k, 0, pair : pair + 1, :] = th
        pars_ref[k, 1, pair : pair + 1, :] = f
        after = times[k]
        s, c = half_turn(after * (th * (0.5 / math.pi)))
        bend = jnp.tanh(times[2] * f)
        damp = bend * lax.rsqrt(bend * (0.5 + 0.5 * bend) + TINY)
        damp_ref[pair, k] = damp
        amp = jnp.exp2(after * (f * -LOG2E)) * damp
        tilted = amp * s
        pulls[pair % 16, k, :, :128] = (amp - tilted * s).astype(BF16)
        pulls[pair % 16, k, :, 128:] = (tilted * c).astype(BF16)

    def finish(pair, k):
        mixed = mm(flipped[pair // 8 % 2, 32 * (pair % 8) : 32 * (pair % 8) + 32], pulls[pair % 16, k])
        m_re = jnp.where(first, mixed[:16, :128], mixed[16:, :128])
        m_im = jnp.where(first, mixed[:16, 128:], mixed[16:, 128:])
        b_re, b_im = (
            jnp.concatenate([inputs_ref[k, c, 2 * pair].astype(F32), inputs_ref[k, c, 2 * pair + 1].astype(F32)], axis=1)
            for c in range(2)
        )
        away = jnp.where(pair // 16 == core, 0, 1)
        at = 32 * k + pair % 16
        ends_ref[away, at : at + 1, :] = jnp.sum(b_re * m_re - b_im * m_im, axis=0, keepdims=True)
        ends_ref[away, at + 16 : at + 17, :] = jnp.sum(b_re * m_im + b_im * m_re, axis=0, keepdims=True)

    units = [(pair, k) for pair in range(32) for k in range(2)]
    done = 0
    for n in range(len(units) + LAG):
        if n == NORM_AT:
            norm()
        if n in DRIVE_AT:
            gather_in(*divmod(DRIVE_AT.index(n), 4))
        if n < len(units):
            pull(*units[n])
        if n == FINISH_AT:
            for copies in fetched:
                copies[1].wait()
        for _ in range(2):
            if done < len(units) and FINISH_AT <= n and done <= n - LAG:
                finish(*units[done])
                done += 1


def shifted_rows(x, by, fill):
    row = lax.broadcasted_iota(jnp.int32, (SPANS, 128), 0)
    moved = pltpu.roll(x, by % SPANS, 0)
    return jnp.where(row >= by if by > 0 else row < SPANS + by, moved, fill)


def local_kernel(start, size, fetching, within, damps, driven, inputs, readout, pars, *refs):
    copies = []
    if fetching:
        *refs, sems = refs
        sources, refs = refs[:fetching], refs[fetching:]
        out_ref, prefix_ref, table_ref, *refs = refs
        targets, refs = refs[:fetching], refs[fetching:]
        for n in range(fetching):
            copies.append(pltpu.make_async_copy(sources[n], targets[n], sems.at[n]))
            copies[n].start()
    else:
        out_ref, prefix_ref, table_ref, *refs = refs
    triangles, proj, turn, lifts, part, states, carry = refs
    row, col = iotas((ROWS, ROWS))
    same = row // SPAN == col // SPAN
    triangles[0] = ((col <= row) & same).astype(BF16)
    triangles[1] = ((col >= row) & same).astype(BF16)
    empty = jnp.zeros((16, 64), BF16)
    hole = jnp.zeros((16, 64), F32)

    def project(j, k, slot):
        pair = start + j
        b00, b01 = inputs[k, 0, 2 * pair], inputs[k, 1, 2 * pair]
        b10, b11 = inputs[k, 0, 2 * pair + 1], inputs[k, 1, 2 * pair + 1]
        rhs = jnp.concatenate(
            [
                jnp.concatenate([b00, empty, b01, empty], axis=1),
                jnp.concatenate([empty, b10, empty, b11], axis=1),
            ],
            axis=0,
        )
        proj[slot] = mm(driven[pair], rhs)

    def lift(j, k, slot):
        pair = start + j
        th, f = pars[k, 0, pair : pair + 1, :], pars[k, 1, pair : pair + 1, :]
        offs = within[k]
        cosine, sine = unit_circle(offs * (th * (0.5 / math.pi)))
        grow = jnp.exp2(offs * (f * LOG2E)) * damps[pair, k]
        fade = jnp.exp2(offs * (f * -LOG2E))
        turn[slot, 0], turn[slot, 1] = fade * cosine, fade * sine
        a_re, a_im = grow * cosine, grow * sine
        p_re, p_im = proj[slot, :, :128], proj[slot, :, 128:]
        lifts[slot, :, :128] = (a_re * p_re + a_im * p_im).astype(BF16)
        lifts[slot, :, 128:] = (a_re * p_im - a_im * p_re).astype(BF16)

    def add_up(j, k, slot):
        total = mm(triangles[k], lifts[slot])
        part[slot, 0], part[slot, 1] = total[:, :128], total[:, 128:]

    def carry_on(j, k, slot):
        edge = pl.ds(SPAN - 1 if k == 0 else 0, SPANS, stride=SPAN)
        d = turn[slot, 0, edge, :], turn[slot, 1, edge, :]
        s = times_of(d, (part[slot, 0, edge, :], part[slot, 1, edge, :]))
        sign = 1 if k == 0 else -1
        for by in (1, 2, 4):
            s_old = tuple(shifted_rows(x, sign * by, 0.0) for x in s)
            d_old = shifted_rows(d[0], sign * by, 1.0), shifted_rows(d[1], sign * by, 0.0)
            s = plus(times_of(d, s_old), s)
            d = times_of(d, d_old)
        carry[slot, 0], carry[slot, 1] = (shifted_rows(x, sign, 0.0) for x in s)
        carry[slot, 2], carry[slot, 3] = shifted_rows(d[0], sign, 1.0), shifted_rows(d[1], sign, 0.0)

    def spread(j, k, slot):
        for n in range(SPANS):
            cut = slice(SPAN * n, SPAN * n + SPAN)
            e = turn[slot, 0, cut, :], turn[slot, 1, cut, :]
            c_re, c_im, d_re, d_im = (jnp.broadcast_to(carry[slot, i, n : n + 1, :], (SPAN, 128)) for i in range(4))
            state = times_of(e, (part[slot, 0, cut, :] + c_re, part[slot, 1, cut, :] + c_im))
            states[j % 2, cut, 256 * k : 256 * k + 128] = state[0].astype(BF16)
            states[j % 2, cut, 256 * k + 128 : 256 * k + 256] = state[1].astype(BF16)
            prefix = times_of(e, (d_re, d_im))
            prefix_ref[j, k, cut, :128] = prefix[0].astype(BF16)
            prefix_ref[j, k, cut, 128:] = prefix[1].astype(BF16)

    def read(j):
        pair = start + j
        tables = []
        for k in range(2):
            for c in range(2):
                upper = jnp.concatenate([readout[k, c, 2 * pair], hole], axis=1)
                lower = jnp.concatenate([hole, readout[k, c, 2 * pair + 1]], axis=1)
                table = jnp.concatenate([upper, lower], axis=0)
                table_ref[j, k, c] = table
                tables.append((table if c == 0 else -table).astype(BF16))
        out_ref[j] = nt(states[j % 2], jnp.concatenate(tables, axis=1))

    units = [(j, k) for j in range(size) for k in range(2)]
    for turn_of in range(len(units) + 6):
        for late, act in ((0, project), (1, lift), (2, add_up), (3, carry_on), (4, spread)):
            at = turn_of - late
            if 0 <= at < len(units):
                act(*units[at], at % SLOTS)
        at = turn_of - 5
        if 0 <= at < len(units) and units[at][1] == 1:
            read(units[at][0])
    for copy in copies:
        copy.wait()


def times_of(a, b):
    return a[0] * b[0] - a[1] * b[1], a[0] * b[1] + a[1] * b[0]


def plus(a, b):
    return a[0] + b[0], a[1] + b[1]


def pick(condition, a, b):
    return tuple(jnp.where(condition, x, y) for x, y in zip(a, b))


def my_pars(pars):
    core = lax.axis_index("c")
    found = []
    for k in range(2):
        angle = pars[k, 0, pl.ds(16 * core, 16), :]
        rate = pars[k, 1, pl.ds(16 * core, 16), :]
        high = jnp.round(angle * (4096 * 0.5 / math.pi)) * (1.0 / 4096)
        coarse = 6433 / 1024
        low = ((angle - high * coarse) - high * (2 * math.pi - coarse)) * (0.5 / math.pi)
        found.append((high, low, rate * -LOG2E))
    return found


def decay_over(span, pars):
    high, low, level = pars
    u = span * high
    cosine, sine = unit_circle((u - jnp.round(u)) + span * low, SINE, COSINE)
    fade = jnp.exp2(span * level)
    return fade * cosine, fade * sine


def states_of(ref, k):
    return ref[32 * k : 32 * k + 16, :], ref[32 * k + 16 : 32 * k + 32, :]


def span_of(ref):
    span = ref[64:72, :]
    return jnp.concatenate([span, span], axis=0)


def keep_states(ref, k, value):
    ref[32 * k : 32 * k + 16, :], ref[32 * k + 16 : 32 * k + 32, :] = value


def keep_at(ref, at, value):
    ref[2 * at], ref[2 * at + 1] = value


def pair_kernel(own, other, pars, total_ref):
    core = lax.axis_index("c")
    mine = my_pars(pars)
    for k in range(2):
        ahead = core == k
        a, b = states_of(own, k), states_of(other, k)
        early, late = pick(ahead, a, b), pick(ahead, b, a)
        step = decay_over(jnp.where(ahead, span_of(other), span_of(own)), mine[k])
        keep_states(total_ref, k, plus(times_of(step, early), late))
    total_ref[64:72, :] = own[64:72, :] + other[64:72, :]


def gather_four(axis, own, one, two, three, data):
    here = lax.axis_index(axis)
    data[here] = own[...]
    data[here + 1 - 2 * (here % 2)] = one[...]
    data[(here + 2) % 4] = two[...]
    data[3 - here] = three[...]
    return here


def run_over(here, data, mine, k):
    zero = jnp.zeros((16, 128), F32)
    state, decay = (zero, zero), (zero + 1.0, zero)
    before, before_decay = state, decay
    for n in range(4) if k == 0 else range(3, -1, -1):
        before = pick(n == here, state, before)
        before_decay = pick(n == here, decay, before_decay)
        step = decay_over(span_of(data.at[n]), mine[k])
        state = plus(times_of(step, state), states_of(data.at[n], k))
        decay = times_of(step, decay)
    return state, before, before_decay


def group_kernel(axis, own, one, two, three, pars, *refs):
    *sends, before_ref, data = refs
    here = gather_four(axis, own, one, two, three, data)
    mine = my_pars(pars)
    totals = []
    for k in range(2):
        total, before, decay = run_over(here, data, mine, k)
        totals.append(total)
        keep_at(before_ref, k, before)
        keep_at(before_ref, 2 + k, decay)
    span = own[64:72, :] + one[64:72, :] + two[64:72, :] + three[64:72, :]
    if len(sends) == 1:
        for k in range(2):
            keep_states(sends[0], k, totals[k])
        sends[0][64:72, :] = span
        return
    here = lax.axis_index("z")
    partners = ((here + 2) % 4, 3 - here, here + 1 - 2 * (here % 2))
    for partner, send in zip(partners, sends):
        keep_states(send, 0, pick(partner > here, totals[0], totals[1]))
        send[32:40, :] = span


def enter_kernel(one, two, three, before_x, before_y, own, other, pars, mine_ref, theirs_ref, data):
    here = lax.axis_index("z")
    data[here] = one[...]
    data[here + 1 - 2 * (here % 2)] = one[...]
    data[(here + 2) % 4] = two[...]
    data[3 - here] = three[...]
    core = lax.axis_index("c")
    mine = my_pars(pars)
    zero = jnp.zeros((16, 128), F32)
    for k in range(2):
        state = (zero, zero)
        for n in range(3) if k == 0 else range(3, 0, -1):
            span = jnp.concatenate([data[n, 32:40, :]] * 2, axis=0)
            new = plus(times_of(decay_over(span, mine[k]), state), states_of(data.at[n], 0))
            state = pick(n < here if k == 0 else n > here, new, state)
        for before in (before_x, before_y):
            state = plus(times_of((before[4 + 2 * k], before[5 + 2 * k]), state), (before[2 * k], before[2 * k + 1]))
        ahead = core == k
        early = pick(ahead, states_of(own, k), states_of(other, k))
        later = plus(times_of(decay_over(jnp.where(ahead, span_of(own), span_of(other)), mine[k]), state), early)
        keep_at(mine_ref, k, pick(ahead, state, later))
        keep_at(theirs_ref, k, pick(ahead, later, state))


def final_kernel(*refs):
    count = len(PIECES)
    own, other = refs[:2]
    nears, prefixes, tables = (refs[2 + count * n : 2 + count * n + count] for n in range(3))
    driven, skip, glu, glu_bias, outw, out_gain, out_ref, entering, response, staged, sems = refs[2 + 3 * count :]
    core = lax.axis_index("c")
    entering[core] = own[...]
    entering[1 - core] = other[...]
    start = 0
    for size, near, prefix, table in zip(PIECES, nears, prefixes, tables):

        def tile(i, start=start, near=near, prefix=prefix, table=table):
            outs = []
            for j in range(4):
                total = None
                for k in range(2):
                    pair = 4 * (start + i) + j
                    er = entering[pair // 16, 2 * k, pl.ds(pair % 16, 1), :]
                    ei = entering[pair // 16, 2 * k + 1, pl.ds(pair % 16, 1), :]
                    cr, ci = table[4 * i + j, k, 0], table[4 * i + j, k, 1]
                    rhs = jnp.concatenate(
                        [(cr * er - ci * ei).astype(BF16), (-(cr * ei + ci * er)).astype(BF16)], axis=1
                    )
                    y = nt(prefix[4 * i + j, k], rhs)
                    total = y if total is None else total + y
                outs.append(total + near[4 * i + j])
            at = 128 * i
            response[:, pl.ds(at + 128 * start, 128)] = jnp.concatenate(outs, axis=1)

        for i in range(size):
            tile(i)
        start += size
    x = response[...] + skip[...] * driven[...].astype(F32)
    active = 0.5 * x * (1.0 + jnp.tanh(math.sqrt(2.0 / math.pi) * (x + 0.044715 * (x * x * x))))
    gate = mm(active.astype(BF16), glu[...]) + glu_bias[...]
    gated = (active * jax.nn.sigmoid(gate)).astype(BF16)
    projected = mm(gated, outw[...])
    copies = []
    for n, r in enumerate(range(0, ROWS, 32)):
        rows = projected[r : r + 32, :]
        scale = lax.rsqrt(jnp.mean(rows * rows, axis=-1, keepdims=True) + EPSILON)
        staged[r : r + 32, :] = (rows * scale * out_gain[...]).astype(BF16)
        copies.append(pltpu.make_async_copy(staged.at[r : r + 32, :], out_ref.at[r : r + 32, :], sems.at[n]))
        copies[n].start()
    for copy in copies:
        copy.wait()


def sds(shape, dtype=F32):
    return jax.ShapeDtypeStruct(shape, dtype)


def params(limit):
    return pltpu.CompilerParams(vmem_limit_bytes=limit * 1024 * 1024)


def run_local(start, size, args, weights):
    spec, distant = pl.BlockSpec(memory_space=VMEM), pl.BlockSpec(memory_space=pltpu.HBM)
    count = len(weights)
    return pl.pallas_call(
        functools.partial(local_kernel, 4 * start, 4 * size, count),
        name=f"local_{start}",
        in_specs=[spec] * len(args) + [distant] * count,
        out_specs=[spec] * (3 + count),
        out_shape=[
            sds((4 * size, ROWS, 32)),
            sds((4 * size, 2, ROWS, 256), BF16),
            sds((4 * size, 2, 2, 32, 128)),
            *(sds(weight.shape, BF16) for weight in weights),
        ],
        scratch_shapes=[
            VMEM((2, ROWS, ROWS), BF16), VMEM((SLOTS, ROWS, 256), F32), VMEM((SLOTS, 2, ROWS, 128), F32),
            VMEM((SLOTS, ROWS, 256), BF16), VMEM((SLOTS, 2, ROWS, 128), F32), VMEM((2, ROWS, 512), BF16),
            VMEM((SLOTS, 4, SPANS, 128), F32),
            *([pltpu.SemaphoreType.DMA((count,))] if count else []),
        ],
        compiler_params=params(8),
        cost_estimate=pl.CostEstimate(flops=size * 5 * 10**8, bytes_accessed=size * 2 * 2**20, transcendentals=0),
    )(*args, *weights)


def simple(kernel, name, shapes, args, scratch=()):
    spec = pl.BlockSpec(memory_space=VMEM)
    return pl.pallas_call(
        kernel,
        name=name,
        in_specs=[spec] * len(args),
        out_specs=[spec] * len(shapes),
        out_shape=[sds(shape) for shape in shapes],
        scratch_shapes=scratch,
        compiler_params=params(4),
    )(*args)


def local(
    tokens, elapsed, norm_gain, in_weight, state_input, state_output, forget_rate, decay_angle,
    skip_gain, glu_weight, glu_bias, out_weight, out_gain,
):
    elapsed_row = elapsed.reshape(1, ROWS)
    inputs = jnp.swapaxes(state_input, 3, 4)
    spec, distant = pl.BlockSpec(memory_space=VMEM), pl.BlockSpec(memory_space=pltpu.HBM)
    driven, pairs, ends, pars, damps, within, inputs_here = pl.pallas_call(
        end_kernel,
        name="ends",
        in_specs=[distant, spec, spec, distant, distant, spec, spec],
        out_specs=[spec] * 7,
        out_shape=[
            sds((ROWS, CHANNELS), BF16), sds((32, ROWS, 32), BF16), sds((2, 72, 128)), sds((2, 2, 32, 128)),
            sds((32, 2, ROWS, ROWS)), sds((2, ROWS, ROWS)), sds((2, 2, 64, 16, 64), BF16),
        ],
        scratch_shapes=[
            VMEM((ROWS, D), BF16), VMEM((ROWS, D), BF16), VMEM((3, ROWS, ROWS), F32), VMEM((CHUNKS, D, 256), BF16), VMEM((2, 256, ROWS), BF16),
            VMEM((ROWS, 256), F32), VMEM((16, 2, ROWS, 256), BF16),
            pltpu.SemaphoreType.DMA((CHUNKS,)), pltpu.SemaphoreType.DMA((CHUNKS,)), pltpu.SemaphoreType.DMA,
        ],
        compiler_params=params(12),
    )(
        *(hbm(a) for a in (tokens, elapsed_row, norm_gain.reshape(1, D), in_weight, inputs, decay_angle, forget_rate))
    )

    pieces, start = [], 0

    def piece_between(before, after, weights=()):
        index = len(pieces)
        start = sum(PIECES[:index])
        pairs_now, _ = lax.optimization_barrier((pairs, before))
        piece = run_local(
            start, PIECES[index],
            (within, damps, pairs_now, inputs_here, state_output, pars), weights,
        )
        *piece, after = lax.optimization_barrier((*piece, after))
        pieces.append(piece)
        return after

    swap = [(0, 1), (1, 0)]
    swaps = ([(0, 1), (1, 0), (2, 3), (3, 2)], [(0, 2), (2, 0), (1, 3), (3, 1)], [(0, 3), (3, 0), (1, 2), (2, 1)])

    def trade(values, axis, order, weights=()):
        found = piece_between(values[order[0]], tuple(lax.ppermute(values[n], axis, swaps[n]) for n in order), weights)
        return tuple(found[order.index(n)] for n in range(3))

    four = VMEM((4, 72, 128), F32)
    keep = ends[0]
    partner = piece_between(keep, lax.ppermute(ends[1], "c", swap))
    (total,) = simple(pair_kernel, "pair", [(72, 128)], (keep, partner, pars))
    befores = []
    for axis in ("y", "x"):
        others = trade((total,) * 3, axis, (0, 2, 1))
        *totals, before = simple(
            functools.partial(group_kernel, axis), f"group_{axis}",
            [(72, 128)] * (axis == "y") + [(40, 128)] * (3 * (axis == "x")) + [(8, 16, 128)],
            (total, *others, pars), [four],
        )
        total = totals[0]
        befores.append(before)
    others = trade(totals[2:] + totals[:2], "z", (1, 2, 0), (hbm(glu_weight), hbm(out_weight)))
    glu_here, outw_here = pieces[-1][3:]
    mine, theirs = simple(
        enter_kernel, "enter", [(4, 16, 128), (4, 16, 128)],
        (*others, befores[1], befores[0], keep, partner, pars), [VMEM((4, 40, 128), F32)],
    )
    other = piece_between(theirs, lax.ppermute(theirs, "c", swap))

    spec = pl.BlockSpec(memory_space=VMEM)
    args = (
        mine, other, *(p[0] for p in pieces), *(p[1] for p in pieces), *(p[2] for p in pieces),
        driven, skip_gain.reshape(1, CHANNELS), glu_here, glu_bias.reshape(1, CHANNELS), outw_here, out_gain.reshape(1, D),
    )
    return pl.pallas_call(
        final_kernel,
        name="final",
        in_specs=[spec] * len(args),
        out_specs=pl.BlockSpec(memory_space=pltpu.HBM),
        out_shape=sds((ROWS, D), BF16),
        scratch_shapes=[
            VMEM((2, 4, 16, 128), F32), VMEM((ROWS, CHANNELS), F32), VMEM((ROWS, D), BF16),
            pltpu.SemaphoreType.DMA((4,)),
        ],
        compiler_params=params(12),
    )(*args)


def hbm(x):
    return pltpu.with_memory_space_constraint(x, pltpu.HBM)


def solution(mesh):
    finer = Mesh(mesh.devices.reshape(4, 4, 4, 2), AXES)
    split = P(AXES, None)
    placed = (split, P(AXES), P(), P(), P(), P(), P(), P(), P(), P(), P(), P(), P())
    return jax.shard_map(local, mesh=finer, in_specs=placed, out_specs=split, check_vma=False)
```

```python
import functools
import math

import jax
import jax.numpy as jnp
from jax import lax
from jax.experimental import pallas as pl
from jax.experimental.pallas import tpu as pltpu
from jax.sharding import Mesh
from jax.sharding import PartitionSpec as P

ROWS = 128
D = 2048
CHANNELS = 1024
CHUNKS = 4
FINISH_AT = 30
LAG = 6
NORM_AT = 24
DRIVE_AT = (24, 25, 26, 27, 28, 30, 32, 34, 36, 38, 40, 42, 46, 48, 50, 52)
SPAN = 16
SPANS = ROWS // SPAN
SLOTS = 6
PIECES = (1, 2, 2, 2, 1)
LOG2E = 1.0 / math.log(2.0)
TINY = 1e-37
EPSILON = 1e-06
AXES = ("z", "x", "y", "c")
VMEM = pltpu.VMEM
F32 = jnp.float32
BF16 = jnp.bfloat16

SINE = (4.44288291, -7.30824512, 3.60634303, -0.84604096, 0.10968436)
COSINE = (1.4142135, -6.97885097, 5.73946067, -1.88355924, 0.31068962)
SINE_SHORT = (4.44287876, -7.30776104, 3.5971931, -0.7896682)
COSINE_SHORT = (1.41420407, -6.97764062, 5.71521917, -1.7282871)


def horner(coefficients, x):
    value = coefficients[-1] * x + coefficients[-2]
    for c in coefficients[-3::-1]:
        value = value * x + c
    return value


def half_turn(turns, sine=SINE_SHORT, cosine=COSINE_SHORT):
    r = turns - jnp.round(turns)
    z = r * r
    return r * horner(sine, z), horner(cosine, z)


def unit_circle(turns, *tables):
    s, c = half_turn(turns, *tables)
    return 1.0 - s * s, s * c


def nt(a, b):
    return lax.dot_general(a, b, (((1,), (1,)), ((), ())), preferred_element_type=F32)


def mm(a, b):
    return jnp.dot(a, b, preferred_element_type=F32)


def iotas(shape):
    return lax.broadcasted_iota(jnp.int32, shape, 0), lax.broadcasted_iota(jnp.int32, shape, 1)


def column_of(row):
    return jnp.broadcast_to(row, (ROWS, ROWS)).T


def in_parts(x):
    high = x.astype(BF16)
    rest = x - high.astype(F32)
    middle = rest.astype(BF16)
    return high, middle, (rest - middle.astype(F32)).astype(BF16)


def sums_of(chosen, parts):
    return sum(mm(chosen.astype(BF16), part) for part in parts)


def pair_row(ref, k, pair):
    return jnp.concatenate([ref[k, pl.ds(2 * pair, 1), :], ref[k, pl.ds(2 * pair + 1, 1), :]], axis=1)


def end_kernel(
    tokens, elapsed, gain, weight, inputs, angle, rate,
    driven_ref, pairs_ref, ends_ref, pars_ref, damp_ref, within_ref, inputs_ref, raw, normed, times, chunks, flipped, summed, pulls, weight_sems, input_sems, token_sem,
):
    core = lax.axis_index("c")

    def fetch(i):
        return (
            pltpu.make_async_copy(
                weight.at[:, pl.ds(256 * i, 256)], chunks.at[i], weight_sems.at[i]
            ),
            pltpu.make_async_copy(inputs.at[:, :, pl.ds(16 * i, 16)], inputs_ref.at[:, :, pl.ds(16 * i, 16)], input_sems.at[i]),
        )

    def norm():
        token_copy.wait()
        for r in range(0, ROWS, 16):
            x = raw[r : r + 16, :].astype(F32)
            scale = lax.rsqrt(jnp.mean(x * x, axis=-1, keepdims=True) + EPSILON)
            normed[r : r + 16, :] = (x * scale * gain[...]).astype(BF16)

    token_copy = pltpu.make_async_copy(tokens, raw, token_sem)
    token_copy.start()
    fetched = [fetch(i) for i in range(CHUNKS)]
    for n in range(2):
        for copies in fetched:
            copies[n].start()
    steps = column_of(elapsed[...])
    parts = in_parts(steps)
    row, col = iotas((ROWS, ROWS))
    same = row // SPAN == col // SPAN
    times[0] = sums_of(col > row, parts)
    times[1] = sums_of(col < row, parts)
    times[2] = steps
    within_ref[0] = sums_of((col <= row) & same, parts)
    within_ref[1] = sums_of((col >= row) & same, parts)
    total = sums_of(jnp.ones((8, ROWS), F32), parts)
    ends_ref[0, 64:] = total
    ends_ref[1, 64:] = total
    first = lax.broadcasted_iota(jnp.int32, (16, 128), 1) < 64

    def gather_in(step, quarter):
        if quarter == 0 and step == 0:
            for copies in fetched:
                copies[0].wait()
        cut = slice(512 * quarter, 512 * quarter + 512)
        value = mm(normed[:, cut], chunks[step, cut, :])
        summed[...] = value if quarter == 0 else summed[...] + value
        if quarter == 3:
            drive(step)

    def drive(step):
        driven = summed[...].astype(BF16)
        driven_ref[:, 256 * step : 256 * step + 256] = driven
        for j in range(8):
            pairs_ref[8 * step + j] = driven[:, 32 * j : 32 * j + 32]
        flipped[step % 2] = driven.astype(F32).T.astype(BF16)

    def pull(pair, k):
        f = pair_row(rate, k, pair)
        th = pair_row(angle, k, pair)
        pars_ref[k, 0, pair : pair + 1, :] = th
        pars_ref[k, 1, pair : pair + 1, :] = f
        after = times[k]
        s, c = half_turn(after * (th * (0.5 / math.pi)))
        bend = jnp.tanh(times[2] * f)
        damp = bend * lax.rsqrt(bend * (0.5 + 0.5 * bend) + TINY)
        damp_ref[pair, k] = damp
        amp = jnp.exp2(after * (f * -LOG2E)) * damp
        tilted = amp * s
        pulls[pair % 16, k, :, :128] = (amp - tilted * s).astype(BF16)
        pulls[pair % 16, k, :, 128:] = (tilted * c).astype(BF16)

    def finish(pair, k):
        mixed = mm(flipped[pair // 8 % 2, 32 * (pair % 8) : 32 * (pair % 8) + 32], pulls[pair % 16, k])
        m_re = jnp.where(first, mixed[:16, :128], mixed[16:, :128])
        m_im = jnp.where(first, mixed[:16, 128:], mixed[16:, 128:])
        b_re, b_im = (
            jnp.concatenate([inputs_ref[k, c, 2 * pair].astype(F32), inputs_ref[k, c, 2 * pair + 1].astype(F32)], axis=1)
            for c in range(2)
        )
        away = jnp.where(pair // 16 == core, 0, 1)
        at = 32 * k + pair % 16
        ends_ref[away, at : at + 1, :] = jnp.sum(b_re * m_re - b_im * m_im, axis=0, keepdims=True)
        ends_ref[away, at + 16 : at + 17, :] = jnp.sum(b_re * m_im + b_im * m_re, axis=0, keepdims=True)

    units = [(pair, k) for pair in range(32) for k in range(2)]
    done = 0
    for n in range(len(units) + LAG):
        if n == NORM_AT:
            norm()
        if n in DRIVE_AT:
            gather_in(*divmod(DRIVE_AT.index(n), 4))
        if n < len(units):
            pull(*units[n])
        if n == FINISH_AT:
            for copies in fetched:
                copies[1].wait()
        for _ in range(2):
            if done < len(units) and FINISH_AT <= n and done <= n - LAG:
                finish(*units[done])
                done += 1


def shifted_rows(x, by, fill):
    row = lax.broadcasted_iota(jnp.int32, (SPANS, 128), 0)
    moved = pltpu.roll(x, by % SPANS, 0)
    return jnp.where(row >= by if by > 0 else row < SPANS + by, moved, fill)


def local_kernel(start, size, fetching, within, damps, driven, inputs, readout, pars, *refs):
    copies = []
    if fetching:
        *refs, sems = refs
        sources, refs = refs[:fetching], refs[fetching:]
        out_ref, prefix_ref, table_ref, *refs = refs
        targets, refs = refs[:fetching], refs[fetching:]
        for n in range(fetching):
            copies.append(pltpu.make_async_copy(sources[n], targets[n], sems.at[n]))
            copies[n].start()
    else:
        out_ref, prefix_ref, table_ref, *refs = refs
    triangles, proj, turn, lifts, part, states, carry = refs
    row, col = iotas((ROWS, ROWS))
    same = row // SPAN == col // SPAN
    triangles[0] = ((col <= row) & same).astype(BF16)
    triangles[1] = ((col >= row) & same).astype(BF16)
    empty = jnp.zeros((16, 64), BF16)
    hole = jnp.zeros((16, 64), F32)

    def project(j, k, slot):
        pair = start + j
        b00, b01 = inputs[k, 0, 2 * pair], inputs[k, 1, 2 * pair]
        b10, b11 = inputs[k, 0, 2 * pair + 1], inputs[k, 1, 2 * pair + 1]
        rhs = jnp.concatenate(
            [
                jnp.concatenate([b00, empty, b01, empty], axis=1),
                jnp.concatenate([empty, b10, empty, b11], axis=1),
            ],
            axis=0,
        )
        proj[slot] = mm(driven[pair], rhs)

    def lift(j, k, slot):
        pair = start + j
        th, f = pars[k, 0, pair : pair + 1, :], pars[k, 1, pair : pair + 1, :]
        offs = within[k]
        cosine, sine = unit_circle(offs * (th * (0.5 / math.pi)))
        grow = jnp.exp2(offs * (f * LOG2E)) * damps[pair, k]
        fade = jnp.exp2(offs * (f * -LOG2E))
        turn[slot, 0], turn[slot, 1] = fade * cosine, fade * sine
        a_re, a_im = grow * cosine, grow * sine
        p_re, p_im = proj[slot, :, :128], proj[slot, :, 128:]
        lifts[slot, :, :128] = (a_re * p_re + a_im * p_im).astype(BF16)
        lifts[slot, :, 128:] = (a_re * p_im - a_im * p_re).astype(BF16)

    def add_up(j, k, slot):
        total = mm(triangles[k], lifts[slot])
        part[slot, 0], part[slot, 1] = total[:, :128], total[:, 128:]

    def carry_on(j, k, slot):
        edge = pl.ds(SPAN - 1 if k == 0 else 0, SPANS, stride=SPAN)
        d = turn[slot, 0, edge, :], turn[slot, 1, edge, :]
        s = times_of(d, (part[slot, 0, edge, :], part[slot, 1, edge, :]))
        sign = 1 if k == 0 else -1
        for by in (1, 2, 4):
            s_old = tuple(shifted_rows(x, sign * by, 0.0) for x in s)
            d_old = shifted_rows(d[0], sign * by, 1.0), shifted_rows(d[1], sign * by, 0.0)
            s = plus(times_of(d, s_old), s)
            d = times_of(d, d_old)
        carry[slot, 0], carry[slot, 1] = (shifted_rows(x, sign, 0.0) for x in s)
        carry[slot, 2], carry[slot, 3] = shifted_rows(d[0], sign, 1.0), shifted_rows(d[1], sign, 0.0)

    def spread(j, k, slot):
        for n in range(SPANS):
            cut = slice(SPAN * n, SPAN * n + SPAN)
            e = turn[slot, 0, cut, :], turn[slot, 1, cut, :]
            c_re, c_im, d_re, d_im = (jnp.broadcast_to(carry[slot, i, n : n + 1, :], (SPAN, 128)) for i in range(4))
            state = times_of(e, (part[slot, 0, cut, :] + c_re, part[slot, 1, cut, :] + c_im))
            states[j % 2, cut, 256 * k : 256 * k + 128] = state[0].astype(BF16)
            states[j % 2, cut, 256 * k + 128 : 256 * k + 256] = state[1].astype(BF16)
            prefix = times_of(e, (d_re, d_im))
            prefix_ref[j, k, cut, :128] = prefix[0].astype(BF16)
            prefix_ref[j, k, cut, 128:] = prefix[1].astype(BF16)

    def read(j):
        pair = start + j
        tables = []
        for k in range(2):
            for c in range(2):
                upper = jnp.concatenate([readout[k, c, 2 * pair], hole], axis=1)
                lower = jnp.concatenate([hole, readout[k, c, 2 * pair + 1]], axis=1)
                table = jnp.concatenate([upper, lower], axis=0)
                table_ref[j, k, c] = table
                tables.append((table if c == 0 else -table).astype(BF16))
        out_ref[j] = nt(states[j % 2], jnp.concatenate(tables, axis=1))

    units = [(j, k) for j in range(size) for k in range(2)]
    for turn_of in range(len(units) + 6):
        for late, act in ((0, project), (1, lift), (2, add_up), (3, carry_on), (4, spread)):
            at = turn_of - late
            if 0 <= at < len(units):
                act(*units[at], at % SLOTS)
        at = turn_of - 5
        if 0 <= at < len(units) and units[at][1] == 1:
            read(units[at][0])
    for copy in copies:
        copy.wait()


def times_of(a, b):
    return a[0] * b[0] - a[1] * b[1], a[0] * b[1] + a[1] * b[0]


def plus(a, b):
    return a[0] + b[0], a[1] + b[1]


def pick(condition, a, b):
    return tuple(jnp.where(condition, x, y) for x, y in zip(a, b))


def my_pars(pars):
    core = lax.axis_index("c")
    found = []
    for k in range(2):
        angle = pars[k, 0, pl.ds(16 * core, 16), :]
        rate = pars[k, 1, pl.ds(16 * core, 16), :]
        high = jnp.round(angle * (4096 * 0.5 / math.pi)) * (1.0 / 4096)
        coarse = 6433 / 1024
        low = ((angle - high * coarse) - high * (2 * math.pi - coarse)) * (0.5 / math.pi)
        found.append((high, low, rate * -LOG2E))
    return found


def decay_over(span, pars):
    high, low, level = pars
    u = span * high
    cosine, sine = unit_circle((u - jnp.round(u)) + span * low, SINE, COSINE)
    fade = jnp.exp2(span * level)
    return fade * cosine, fade * sine


def states_of(ref, k):
    return ref[32 * k : 32 * k + 16, :], ref[32 * k + 16 : 32 * k + 32, :]


def span_of(ref):
    span = ref[64:72, :]
    return jnp.concatenate([span, span], axis=0)


def keep_states(ref, k, value):
    ref[32 * k : 32 * k + 16, :], ref[32 * k + 16 : 32 * k + 32, :] = value


def keep_at(ref, at, value):
    ref[2 * at], ref[2 * at + 1] = value


def pair_kernel(own, other, pars, total_ref):
    core = lax.axis_index("c")
    mine = my_pars(pars)
    for k in range(2):
        ahead = core == k
        a, b = states_of(own, k), states_of(other, k)
        early, late = pick(ahead, a, b), pick(ahead, b, a)
        step = decay_over(jnp.where(ahead, span_of(other), span_of(own)), mine[k])
        keep_states(total_ref, k, plus(times_of(step, early), late))
    total_ref[64:72, :] = own[64:72, :] + other[64:72, :]


def gather_four(axis, own, one, two, three, data):
    here = lax.axis_index(axis)
    data[here] = own[...]
    data[here + 1 - 2 * (here % 2)] = one[...]
    data[(here + 2) % 4] = two[...]
    data[3 - here] = three[...]
    return here


def run_over(here, data, mine, k):
    zero = jnp.zeros((16, 128), F32)
    state, decay = (zero, zero), (zero + 1.0, zero)
    before, before_decay = state, decay
    for n in range(4) if k == 0 else range(3, -1, -1):
        before = pick(n == here, state, before)
        before_decay = pick(n == here, decay, before_decay)
        step = decay_over(span_of(data.at[n]), mine[k])
        state = plus(times_of(step, state), states_of(data.at[n], k))
        decay = times_of(step, decay)
    return state, before, before_decay


def group_kernel(axis, own, one, two, three, pars, *refs):
    *sends, before_ref, data = refs
    here = gather_four(axis, own, one, two, three, data)
    mine = my_pars(pars)
    totals = []
    for k in range(2):
        total, before, decay = run_over(here, data, mine, k)
        totals.append(total)
        keep_at(before_ref, k, before)
        keep_at(before_ref, 2 + k, decay)
    span = own[64:72, :] + one[64:72, :] + two[64:72, :] + three[64:72, :]
    if len(sends) == 1:
        for k in range(2):
            keep_states(sends[0], k, totals[k])
        sends[0][64:72, :] = span
        return
    here = lax.axis_index("z")
    partners = ((here + 2) % 4, 3 - here, here + 1 - 2 * (here % 2))
    for partner, send in zip(partners, sends):
        keep_states(send, 0, pick(partner > here, totals[0], totals[1]))
        send[32:40, :] = span


def enter_kernel(one, two, three, before_x, before_y, own, other, pars, mine_ref, theirs_ref, data):
    here = lax.axis_index("z")
    data[here] = one[...]
    data[here + 1 - 2 * (here % 2)] = one[...]
    data[(here + 2) % 4] = two[...]
    data[3 - here] = three[...]
    core = lax.axis_index("c")
    mine = my_pars(pars)
    zero = jnp.zeros((16, 128), F32)
    for k in range(2):
        state = (zero, zero)
        for n in range(3) if k == 0 else range(3, 0, -1):
            span = jnp.concatenate([data[n, 32:40, :]] * 2, axis=0)
            new = plus(times_of(decay_over(span, mine[k]), state), states_of(data.at[n], 0))
            state = pick(n < here if k == 0 else n > here, new, state)
        for before in (before_x, before_y):
            state = plus(times_of((before[4 + 2 * k], before[5 + 2 * k]), state), (before[2 * k], before[2 * k + 1]))
        ahead = core == k
        early = pick(ahead, states_of(own, k), states_of(other, k))
        later = plus(times_of(decay_over(jnp.where(ahead, span_of(own), span_of(other)), mine[k]), state), early)
        keep_at(mine_ref, k, pick(ahead, state, later))
        keep_at(theirs_ref, k, pick(ahead, later, state))


def final_kernel(*refs):
    count = len(PIECES)
    own, other = refs[:2]
    nears, prefixes, tables = (refs[2 + count * n : 2 + count * n + count] for n in range(3))
    driven, skip, glu, glu_bias, outw, out_gain, out_ref, entering, response, staged, sems = refs[2 + 3 * count :]
    core = lax.axis_index("c")
    entering[core] = own[...]
    entering[1 - core] = other[...]
    start = 0
    for size, near, prefix, table in zip(PIECES, nears, prefixes, tables):

        def tile(i, start=start, near=near, prefix=prefix, table=table):
            outs = []
            for j in range(4):
                total = None
                for k in range(2):
                    pair = 4 * (start + i) + j
                    er = entering[pair // 16, 2 * k, pl.ds(pair % 16, 1), :]
                    ei = entering[pair // 16, 2 * k + 1, pl.ds(pair % 16, 1), :]
                    cr, ci = table[4 * i + j, k, 0], table[4 * i + j, k, 1]
                    rhs = jnp.concatenate(
                        [(cr * er - ci * ei).astype(BF16), (-(cr * ei + ci * er)).astype(BF16)], axis=1
                    )
                    y = nt(prefix[4 * i + j, k], rhs)
                    total = y if total is None else total + y
                outs.append(total + near[4 * i + j])
            at = 128 * i
            response[:, pl.ds(at + 128 * start, 128)] = jnp.concatenate(outs, axis=1)

        for i in range(size):
            tile(i)
        start += size
    x = response[...] + skip[...] * driven[...].astype(F32)
    active = 0.5 * x * (1.0 + jnp.tanh(math.sqrt(2.0 / math.pi) * (x + 0.044715 * (x * x * x))))
    gate = mm(active.astype(BF16), glu[...]) + glu_bias[...]
    gated = (active * jax.nn.sigmoid(gate)).astype(BF16)
    projected = mm(gated, outw[...])
    copies = []
    for n, r in enumerate(range(0, ROWS, 32)):
        rows = projected[r : r + 32, :]
        scale = lax.rsqrt(jnp.mean(rows * rows, axis=-1, keepdims=True) + EPSILON)
        staged[r : r + 32, :] = (rows * scale * out_gain[...]).astype(BF16)
        copies.append(pltpu.make_async_copy(staged.at[r : r + 32, :], out_ref.at[r : r + 32, :], sems.at[n]))
        copies[n].start()
    for copy in copies:
        copy.wait()


def sds(shape, dtype=F32):
    return jax.ShapeDtypeStruct(shape, dtype)


def params(limit):
    return pltpu.CompilerParams(vmem_limit_bytes=limit * 1024 * 1024)


def run_local(start, size, args, weights):
    spec, distant = pl.BlockSpec(memory_space=VMEM), pl.BlockSpec(memory_space=pltpu.HBM)
    count = len(weights)
    return pl.pallas_call(
        functools.partial(local_kernel, 4 * start, 4 * size, count),
        name=f"local_{start}",
        in_specs=[spec] * len(args) + [distant] * count,
        out_specs=[spec] * (3 + count),
        out_shape=[
            sds((4 * size, ROWS, 32)),
            sds((4 * size, 2, ROWS, 256), BF16),
            sds((4 * size, 2, 2, 32, 128)),
            *(sds(weight.shape, BF16) for weight in weights),
        ],
        scratch_shapes=[
            VMEM((2, ROWS, ROWS), BF16), VMEM((SLOTS, ROWS, 256), F32), VMEM((SLOTS, 2, ROWS, 128), F32),
            VMEM((SLOTS, ROWS, 256), BF16), VMEM((SLOTS, 2, ROWS, 128), F32), VMEM((2, ROWS, 512), BF16),
            VMEM((SLOTS, 4, SPANS, 128), F32),
            *([pltpu.SemaphoreType.DMA((count,))] if count else []),
        ],
        compiler_params=params(8),
        cost_estimate=pl.CostEstimate(flops=size * 5 * 10**8, bytes_accessed=size * 2 * 2**20, transcendentals=0),
    )(*args, *weights)


def simple(kernel, name, shapes, args, scratch=()):
    spec = pl.BlockSpec(memory_space=VMEM)
    return pl.pallas_call(
        kernel,
        name=name,
        in_specs=[spec] * len(args),
        out_specs=[spec] * len(shapes),
        out_shape=[sds(shape) for shape in shapes],
        scratch_shapes=scratch,
        compiler_params=params(4),
    )(*args)


def local(
    tokens, elapsed, norm_gain, in_weight, state_input, state_output, forget_rate, decay_angle,
    skip_gain, glu_weight, glu_bias, out_weight, out_gain,
):
    elapsed_row = elapsed.reshape(1, ROWS)
    inputs = jnp.swapaxes(state_input, 3, 4)
    spec, distant = pl.BlockSpec(memory_space=VMEM), pl.BlockSpec(memory_space=pltpu.HBM)
    driven, pairs, ends, pars, damps, within, inputs_here = pl.pallas_call(
        end_kernel,
        name="ends",
        in_specs=[distant, spec, spec, distant, distant, spec, spec],
        out_specs=[spec] * 7,
        out_shape=[
            sds((ROWS, CHANNELS), BF16), sds((32, ROWS, 32), BF16), sds((2, 72, 128)), sds((2, 2, 32, 128)),
            sds((32, 2, ROWS, ROWS)), sds((2, ROWS, ROWS)), sds((2, 2, 64, 16, 64), BF16),
        ],
        scratch_shapes=[
            VMEM((ROWS, D), BF16), VMEM((ROWS, D), BF16), VMEM((3, ROWS, ROWS), F32), VMEM((CHUNKS, D, 256), BF16), VMEM((2, 256, ROWS), BF16),
            VMEM((ROWS, 256), F32), VMEM((16, 2, ROWS, 256), BF16),
            pltpu.SemaphoreType.DMA((CHUNKS,)), pltpu.SemaphoreType.DMA((CHUNKS,)), pltpu.SemaphoreType.DMA,
        ],
        compiler_params=params(12),
    )(
        *(hbm(a) for a in (tokens, elapsed_row, norm_gain.reshape(1, D), in_weight, inputs, decay_angle, forget_rate))
    )

    pieces, start = [], 0

    def piece_between(before, after, weights=()):
        index = len(pieces)
        start = sum(PIECES[:index])
        pairs_now, _ = lax.optimization_barrier((pairs, before))
        piece = run_local(
            start, PIECES[index],
            (within, damps, pairs_now, inputs_here, state_output, pars), weights,
        )
        *piece, after = lax.optimization_barrier((*piece, after))
        pieces.append(piece)
        return after

    swap = [(0, 1), (1, 0)]
    swaps = ([(0, 1), (1, 0), (2, 3), (3, 2)], [(0, 2), (2, 0), (1, 3), (3, 1)], [(0, 3), (3, 0), (1, 2), (2, 1)])

    def trade(values, axis, order, weights=()):
        found = piece_between(values[order[0]], tuple(lax.ppermute(values[n], axis, swaps[n]) for n in order), weights)
        return tuple(found[order.index(n)] for n in range(3))

    four = VMEM((4, 72, 128), F32)
    keep = ends[0]
    partner = piece_between(keep, lax.ppermute(ends[1], "c", swap))
    (total,) = simple(pair_kernel, "pair", [(72, 128)], (keep, partner, pars))
    befores = []
    for axis in ("y", "x"):
        others = trade((total,) * 3, axis, (0, 2, 1))
        *totals, before = simple(
            functools.partial(group_kernel, axis), f"group_{axis}",
            [(72, 128)] * (axis == "y") + [(40, 128)] * (3 * (axis == "x")) + [(8, 16, 128)],
            (total, *others, pars), [four],
        )
        total = totals[0]
        befores.append(before)
    others = trade(totals[2:] + totals[:2], "z", (1, 2, 0), (hbm(glu_weight), hbm(out_weight)))
    glu_here, outw_here = pieces[-1][3:]
    mine, theirs = simple(
        enter_kernel, "enter", [(4, 16, 128), (4, 16, 128)],
        (*others, befores[1], befores[0], keep, partner, pars), [VMEM((4, 40, 128), F32)],
    )
    other = piece_between(theirs, lax.ppermute(theirs, "c", swap))

    spec = pl.BlockSpec(memory_space=VMEM)
    args = (
        mine, other, *(p[0] for p in pieces), *(p[1] for p in pieces), *(p[2] for p in pieces),
        driven, skip_gain.reshape(1, CHANNELS), glu_here, glu_bias.reshape(1, CHANNELS), outw_here, out_gain.reshape(1, D),
    )
    return pl.pallas_call(
        final_kernel,
        name="final",
        in_specs=[spec] * len(args),
        out_specs=pl.BlockSpec(memory_space=pltpu.HBM),
        out_shape=sds((ROWS, D), BF16),
        scratch_shapes=[
            VMEM((2, 4, 16, 128), F32), VMEM((ROWS, CHANNELS), F32), VMEM((ROWS, D), BF16),
            pltpu.SemaphoreType.DMA((4,)),
        ],
        compiler_params=params(12),
    )(*args)


def hbm(x):
    return pltpu.with_memory_space_constraint(x, pltpu.HBM)


def solution(mesh):
    finer = Mesh(mesh.devices.reshape(4, 4, 4, 2), AXES)
    split = P(AXES, None)
    placed = (split, P(AXES), P(), P(), P(), P(), P(), P(), P(), P(), P(), P(), P())
    return jax.shard_map(local, mesh=finer, in_specs=placed, out_specs=split, check_vma=False)
```
